32 devices in a mesh: sp: 8 (over z, x), tp: 4 (over y, core).
Axes of the slice: x: 2, y: 2, z: 4, core: 2. Of those that a mesh axis runs over, the one named last changes fastest.
Arguments:
- tokens: bfloat16 [1024, 2048], P(('sp', 'tp')), may hold values from -6 to 6
- pre_gain: bfloat16 [2048], replicated, may hold values from 0.099609375 to 1.8984375
- w_query: bfloat16 [2048, 1024], P('sp', 'tp'), may hold values from -0.125 to 0.125
- w_key: bfloat16 [2048, 1024], P('sp', 'tp'), may hold values from -0.125 to 0.125
- w_value: bfloat16 [2048, 2048], P('sp', 'tp'), may hold values from -0.125 to 0.125
- w_igate: bfloat16 [2048, 8], replicated, may hold values from -1 to 1
- w_fgate: bfloat16 [2048, 8], replicated, may hold values from -0.125 to 0.125
- forget_bias: float32 [8], replicated, may hold values from 4 to 16
- gate_drift: float32 [1024, 8], P('sp'), may hold values from -2 to 2, as said below
- head_gain: bfloat16 [2048], replicated, may hold values from 0.099609375 to 1.8984375
- w_out: bfloat16 [2048, 2048], P('sp', 'tp'), may hold values from -0.125 to 0.125
Outputs:
- layer_out: bfloat16 [1024, 2048], P(('sp', 'tp'))
The draws below stay inside these ranges and needn't reach their ends.
Inputs may be any that keep to these rules, and one draw needn't show every extreme that they name: `gate_drift`: constant over aligned spans of 128 positions.
All inputs are finite; a program needn't handle non-finite values.
Results may differ from the reference program's by a relative error of at most 0.02.
Values may be sent and summed in bfloat16 or wider, within the bound.
A program may use at most 64 MiB of HBM per device.

```python
import math
import jax
import jax.numpy as jnp
from jax import lax

D = 2048
HEADS = 8
DK = 128
DV = 256
BLOCK = 64
TOKENS = 1024
HEADS_DEV = 2
N_TP = 4


def gate_columns(key):
    return jax.random.normal(jax.random.fold_in(key, 7), (D, HEADS), jnp.float32)


def draw_w_igate(key, part):
    base_cols = gate_columns(key)
    spread_scale = 1.0
    return jnp.clip(base_cols * (spread_scale / math.sqrt(D)), -1.0, 1.0).astype(jnp.bfloat16)


def draw_tokens(key, part):
    rough_rows = jax.random.normal(jax.random.fold_in(key, 1), (TOKENS, D), jnp.float32)
    return jnp.clip(rough_rows, -6.0, 6.0).astype(jnp.bfloat16)


def draw_forget_bias(key, part):
    head_order = jax.random.permutation(jax.random.fold_in(key, 4), HEADS)
    slow_count = HEADS // 2
    slow_heads = head_order < slow_count
    jitter = jax.random.uniform(jax.random.fold_in(key, 5), (HEADS,), jnp.float32, -0.3, 0.3)
    return jnp.where(slow_heads, math.log(TOKENS) + 0.8, math.log(100.0)) + jitter


def draw_gate_drift(key, part):
    span_count = TOKENS // (2 * BLOCK)
    span_level = jax.random.uniform(jax.random.fold_in(key, 6), (span_count, HEADS), jnp.float32, -1.5, 1.5)
    return jnp.repeat(span_level, 2 * BLOCK, axis=0)


def block_scale(key, shape, shards, low, high):
    def one(position, blocks):
        heights = jax.random.uniform(jax.random.fold_in(jax.random.fold_in(key, 6), position), (blocks,), jnp.float32, low / len(shards), high / len(shards))
        return jnp.repeat(jnp.exp(heights), shape[position] // blocks).reshape((-1,) + (1,) * (len(shape) - position - 1))

    level = one(*shards[0])
    for cut in shards[1:]:
        level = level * one(*cut)
    return level


def noise(stream_key, extent, spread, most, cuts=(), dtype=jnp.bfloat16):
    factor_of = block_scale(stream_key, extent, cuts, -0.22, 0.18) if cuts else 1.0
    entries = jax.random.normal(stream_key, extent, jnp.float32) * spread * factor_of
    return jnp.minimum(jnp.maximum(entries, -most), most).astype(dtype)


def setup_inputs(seed: int = 0) -> dict:
    streams_of = jax.random.split(jax.random.key(seed), 12)
    tokens = draw_tokens(jax.random.fold_in(streams_of[11], 71), 0)
    pre_gain = jnp.clip(1.0 + 0.18 * jax.random.normal(streams_of[1], (D,), jnp.float32), 0.099609375, 1.8984375).astype(jnp.bfloat16)
    w_query = noise(streams_of[2], (D, HEADS * DK), D ** -0.5, 0.125, ((0, 8), (1, 4)))
    w_key = noise(streams_of[3], (D, HEADS * DK), D ** -0.5, 0.125, ((0, 8), (1, 4)))
    w_value = noise(streams_of[4], (D, HEADS * DV), D ** -0.5, 0.125, ((0, 8), (1, 4)))
    w_igate = draw_w_igate(jax.random.fold_in(streams_of[11], 71), 0)
    w_fgate = noise(streams_of[6], (D, HEADS), D ** -0.5, 0.125)
    forget_bias = draw_forget_bias(jax.random.fold_in(streams_of[11], 71), 0)
    gate_drift = draw_gate_drift(jax.random.fold_in(streams_of[11], 71), 0)
    head_gain = jnp.clip(1.0 + 0.18 * jax.random.normal(streams_of[9], (HEADS * DV,), jnp.float32), 0.099609375, 1.8984375).astype(jnp.bfloat16)
    w_out = noise(streams_of[10], (D, HEADS * DV), (HEADS * DV) ** -0.5, 0.125, ((0, 8), (1, 4)))
    return dict(tokens=tokens, pre_gain=pre_gain, w_query=w_query, w_key=w_key, w_value=w_value, w_igate=w_igate, w_fgate=w_fgate, forget_bias=forget_bias, gate_drift=gate_drift, head_gain=head_gain, w_out=w_out)


norm_floor = 0.1
lowest_log = -1e+30
highest = lax.Precision.HIGHEST

def advance(memory, summary):
    old_mat, old_vec, old_top = memory
    span_log, span_top, span_mat, span_vec = summary
    new_top = jnp.maximum(span_log + old_top, span_top)
    kept_part = jnp.exp(span_log + old_top - new_top)
    fresh_part = jnp.exp(span_top - new_top)
    return (kept_part[:, None, None] * old_mat + fresh_part[:, None, None] * span_mat, kept_part[:, None] * old_vec + fresh_part[:, None] * span_vec, new_top)

def blend_parts(first_part, second_part):
    numer_first, denom_first, peak_first = first_part
    numer_second, denom_second, peak_second = second_part
    new_top = jnp.maximum(peak_first, peak_second)
    weight_first = jnp.exp(peak_first - new_top)
    weight_second = jnp.exp(peak_second - new_top)
    return (weight_first[..., None] * numer_first + weight_second[..., None] * numer_second, weight_first * denom_first + weight_second * denom_second, new_top)

def reference(tokens, pre_gain, w_query, w_key, w_value, w_igate, w_fgate, forget_bias, gate_drift, head_gain, w_out):
    token_wide = tokens.astype(jnp.float32)
    scaled = token_wide * lax.rsqrt(lax.optimization_barrier(jnp.mean(token_wide * token_wide, axis=1, keepdims=True)) + norm_floor)
    normed = (scaled * pre_gain.astype(jnp.float32)).astype(jnp.bfloat16)
    queries = jnp.dot(normed, w_query, preferred_element_type=jnp.float32).astype(jnp.bfloat16)
    keys_all = (jnp.dot(normed, w_key, preferred_element_type=jnp.float32) * DK ** (-0.5)).astype(jnp.bfloat16)
    values_all = jnp.dot(normed, w_value, preferred_element_type=jnp.float32).astype(jnp.bfloat16)
    log_input = jnp.dot(normed, w_igate, preferred_element_type=jnp.float32)
    forget_pre = jnp.dot(normed, w_fgate, preferred_element_type=jnp.float32) + forget_bias
    log_forget = jax.nn.log_sigmoid(forget_pre + gate_drift)
    blocks = TOKENS // BLOCK
    head_gains = head_gain.astype(jnp.float32).reshape(HEADS, DV)
    causal = jnp.arange(BLOCK)[:, None] >= jnp.arange(BLOCK)[None, :]

    def block_step(carry_state, inputs):
        memory_mat, memory_vec, memory_top = carry_state
        query_blk, key_blk, value_blk, input_row, forget_row = inputs
        query_wide = query_blk.astype(jnp.float32)
        key_wide = key_blk.astype(jnp.float32)
        value_wide = value_blk.astype(jnp.float32)
        input_gate = input_row.T
        forget_gate = forget_row.T
        within = jnp.cumsum(forget_gate, axis=1)
        log_pair = jnp.where(causal, within[:, :, None] - within[:, None, :] + input_gate[:, None, :], -jnp.inf)
        peak_intra = lax.optimization_barrier(jnp.max(log_pair, axis=2))
        scores = jnp.einsum('shd,rhd->hsr', query_wide, key_wide, precision=highest)
        weights = scores * jnp.exp(log_pair - peak_intra[:, :, None])
        weights_low = lax.optimization_barrier(weights.astype(jnp.bfloat16))
        numer_intra = jnp.einsum('hsr,rhv->hsv', weights_low.astype(jnp.float32), value_wide, precision=highest)
        denom_intra = lax.optimization_barrier(jnp.sum(weights, axis=2))
        carried_log = within + memory_top[:, None]
        numer_carry = jnp.einsum('hvd,shd->hsv', memory_mat, query_wide, precision=highest)
        denom_carry = jnp.einsum('hd,shd->hs', memory_vec, query_wide, precision=highest)
        numerator, denominator, peak_log = blend_parts((numer_carry, denom_carry, carried_log), (numer_intra, denom_intra, peak_intra))
        hidden = numerator / jnp.maximum(jnp.abs(denominator), jnp.exp(-peak_log))[:, :, None]
        hidden = hidden.transpose(1, 0, 2)
        normed_heads = hidden * lax.rsqrt(lax.optimization_barrier(jnp.mean(hidden * hidden, axis=2, keepdims=True)) + norm_floor) * head_gains
        span_log = within[:, -1]
        log_write = span_log[:, None] - within + input_gate
        span_top = lax.optimization_barrier(jnp.max(log_write, axis=1))
        write_scale = jnp.exp(log_write - span_top[:, None])
        key_scaled = key_wide * write_scale.T[:, :, None]
        span_mat = jnp.einsum('rhv,rhd->hvd', value_wide, key_scaled, precision=highest)
        span_vec = lax.optimization_barrier(jnp.sum(key_scaled, axis=0))
        new_state = advance(carry_state, (span_log, span_top, span_mat, span_vec))
        return (new_state, normed_heads.astype(jnp.bfloat16).reshape(BLOCK, HEADS * DV))
    init_state = (jnp.zeros((HEADS, DV, DK), jnp.float32), jnp.zeros((HEADS, DK), jnp.float32), jnp.full((HEADS,), lowest_log, jnp.float32))
    scanned = (queries.reshape(blocks, BLOCK, HEADS, DK), keys_all.reshape(blocks, BLOCK, HEADS, DK), values_all.reshape(blocks, BLOCK, HEADS, DV), log_input.reshape(blocks, BLOCK, HEADS), log_forget.reshape(blocks, BLOCK, HEADS))
    outputs = lax.scan(block_step, init_state, scanned)[1]
    normed_all = outputs.reshape(TOKENS, HEADS * DV)
    group_width = HEADS_DEV * DV
    total_sum = jnp.zeros((TOKENS, D), jnp.float32)
    for group_index in range(N_TP):
        columns = slice(group_index * group_width, (group_index + 1) * group_width)
        partial_value = lax.dot_general(normed_all[:, columns], w_out[:, columns], (((1,), (1,)), ((), ())), preferred_element_type=jnp.float32)
        partial_value = lax.optimization_barrier(partial_value.astype(jnp.bfloat16))
        total_sum = total_sum + partial_value.astype(jnp.float32)
    return total_sum.astype(jnp.bfloat16)
```

```python
import functools

import jax
import jax.numpy as jnp
from jax import lax
from jax.experimental import pallas as pl
from jax.experimental.pallas import tpu as pltpu
from jax.sharding import PartitionSpec as P

BLOCK = 64


norm_floor = 0.1
lowest_log = -1e30
highest = lax.Precision.HIGHEST


def prefix(value, axis, combine, identity):
    peers, position = (lax.axis_size(axis), lax.axis_index(axis))
    everything = jax.tree.map(
        lambda part, kind: lax.all_gather(part.astype(kind), axis),
        value,
        jax.tree.map(lambda a: jnp.bfloat16 if a.dtype == jnp.float32 else a.dtype, value),
    )
    start = jax.tree.map(
        lambda part, zero: jnp.broadcast_to(jnp.asarray(zero, part.dtype), part.shape),
        value,
        identity,
    )

    def step(k, before):
        reached = k < position
        new = combine(
            before, jax.tree.map(lambda part, own: part[k].astype(own.dtype), everything, value)
        )
        return jax.tree.map(lambda a, b: jnp.where(reached, a, b), new, before)

    return lax.fori_loop(0, peers, step, start)


def advance(memory, summary):
    old_mat, old_vec, old_top = memory
    span_log, span_top, span_mat, span_vec = summary
    new_top = jnp.maximum(span_log + old_top, span_top)
    kept_part = jnp.exp(span_log + old_top - new_top)
    fresh_part = jnp.exp(span_top - new_top)
    return (
        kept_part[:, None, None] * old_mat + fresh_part[:, None, None] * span_mat,
        kept_part[:, None] * old_vec + fresh_part[:, None] * span_vec,
        new_top,
    )


def prefix_states(initial, summary):

    def stepper(memory, one_block):
        return (advance(memory, one_block), memory)

    return lax.scan(stepper, initial, summary)


def join_devices(earlier, later_part):
    early_log, early_mat, early_vec, early_top = earlier
    late_log, late_mat, late_vec, late_top = later_part
    new_top = jnp.maximum(late_log + early_top, late_top)
    kept_part = jnp.exp(late_log + early_top - new_top)
    fresh_part = jnp.exp(late_top - new_top)
    return (
        early_log + late_log,
        kept_part[:, None, None] * early_mat + fresh_part[:, None, None] * late_mat,
        kept_part[:, None] * early_vec + fresh_part[:, None] * late_vec,
        new_top,
    )


def blend_parts(first_part, second_part):
    numer_first, denom_first, peak_first = first_part
    numer_second, denom_second, peak_second = second_part
    new_top = jnp.maximum(peak_first, peak_second)
    weight_first = jnp.exp(peak_first - new_top)
    weight_second = jnp.exp(peak_second - new_top)
    return (
        weight_first[..., None] * numer_first + weight_second[..., None] * numer_second,
        weight_first * denom_first + weight_second * denom_second,
        new_top,
    )


def on_device(
    tokens,
    pre_gain,
    w_query,
    w_key,
    w_value,
    w_igate,
    w_fgate,
    forget_bias,
    gate_drift,
    head_gain,
    w_out,
):
    tp_size = lax.axis_size("tp")
    head_count = w_igate.shape[1]
    local_heads = head_count // tp_size
    first_head = lax.axis_index("tp") * local_heads
    key_width = w_query.shape[1] // local_heads
    value_width = w_value.shape[1] // local_heads
    token_wide = tokens.astype(jnp.float32)
    scaled = token_wide * lax.rsqrt(
        jnp.mean(token_wide * token_wide, axis=1, keepdims=True) + norm_floor
    )
    normed = (scaled * pre_gain.astype(jnp.float32)).astype(jnp.bfloat16)
    gate_cols = jnp.concatenate(
        [
            lax.dynamic_slice_in_dim(w_igate, first_head, local_heads, 1),
            lax.dynamic_slice_in_dim(w_fgate, first_head, local_heads, 1),
        ],
        axis=1,
    )
    key_scale = key_width ** (-0.5)
    wq_full, wk_full, wv_full = (
        lax.all_gather(w_query, "sp", axis=0, tiled=True),
        lax.all_gather(w_key, "sp", axis=0, tiled=True),
        lax.all_gather(w_value, "sp", axis=0, tiled=True),
    )
    row_piece = lax.all_gather(normed, "tp", axis=0, tiled=True)
    queries_part = jnp.dot(row_piece, wq_full, preferred_element_type=jnp.float32).astype(
        jnp.bfloat16
    )
    keys_part = (
        jnp.dot(row_piece, wk_full, preferred_element_type=jnp.float32) * key_scale
    ).astype(jnp.bfloat16)
    values_part = jnp.dot(row_piece, wv_full, preferred_element_type=jnp.float32).astype(
        jnp.bfloat16
    )
    gate_part = jnp.dot(row_piece, gate_cols, preferred_element_type=jnp.float32)
    group_len = queries_part.shape[0]
    blocks = group_len // BLOCK
    log_input = gate_part[:, :local_heads]
    forget_pre = gate_part[:, local_heads:] + lax.dynamic_slice_in_dim(
        forget_bias, first_head, local_heads, 0
    )
    log_forget = jax.nn.log_sigmoid(
        forget_pre + lax.dynamic_slice_in_dim(gate_drift, first_head, local_heads, 1)
    )
    query_blk = queries_part.reshape(blocks, BLOCK, local_heads, key_width)
    key_blk = keys_part.reshape(blocks, BLOCK, local_heads, key_width)
    value_blk = values_part.reshape(blocks, BLOCK, local_heads, value_width)
    input_blk = log_input.reshape(blocks, BLOCK, local_heads).transpose(0, 2, 1)
    forget_blk = log_forget.reshape(blocks, BLOCK, local_heads).transpose(0, 2, 1)
    within = jnp.cumsum(forget_blk, axis=2)
    causal = jnp.arange(BLOCK)[:, None] >= jnp.arange(BLOCK)[None, :]
    log_pair = jnp.where(
        causal, within[..., :, None] - within[..., None, :] + input_blk[..., None, :], -jnp.inf
    )
    peak_intra = jnp.max(log_pair, axis=3)
    scores = jnp.einsum("nshd,nrhd->nhsr", query_blk, key_blk, preferred_element_type=jnp.float32)
    weights = scores * jnp.exp(log_pair - peak_intra[..., None])
    numer_intra = jnp.einsum(
        "nhsr,nrhv->nhsv",
        weights.astype(jnp.bfloat16),
        value_blk,
        preferred_element_type=jnp.float32,
    )
    denom_intra = jnp.sum(weights, axis=3)
    span_log = within[..., -1]
    log_write = span_log[..., None] - within + input_blk
    span_top = jnp.max(log_write, axis=2)
    write_scale = jnp.exp(log_write - span_top[..., None])
    key_scaled = key_blk.astype(jnp.float32) * write_scale.transpose(0, 2, 1)[..., None]
    value_wide = value_blk.astype(jnp.float32)
    span_mat = jnp.einsum("nrhv,nrhd->nhvd", value_wide, key_scaled, precision=highest)
    span_vec = jnp.sum(key_scaled, axis=1)
    summary = (span_log, span_top, span_mat, span_vec)
    empty_state = (
        jnp.zeros((local_heads, value_width, key_width), jnp.float32),
        jnp.zeros((local_heads, key_width), jnp.float32),
        jnp.full((local_heads,), lowest_log, jnp.float32),
    )
    local_end, local_starts = prefix_states(empty_state, summary)
    device_summary = (jnp.sum(span_log, axis=0),) + local_end
    identity_all = (jnp.zeros((local_heads,), jnp.float32),) + empty_state
    incoming = prefix(device_summary, "sp", join_devices, identity_all)
    query_wide = query_blk.astype(jnp.float32)
    intra_part = (numer_intra, denom_intra, peak_intra)
    start_mat, start_vec, start_top = local_starts
    local_part = (
        jnp.einsum("nhvd,nshd->nhsv", start_mat, query_wide, precision=highest),
        jnp.einsum("nhd,nshd->nhs", start_vec, query_wide, precision=highest),
        within + start_top[..., None],
    )
    numerator, denominator, peak_log = blend_parts(local_part, intra_part)
    entry_log, entry_mat, entry_vec, entry_top = incoming
    before_log = jnp.concatenate(
        [jnp.zeros((1, local_heads), jnp.float32), jnp.cumsum(span_log, axis=0)[:-1]], axis=0
    )
    from_left = (
        jnp.einsum("hvd,nshd->nhsv", entry_mat, query_wide, precision=highest),
        jnp.einsum("hd,nshd->nhs", entry_vec, query_wide, precision=highest),
        within + (before_log + entry_top[None, :])[..., None],
    )
    numerator, denominator, peak_log = blend_parts((numerator, denominator, peak_log), from_left)
    hidden = numerator / jnp.maximum(jnp.abs(denominator), jnp.exp(-peak_log))[..., None]
    hidden = hidden.transpose(0, 2, 1, 3).reshape(group_len, local_heads, value_width)
    head_gains = lax.dynamic_slice_in_dim(
        head_gain, first_head * value_width, local_heads * value_width, 0
    )
    head_gains = head_gains.astype(jnp.float32).reshape(local_heads, value_width)
    normed_heads = (
        hidden
        * lax.rsqrt(jnp.mean(hidden * hidden, axis=2, keepdims=True) + norm_floor)
        * head_gains
    )
    normed_heads = normed_heads.astype(jnp.bfloat16).reshape(group_len, local_heads * value_width)
    out_slab = lax.all_gather(w_out, "sp", axis=0, tiled=True)
    return lax.psum_scatter(
        lax.dot_general(
            normed_heads, out_slab, (((1,), (1,)), ((), ())), preferred_element_type=jnp.float32
        ).astype(jnp.bfloat16),
        "tp",
        scatter_dimension=0,
        tiled=True,
    )


drift_span = 128
MESH = pl.DeviceIdType.MESH
f32 = jnp.float32
bf16 = jnp.bfloat16


def dot_nt(a, b):
    return lax.dot_general(a, b, (((1,), (1,)), ((), ())), preferred_element_type=f32)


def layer_kernel(
    n,
    tp,
    tokens,
    pre_gain,
    w_key,
    w_value,
    w_query,
    w_igate,
    w_fgate,
    forget_bias,
    drift,
    head_gain,
    w_out,
    out,
    tok_own,
    tok_all,
    normed,
    gain_in,
    igate_in,
    fgate_in,
    bias_in,
    head_gain_in,
    drift_in,
    key_own,
    value_own,
    query_own,
    key_all,
    value_all,
    query_all,
    out_all,
    acc,
    state_all,
    aux_all,
    heads,
    heads_in,
    part,
    final_in,
    load_sems,
    tok_send,
    tok_recv,
    drift_send,
    drift_recv,
    w_send,
    w_recv,
    out_send,
    out_recv,
    state_send,
    state_recv,
    aux_send,
    aux_recv,
    heads_send,
    heads_recv,
    final_send,
    final_recv,
):
    s = lax.axis_index("sp")
    t = lax.axis_index("tp")
    layers = n // 2
    z = s // 2
    x = s % 2
    y = t // 2
    c = t % 2
    zh = z // 2
    zl = z % 2
    near = zh == c
    far = jnp.logical_not(near)
    head = layers * y + z
    rows = tok_own.shape[0]
    span = rows * tp
    length = 2 * span
    depth = key_own.shape[1]
    dk = key_own.shape[2]
    dv = value_own.shape[2]

    def flip(value):
        return 1 - value

    def at_layer(dz):
        if dz == 0:
            return z
        if dz == 1:
            return 2 * zh + flip(zl)
        if dz == 2:
            return 2 * flip(zh) + zl
        return 2 * flip(zh) + flip(zl)

    def dev(zz, xx, yy, cc):
        return 2 * zz + xx, 2 * yy + cc

    def load(source, target, sem):
        copy = pltpu.make_async_copy(source, target, sem)
        copy.start()
        return copy

    pieces = (
        (w_key, key_own, key_all),
        (w_value, value_own, value_all),
        (w_query, query_own, query_all),
    )

    def token_slot(parity, to_t):
        start = pl.multiple_of((parity * tp + to_t) * rows, rows)
        return tok_all.at[pl.ds(start, rows)]

    own_slot = token_slot(zl, t)
    load_tokens = load(tokens, tok_own, load_sems.at[0])
    loads_own = []
    for p, (w_hbm, own, full) in enumerate(pieces):
        width = own.shape[2]
        loads_own.append(
            [
                load(
                    w_hbm.at[:, pl.ds(j * width, width)],
                    own.at[j],
                    load_sems.at[1 + 2 * p + j],
                )
                for j in range(2)
            ]
        )
    chunk = out_all.shape[3] // 2
    loads_out = [
        load(
            w_out.at[pl.ds(i * chunk, chunk)],
            out_all.at[zh, x, c, pl.ds(i * chunk, chunk)],
            load_sems.at[7 + i],
        )
        for i in range(2)
    ]
    small = (
        (pre_gain, gain_in),
        (w_igate, igate_in),
        (w_fgate, fgate_in),
        (forget_bias, bias_in),
        (head_gain, head_gain_in),
    )
    loads_small = [load(a, b, load_sems.at[9 + i]) for i, (a, b) in enumerate(small)]

    @pl.when(near)
    def _():
        pltpu.make_async_copy(tokens, own_slot, tok_recv.at[zl, 0, c]).start()
        pltpu.make_async_copy(drift, drift_in.at[zl], drift_recv.at[zl]).start()
        for p, (w_hbm, own, full) in enumerate(pieces):
            width = own.shape[2]
            for j in range(2):

                @pl.when(zl == j)
                def _():
                    pltpu.make_async_copy(
                        w_hbm.at[:, pl.ds(j * width, width)], full.at[s], w_recv.at[p, s]
                    ).start()

    load_drift = load(drift, drift_in.at[2], load_sems.at[14])

    barrier = pltpu.get_barrier_semaphore()
    me = s * tp + t
    for i in range(1, n * tp):
        other = lax.rem(me + i, n * tp)
        pl.semaphore_signal(
            barrier,
            inc=1,
            device_id={"sp": other // tp, "tp": lax.rem(other, tp)},
            device_id_type=MESH,
        )

    @pl.when(c == 0)
    def _():
        state_all[layers:, :, :] = jnp.zeros((layers, dk, dv), bf16)
        aux_all[layers:, :, :] = jnp.zeros((layers, aux_all.shape[1], dk), f32)

    pl.semaphore_wait(barrier, n * tp - 1)

    started = []

    def send(source, target, send_sem, recv_sem, to, flag=None, keep=None):
        copy = pltpu.make_async_remote_copy(
            src_ref=source,
            dst_ref=target,
            send_sem=send_sem,
            recv_sem=recv_sem,
            device_id={"sp": to[0], "tp": to[1]},
            device_id_type=MESH,
        )
        if keep is not None:

            @pl.when(keep)
            def _():
                pltpu.make_async_copy(source, target, recv_sem).start()

            flag = jnp.logical_not(keep)
        if flag is None:
            copy.start()
        else:

            @pl.when(flag)
            def _():
                copy.start()

        started.append((flag, copy))

    def arrived(target, sem):
        pltpu.make_async_copy(target, target, sem).wait()

    load_tokens.wait()
    mine = tok_recv.at[zl, 0, c]
    send(tok_own, own_slot, tok_send.at[0], mine, dev(at_layer(2), x, y, zh))
    send(tok_own, own_slot, tok_send.at[1], mine, dev(at_layer(1), x, y, zh))
    send(
        tok_own, own_slot, tok_send.at[2], tok_recv.at[zl, 1, c], dev(z, x, flip(y), zh)
    )
    send(tok_own, own_slot, tok_send.at[3], mine, dev(z, x, y, flip(c)), flag=far)
    load_drift.wait()
    for i in range(1, 4):
        send(
            drift_in.at[2],
            drift_in.at[zl],
            drift_send.at[i - 1],
            drift_recv.at[zl],
            dev(at_layer(i), x, y, c),
            flag=near,
        )

    layer_a = 2 * c + zl
    layer_b = 2 * c + flip(zl)

    def first_send(p):
        _, own, full = pieces[p]
        for j in range(2):
            loads_own[p][j].wait()
        send(
            own.at[zl],
            full.at[s],
            w_send.at[p, 0],
            w_recv.at[p, s],
            dev(layer_a, x, y, zh),
            flag=far,
        )
        send(
            own.at[flip(zl)],
            full.at[s],
            w_send.at[p, 1],
            w_recv.at[p, s],
            dev(layer_b, x, y, zh),
        )

    def pass_on(p, block, i, across):
        _, _, full = pieces[p]
        sem = w_recv.at[p, block]
        arrived(full.at[block], sem)
        if across:
            send(full.at[block], full.at[block], w_send.at[p, 2 + i], sem, dev(z, flip(x), y, c))
        send(full.at[block], full.at[block], w_send.at[p, 4 + i], sem, dev(z, x, y, flip(c)))

    block_a = 2 * layer_a + x
    block_b = 2 * layer_b + x
    cross_a = 2 * layer_a + flip(x)
    cross_b = 2 * layer_b + flip(x)

    def pass_first(p, which):
        pass_on(p, (block_a, block_b)[which], which, True)

    def pass_cross(p):
        pass_on(p, cross_a, 2, False)
        pass_on(p, cross_b, 3, False)

    for p in range(3):
        first_send(p)

    def out_chunk(zb, xb, cb, i):
        return out_all.at[zb, xb, cb, pl.ds(i * chunk, chunk)]

    def out_pass(zb, xb, i, base, to):
        for k, target in enumerate(to):
            part_ref = out_chunk(zb, xb, c, i)
            send(
                part_ref,
                part_ref,
                out_send.at[base + k, i],
                out_recv.at[zb, xb, c, i],
                target,
            )

    to_x = dev(z, flip(x), y, c)
    to_core = dev(z, x, y, flip(c))
    to_half = dev(at_layer(2), x, y, c)

    def token_pass(parity, c_src, i, onward):
        slot = token_slot(parity, 2 * y + c_src)
        arrived(slot, tok_recv.at[parity, 0, c_src])
        if onward:
            send(
                slot,
                slot,
                tok_send.at[4 + i],
                tok_recv.at[parity, 0, c_src],
                dev(at_layer(1), x, y, c),
                flag=far,
            )
        send(
            slot,
            slot,
            tok_send.at[6 + i],
            tok_recv.at[parity, 1, c_src],
            dev(z, x, flip(y), c),
            flag=far if onward else None,
        )

    for copy in loads_small:
        copy.wait()
    gain = gain_in[...].astype(f32)

    def normalize(parity, to_t):
        start = pl.multiple_of((parity * tp + to_t) * rows, rows)
        wide = tok_all[pl.ds(start, rows), :].astype(f32)
        scale = lax.rsqrt(jnp.mean(wide * wide, axis=1, keepdims=True) + norm_floor)
        normed[pl.ds(start, rows), :] = (wide * scale * gain).astype(bf16)

    for c_src in range(2):
        token_pass(zl, c_src, c_src, True)
    for c_src in range(2):
        token_pass(flip(zl), c_src, 2 + c_src, False)
    for copy in loads_out:
        copy.wait()
    for i in range(2):
        out_pass(zh, x, i, 0, (to_x, to_core))
    pass_first(0, 0)
    pass_first(0, 1)
    for parity in range(2):
        for c_src in range(2):
            normalize(parity, 2 * y + c_src)
    pass_cross(0)
    pass_first(1, 0)
    pass_first(1, 1)
    for parity in range(2):
        for c_src in range(2):
            to_t = 2 * flip(y) + c_src
            arrived(token_slot(parity, to_t), tok_recv.at[parity, 1, c_src])
            normalize(parity, to_t)

    cols = (slice(0, dk), slice(dk, dk + dv), slice(dk + dv, 2 * dk + dv))
    direct = (block_a, block_b, cross_a, cross_b)
    relayed = [2 * (2 * flip(c) + k) + xx for k in range(2) for xx in range(2)]

    def product(p, block, fresh):
        at = pl.ds(pl.multiple_of(block * depth, depth), depth)
        term = jnp.dot(normed[:, at], pieces[p][2][block], preferred_element_type=f32)
        acc[:, cols[p]] = term if fresh else acc[:, cols[p]] + term

    def direct_products(p):
        for i, block in enumerate(direct):
            product(p, block, i == 0)

    def relayed_products(p):
        for block in relayed:
            arrived(pieces[p][2].at[block], w_recv.at[p, block])
            product(p, block, False)

    direct_products(0)
    pass_cross(1)
    for i in range(2):
        out_pass(zh, x, i, 2, (to_half,))
    relayed_products(0)

    all_normed = normed[...]
    gate_in = dot_nt(all_normed, igate_in[...])
    gate_forget = dot_nt(all_normed, fgate_in[...])
    pick = lax.broadcasted_iota(jnp.int32, gate_in.shape, 1) == head
    pick_bias = lax.broadcasted_iota(jnp.int32, bias_in.shape, 1) == head
    bias = jnp.sum(jnp.where(pick_bias, bias_in[...], 0.0), axis=1, keepdims=True)
    forget_all = jnp.sum(jnp.where(pick, gate_forget, 0.0), axis=1, keepdims=True) + bias
    input_all = jnp.sum(jnp.where(pick, gate_in, 0.0), axis=1, keepdims=True)
    row_id = lax.broadcasted_iota(jnp.int32, (span, span), 0)
    col_id = lax.broadcasted_iota(jnp.int32, (span, span), 1)
    causal = row_id >= col_id
    eye = row_id == col_id
    gates = []
    for j in range(2):
        arrived(drift_in.at[j], drift_recv.at[j])
        offset = drift_in[j, pl.ds(head, 1), :][:, :1]
        pre = forget_all[j * span : (j + 1) * span] + offset
        in_col = input_all[j * span : (j + 1) * span]
        lf_col = jnp.minimum(pre, 0.0) - jnp.log1p(jnp.exp(-jnp.abs(pre)))
        lf_row = jnp.sum(jnp.where(eye, lf_col, 0.0), axis=0, keepdims=True)
        in_row = jnp.sum(jnp.where(eye, in_col, 0.0), axis=0, keepdims=True)
        b_col = jnp.sum(jnp.where(causal, lf_row, 0.0), axis=1, keepdims=True)
        b_row = jnp.sum(jnp.where(row_id <= col_id, lf_col, 0.0), axis=0, keepdims=True)
        total = jnp.sum(lf_col, axis=0, keepdims=True)
        write = total - b_col + in_col
        top = jnp.max(write, axis=0, keepdims=True)
        write_scale = jnp.exp(write - top)
        log_pair = jnp.where(causal, b_col - b_row + in_row, lowest_log)
        peak = jnp.max(log_pair, axis=1, keepdims=True)
        decay = jnp.where(causal, jnp.exp(log_pair - peak), 0.0)
        gates.append((b_col, total, top, write_scale, peak, decay))

    pass_first(2, 0)
    pass_first(2, 1)
    direct_products(1)
    relayed_products(1)
    pass_cross(2)

    spans = [4 * c + 2 * j + x for j in range(2)]
    keys = (acc[:, cols[0]] * (dk**-0.5)).astype(bf16)
    values = acc[:, cols[1]].astype(bf16)
    for j in range(2):
        b_col, total, top, write_scale, peak, decay = gates[j]
        at = slice(j * span, (j + 1) * span)
        key_scaled = keys[at].astype(f32) * write_scale
        state_all[spans[j]] = jnp.dot(
            key_scaled.T.astype(bf16), values[at], preferred_element_type=f32
        ).astype(bf16)
        mine = spans[j]
        aux_all[mine, 0:1, :] = jnp.broadcast_to(total, (1, dk))
        aux_all[mine, 1:2, :] = jnp.broadcast_to(top, (1, dk))
        aux_all[mine, 2:3, :] = jnp.sum(key_scaled, axis=0, keepdims=True)
        aux_all[mine, 3:, :] = jnp.zeros((aux_all.shape[1] - 3, dk), f32)
    late = c == 1
    early = c == 0
    for k, (to, flag) in enumerate(
        (
            (dev(z, flip(x), y, c), None),
            (dev(z, flip(x), y, flip(c)), early),
            (dev(z, x, y, flip(c)), early),
        )
    ):
        for j in range(2):
            mine = spans[j]
            send(
                aux_all.at[mine],
                aux_all.at[mine],
                aux_send.at[k, j],
                aux_recv.at[mine],
                to,
                flag=flag,
            )
            send(
                state_all.at[mine],
                state_all.at[mine],
                state_send.at[k, j],
                state_recv.at[mine],
                to,
                flag=flag,
            )

    direct_products(2)
    relayed_products(2)
    queries = acc[:, cols[2]].astype(bf16)
    intra = []
    for j in range(2):
        b_col, total, top, write_scale, peak, decay = gates[j]
        at = slice(j * span, (j + 1) * span)
        weights = dot_nt(queries[at], keys[at]) * decay
        numer = jnp.dot(weights.astype(bf16), values[at], preferred_element_type=f32)
        denom = jnp.sum(weights, axis=1, keepdims=True)
        intra.append((numer, denom))

    for j in range(2):
        theirs = 4 * c + 2 * j + flip(x)
        arrived(aux_all.at[theirs], aux_recv.at[theirs])
        arrived(state_all.at[theirs], state_recv.at[theirs])

    @pl.when(late)
    def _():
        for m in range(layers):
            arrived(aux_all.at[m], aux_recv.at[m])
            arrived(state_all.at[m], state_recv.at[m])

    span_rows = aux_all[:, 0, :]
    top_rows = aux_all[:, 1, :]
    vec_rows = aux_all[:, 2, :]
    place = lax.broadcasted_iota(jnp.int32, span_rows.shape, 0)
    gain_row = head_gain_in[:, pl.ds(pl.multiple_of(head * dv, dv), dv)].astype(f32)
    for j in range(2):
        b_col, total, top, write_scale, peak, decay = gates[j]
        numer, denom = intra[j]
        at = slice(j * span, (j + 1) * span)
        before = place < spans[j]
        logs = top_rows
        for m in range(1, n):
            between = (place < m) & (spans[j] > m)
            logs = logs + jnp.where(between, span_rows[m : m + 1, :], 0.0)
        logs = jnp.where(before, logs, lowest_log)
        entry = jnp.max(logs, axis=0, keepdims=True)
        weight = jnp.where(before, jnp.exp(logs - entry), 0.0)
        vec = jnp.sum(weight * vec_rows, axis=0, keepdims=True)
        mat = jnp.zeros((dk, dv), f32)
        for m in range(n - 1):
            mat = mat + weight[m : m + 1, :1] * state_all[m].astype(f32)
        carried = b_col + entry[:, :1]
        new_top = jnp.maximum(peak, carried)
        w_intra = jnp.exp(peak - new_top)
        w_carry = jnp.exp(carried - new_top)
        numer = w_intra * numer + w_carry * jnp.dot(
            queries[at], mat.astype(bf16), preferred_element_type=f32
        )
        denom = w_intra * denom + w_carry * jnp.sum(
            queries[at].astype(f32) * vec, axis=1, keepdims=True
        )
        hidden = numer / jnp.maximum(jnp.abs(denom), jnp.exp(-new_top))
        heads[j] = (
            hidden
            * lax.rsqrt(jnp.mean(hidden * hidden, axis=1, keepdims=True) + norm_floor)
            * gain_row
        ).astype(bf16)
        for d in range(2):
            send(
                heads.at[j],
                heads_in.at[z],
                heads_send.at[j, d],
                heads_recv.at[z],
                dev(2 * c + d, x, y, j),
                keep=near & (zl == d) & (c == j),
            )

    for i in range(2):
        arrived(out_chunk(zh, flip(x), c, i), out_recv.at[zh, flip(x), c, i])
        out_pass(zh, flip(x), i, 3, (to_core,))
    for i in range(2):
        arrived(out_chunk(flip(zh), x, c, i), out_recv.at[flip(zh), x, c, i])
        out_pass(flip(zh), x, i, 4, (to_x, to_core))
    for i in range(2):
        arrived(out_chunk(flip(zh), flip(x), c, i), out_recv.at[flip(zh), flip(x), c, i])
        out_pass(flip(zh), flip(x), i, 6, (to_core,))
    for zb in range(2):
        for xb in range(2):
            for i in range(2):
                arrived(out_chunk(zb, xb, flip(c), i), out_recv.at[zb, xb, flip(c), i])
    for m in range(layers):
        arrived(heads_in.at[m], heads_recv.at[m])

    features = out_all.shape[3]
    home = 2 * zh + c
    for zb in range(2):
        for xb in range(2):
            total = jnp.zeros((span, features), f32)
            for m in range(layers):
                total = total + dot_nt(
                    heads_in[m], out_all[zb, xb, m // 2, :, (m % 2) * dv : (m % 2 + 1) * dv]
                )
            part[zb, :, xb * features : (xb + 1) * features] = total.astype(bf16)
        for yy in range(2):
            for cc in range(2):
                send(
                    part.at[zb, pl.ds((2 * yy + cc) * rows, rows)],
                    final_in.at[zl, y, zb],
                    final_send.at[zb, yy, cc],
                    final_recv.at[zl, y, zb],
                    dev(home, x, yy, cc),
                    keep=(zl == c) & (y == yy) & (c == cc),
                )
    wide = 2 * features
    for zb in range(2):
        for zz in range(2):
            total = jnp.zeros((rows, wide), f32)
            for yy in range(2):
                arrived(final_in.at[zz, yy, zb], final_recv.at[zz, yy, zb])
                total = total + final_in[zz, yy, zb].astype(f32)
            at = (zz + 2 * zb) * wide
            out[:, at : at + wide] = total.astype(bf16)

    for flag, copy in started:
        if flag is None:
            copy.wait_send()
        else:

            @pl.when(flag)
            def _():
                copy.wait_send()


def on_device_layers(
    n,
    tp,
    tokens,
    pre_gain,
    w_query,
    w_key,
    w_value,
    w_igate,
    w_fgate,
    forget_bias,
    gate_drift,
    head_gain,
    w_out,
):
    heads = w_igate.shape[1]
    rows, width = tokens.shape
    span = rows * tp
    if (
        heads != 2 * tp
        or n != heads
        or gate_drift.shape[0] != span
        or span > drift_span
    ):
        return on_device(
            tokens,
            pre_gain,
            w_query,
            w_key,
            w_value,
            w_igate,
            w_fgate,
            forget_bias,
            gate_drift,
            head_gain,
            w_out,
        )
    layers = n // 2
    depth = w_query.shape[0]
    dk = w_query.shape[1] // 2
    dv = w_value.shape[1] // 2
    features = w_out.shape[0]
    anywhere = pl.BlockSpec(memory_space=pl.ANY)
    dma = pltpu.SemaphoreType.DMA
    vmem = pltpu.VMEM
    return pl.pallas_call(
        functools.partial(layer_kernel, n, tp),
        out_shape=jax.ShapeDtypeStruct((rows, features * n), bf16),
        in_specs=[anywhere] * 11,
        out_specs=pl.BlockSpec(memory_space=pltpu.VMEM),
        scratch_shapes=[
            vmem((rows, width), bf16),
            vmem((2 * span, width), bf16),
            vmem((2 * span, width), bf16),
            vmem((1, width), bf16),
            vmem((heads, width), bf16),
            vmem((heads, width), bf16),
            vmem((1, heads), f32),
            vmem((1, heads * dv), bf16),
            vmem((3, heads, span), f32),
            vmem((2, depth, dk), bf16),
            vmem((2, depth, dv), bf16),
            vmem((2, depth, dk), bf16),
            vmem((n, depth, dk), bf16),
            vmem((n, depth, dv), bf16),
            vmem((n, depth, dk), bf16),
            vmem((2, 2, 2, features, 2 * dv), bf16),
            vmem((2 * span, 2 * dk + dv), f32),
            vmem((n, dk, dv), bf16),
            vmem((n, 8, dk), f32),
            vmem((2, span, dv), bf16),
            vmem((layers, span, dv), bf16),
            vmem((2, span, 2 * features), bf16),
            vmem((2, 2, 2, rows, 2 * features), bf16),
            dma((15,)),
            dma((10,)),
            dma((2, 2, 2)),
            dma((3,)),
            dma((2,)),
            dma((3, 8)),
            dma((3, n)),
            dma((7, 2)),
            dma((2, 2, 2, 2)),
            dma((3, 2)),
            dma((n,)),
            dma((3, 2)),
            dma((n,)),
            dma((2, 2)),
            dma((layers,)),
            dma((2, 2, 2)),
            dma((2, 2, 2)),
        ],
        compiler_params=pltpu.CompilerParams(collective_id=0, has_side_effects=True),
    )(
        tokens,
        pre_gain[None, :],
        w_key,
        w_value,
        w_query,
        w_igate.T,
        w_fgate.T,
        forget_bias[None, :],
        gate_drift.T,
        head_gain[None, :],
        w_out,
    )


def solution(mesh):
    in_specs = (
        P(("sp", "tp"), None),
        P(),
        P("sp", "tp"),
        P("sp", "tp"),
        P("sp", "tp"),
        P(),
        P(),
        P(),
        P("sp", None),
        P(),
        P("sp", "tp"),
    )
    out_specs = P(("sp", "tp"), None)
    body = on_device
    if mesh.shape["sp"] == 2 * mesh.shape["tp"] and mesh.shape["tp"] == 4:
        body = functools.partial(on_device_layers, mesh.shape["sp"], mesh.shape["tp"])
    return jax.shard_map(
        body, mesh=mesh, in_specs=in_specs, out_specs=out_specs, check_vma=False
    )
```

```python
import functools

import jax
import jax.numpy as jnp
from jax import lax
from jax.experimental import pallas as pl
from jax.experimental.pallas import tpu as pltpu
from jax.sharding import PartitionSpec as P

BLOCK = 64


norm_floor = 0.1
lowest_log = -1e30
highest = lax.Precision.HIGHEST


def prefix(value, axis, combine, identity):
    peers, position = (lax.axis_size(axis), lax.axis_index(axis))
    everything = jax.tree.map(
        lambda part, kind: lax.all_gather(part.astype(kind), axis),
        value,
        jax.tree.map(lambda a: jnp.bfloat16 if a.dtype == jnp.float32 else a.dtype, value),
    )
    start = jax.tree.map(
        lambda part, zero: jnp.broadcast_to(jnp.asarray(zero, part.dtype), part.shape),
        value,
        identity,
    )

    def step(k, before):
        reached = k < position
        new = combine(
            before, jax.tree.map(lambda part, own: part[k].astype(own.dtype), everything, value)
        )
        return jax.tree.map(lambda a, b: jnp.where(reached, a, b), new, before)

    return lax.fori_loop(0, peers, step, start)


def advance(memory, summary):
    old_mat, old_vec, old_top = memory
    span_log, span_top, span_mat, span_vec = summary
    new_top = jnp.maximum(span_log + old_top, span_top)
    kept_part = jnp.exp(span_log + old_top - new_top)
    fresh_part = jnp.exp(span_top - new_top)
    return (
        kept_part[:, None, None] * old_mat + fresh_part[:, None, None] * span_mat,
        kept_part[:, None] * old_vec + fresh_part[:, None] * span_vec,
        new_top,
    )


def prefix_states(initial, summary):

    def stepper(memory, one_block):
        return (advance(memory, one_block), memory)

    return lax.scan(stepper, initial, summary)


def join_devices(earlier, later_part):
    early_log, early_mat, early_vec, early_top = earlier
    late_log, late_mat, late_vec, late_top = later_part
    new_top = jnp.maximum(late_log + early_top, late_top)
    kept_part = jnp.exp(late_log + early_top - new_top)
    fresh_part = jnp.exp(late_top - new_top)
    return (
        early_log + late_log,
        kept_part[:, None, None] * early_mat + fresh_part[:, None, None] * late_mat,
        kept_part[:, None] * early_vec + fresh_part[:, None] * late_vec,
        new_top,
    )


def blend_parts(first_part, second_part):
    numer_first, denom_first, peak_first = first_part
    numer_second, denom_second, peak_second = second_part
    new_top = jnp.maximum(peak_first, peak_second)
    weight_first = jnp.exp(peak_first - new_top)
    weight_second = jnp.exp(peak_second - new_top)
    return (
        weight_first[..., None] * numer_first + weight_second[..., None] * numer_second,
        weight_first * denom_first + weight_second * denom_second,
        new_top,
    )


def on_device(
    tokens,
    pre_gain,
    w_query,
    w_key,
    w_value,
    w_igate,
    w_fgate,
    forget_bias,
    gate_drift,
    head_gain,
    w_out,
):
    tp_size = lax.axis_size("tp")
    head_count = w_igate.shape[1]
    local_heads = head_count // tp_size
    first_head = lax.axis_index("tp") * local_heads
    key_width = w_query.shape[1] // local_heads
    value_width = w_value.shape[1] // local_heads
    token_wide = tokens.astype(jnp.float32)
    scaled = token_wide * lax.rsqrt(
        jnp.mean(token_wide * token_wide, axis=1, keepdims=True) + norm_floor
    )
    normed = (scaled * pre_gain.astype(jnp.float32)).astype(jnp.bfloat16)
    gate_cols = jnp.concatenate(
        [
            lax.dynamic_slice_in_dim(w_igate, first_head, local_heads, 1),
            lax.dynamic_slice_in_dim(w_fgate, first_head, local_heads, 1),
        ],
        axis=1,
    )
    key_scale = key_width ** (-0.5)
    wq_full, wk_full, wv_full = (
        lax.all_gather(w_query, "sp", axis=0, tiled=True),
        lax.all_gather(w_key, "sp", axis=0, tiled=True),
        lax.all_gather(w_value, "sp", axis=0, tiled=True),
    )
    row_piece = lax.all_gather(normed, "tp", axis=0, tiled=True)
    queries_part = jnp.dot(row_piece, wq_full, preferred_element_type=jnp.float32).astype(
        jnp.bfloat16
    )
    keys_part = (
        jnp.dot(row_piece, wk_full, preferred_element_type=jnp.float32) * key_scale
    ).astype(jnp.bfloat16)
    values_part = jnp.dot(row_piece, wv_full, preferred_element_type=jnp.float32).astype(
        jnp.bfloat16
    )
    gate_part = jnp.dot(row_piece, gate_cols, preferred_element_type=jnp.float32)
    group_len = queries_part.shape[0]
    blocks = group_len // BLOCK
    log_input = gate_part[:, :local_heads]
    forget_pre = gate_part[:, local_heads:] + lax.dynamic_slice_in_dim(
        forget_bias, first_head, local_heads, 0
    )
    log_forget = jax.nn.log_sigmoid(
        forget_pre + lax.dynamic_slice_in_dim(gate_drift, first_head, local_heads, 1)
    )
    query_blk = queries_part.reshape(blocks, BLOCK, local_heads, key_width)
    key_blk = keys_part.reshape(blocks, BLOCK, local_heads, key_width)
    value_blk = values_part.reshape(blocks, BLOCK, local_heads, value_width)
    input_blk = log_input.reshape(blocks, BLOCK, local_heads).transpose(0, 2, 1)
    forget_blk = log_forget.reshape(blocks, BLOCK, local_heads).transpose(0, 2, 1)
    within = jnp.cumsum(forget_blk, axis=2)
    causal = jnp.arange(BLOCK)[:, None] >= jnp.arange(BLOCK)[None, :]
    log_pair = jnp.where(
        causal, within[..., :, None] - within[..., None, :] + input_blk[..., None, :], -jnp.inf
    )
    peak_intra = jnp.max(log_pair, axis=3)
    scores = jnp.einsum("nshd,nrhd->nhsr", query_blk, key_blk, preferred_element_type=jnp.float32)
    weights = scores * jnp.exp(log_pair - peak_intra[..., None])
    numer_intra = jnp.einsum(
        "nhsr,nrhv->nhsv",
        weights.astype(jnp.bfloat16),
        value_blk,
        preferred_element_type=jnp.float32,
    )
    denom_intra = jnp.sum(weights, axis=3)
    span_log = within[..., -1]
    log_write = span_log[..., None] - within + input_blk
    span_top = jnp.max(log_write, axis=2)
    write_scale = jnp.exp(log_write - span_top[..., None])
    key_scaled = key_blk.astype(jnp.float32) * write_scale.transpose(0, 2, 1)[..., None]
    value_wide = value_blk.astype(jnp.float32)
    span_mat = jnp.einsum("nrhv,nrhd->nhvd", value_wide, key_scaled, precision=highest)
    span_vec = jnp.sum(key_scaled, axis=1)
    summary = (span_log, span_top, span_mat, span_vec)
    empty_state = (
        jnp.zeros((local_heads, value_width, key_width), jnp.float32),
        jnp.zeros((local_heads, key_width), jnp.float32),
        jnp.full((local_heads,), lowest_log, jnp.float32),
    )
    local_end, local_starts = prefix_states(empty_state, summary)
    device_summary = (jnp.sum(span_log, axis=0),) + local_end
    identity_all = (jnp.zeros((local_heads,), jnp.float32),) + empty_state
    incoming = prefix(device_summary, "sp", join_devices, identity_all)
    query_wide = query_blk.astype(jnp.float32)
    intra_part = (numer_intra, denom_intra, peak_intra)
    start_mat, start_vec, start_top = local_starts
    local_part = (
        jnp.einsum("nhvd,nshd->nhsv", start_mat, query_wide, precision=highest),
        jnp.einsum("nhd,nshd->nhs", start_vec, query_wide, precision=highest),
        within + start_top[..., None],
    )
    numerator, denominator, peak_log = blend_parts(local_part, intra_part)
    entry_log, entry_mat, entry_vec, entry_top = incoming
    before_log = jnp.concatenate(
        [jnp.zeros((1, local_heads), jnp.float32), jnp.cumsum(span_log, axis=0)[:-1]], axis=0
    )
    from_left = (
        jnp.einsum("hvd,nshd->nhsv", entry_mat, query_wide, precision=highest),
        jnp.einsum("hd,nshd->nhs", entry_vec, query_wide, precision=highest),
        within + (before_log + entry_top[None, :])[..., None],
    )
    numerator, denominator, peak_log = blend_parts((numerator, denominator, peak_log), from_left)
    hidden = numerator / jnp.maximum(jnp.abs(denominator), jnp.exp(-peak_log))[..., None]
    hidden = hidden.transpose(0, 2, 1, 3).reshape(group_len, local_heads, value_width)
    head_gains = lax.dynamic_slice_in_dim(
        head_gain, first_head * value_width, local_heads * value_width, 0
    )
    head_gains = head_gains.astype(jnp.float32).reshape(local_heads, value_width)
    normed_heads = (
        hidden
        * lax.rsqrt(jnp.mean(hidden * hidden, axis=2, keepdims=True) + norm_floor)
        * head_gains
    )
    normed_heads = normed_heads.astype(jnp.bfloat16).reshape(group_len, local_heads * value_width)
    out_slab = lax.all_gather(w_out, "sp", axis=0, tiled=True)
    return lax.psum_scatter(
        lax.dot_general(
            normed_heads, out_slab, (((1,), (1,)), ((), ())), preferred_element_type=jnp.float32
        ).astype(jnp.bfloat16),
        "tp",
        scatter_dimension=0,
        tiled=True,
    )


drift_span = 128
MESH = pl.DeviceIdType.MESH
f32 = jnp.float32
bf16 = jnp.bfloat16


def dot_nt(a, b):
    return lax.dot_general(a, b, (((1,), (1,)), ((), ())), preferred_element_type=f32)


def layer_kernel(
    n,
    tp,
    tokens,
    pre_gain,
    w_key,
    w_value,
    w_query,
    w_igate,
    w_fgate,
    forget_bias,
    drift,
    head_gain,
    w_out,
    out,
    tok_own,
    tok_all,
    normed,
    gain_in,
    igate_in,
    fgate_in,
    bias_in,
    head_gain_in,
    drift_in,
    key_own,
    value_own,
    query_own,
    key_all,
    value_all,
    query_all,
    out_all,
    acc,
    state_all,
    aux_all,
    heads,
    heads_in,
    part,
    final_in,
    load_sems,
    tok_send,
    tok_recv,
    drift_send,
    drift_recv,
    w_send,
    w_recv,
    out_send,
    out_recv,
    state_send,
    state_recv,
    aux_send,
    aux_recv,
    heads_send,
    heads_recv,
    final_send,
    final_recv,
):
    s = lax.axis_index("sp")
    t = lax.axis_index("tp")
    layers = n // 2
    z = s // 2
    x = s % 2
    y = t // 2
    c = t % 2
    zh = z // 2
    zl = z % 2
    near = zh == c
    far = jnp.logical_not(near)
    head = layers * y + z
    rows = tok_own.shape[0]
    span = rows * tp
    length = 2 * span
    depth = key_own.shape[1]
    dk = key_own.shape[2]
    dv = value_own.shape[2]

    def flip(value):
        return 1 - value

    def at_layer(dz):
        if dz == 0:
            return z
        if dz == 1:
            return 2 * zh + flip(zl)
        if dz == 2:
            return 2 * flip(zh) + zl
        return 2 * flip(zh) + flip(zl)

    def dev(zz, xx, yy, cc):
        return 2 * zz + xx, 2 * yy + cc

    def load(source, target, sem):
        copy = pltpu.make_async_copy(source, target, sem)
        copy.start()
        return copy

    pieces = (
        (w_key, key_own, key_all),
        (w_value, value_own, value_all),
        (w_query, query_own, query_all),
    )

    def token_slot(parity, to_t):
        start = pl.multiple_of((parity * tp + to_t) * rows, rows)
        return tok_all.at[pl.ds(start, rows)]

    own_slot = token_slot(zl, t)
    load_tokens = load(tokens, tok_own, load_sems.at[0])
    loads_own = []
    for p, (w_hbm, own, full) in enumerate(pieces):
        width = own.shape[2]
        loads_own.append(
            [
                load(
                    w_hbm.at[:, pl.ds(j * width, width)],
                    own.at[j],
                    load_sems.at[1 + 2 * p + j],
                )
                for j in range(2)
            ]
        )
    chunk = out_all.shape[3] // 2
    loads_out = [
        load(
            w_out.at[pl.ds(i * chunk, chunk)],
            out_all.at[zh, x, c, pl.ds(i * chunk, chunk)],
            load_sems.at[7 + i],
        )
        for i in range(2)
    ]
    small = (
        (pre_gain, gain_in),
        (w_igate, igate_in),
        (w_fgate, fgate_in),
        (forget_bias, bias_in),
        (head_gain, head_gain_in),
    )
    loads_small = [load(a, b, load_sems.at[9 + i]) for i, (a, b) in enumerate(small)]

    @pl.when(near)
    def _():
        pltpu.make_async_copy(tokens, own_slot, tok_recv.at[zl, 0, c]).start()
        pltpu.make_async_copy(drift, drift_in.at[zl], drift_recv.at[zl]).start()
        for p, (w_hbm, own, full) in enumerate(pieces):
            width = own.shape[2]
            for j in range(2):

                @pl.when(zl == j)
                def _():
                    pltpu.make_async_copy(
                        w_hbm.at[:, pl.ds(j * width, width)], full.at[s], w_recv.at[p, s]
                    ).start()

    load_drift = load(drift, drift_in.at[2], load_sems.at[14])

    barrier = pltpu.get_barrier_semaphore()
    me = s * tp + t
    for i in range(1, n * tp):
        other = lax.rem(me + i, n * tp)
        pl.semaphore_signal(
            barrier,
            inc=1,
            device_id={"sp": other // tp, "tp": lax.rem(other, tp)},
            device_id_type=MESH,
        )

    @pl.when(c == 0)
    def _():
        state_all[layers:, :, :] = jnp.zeros((layers, dk, dv), bf16)
        aux_all[layers:, :, :] = jnp.zeros((layers, aux_all.shape[1], dk), f32)

    pl.semaphore_wait(barrier, n * tp - 1)

    started = []

    def plan(source, target, send_sem, recv_sem, to, flag=None):
        copy = pltpu.make_async_remote_copy(
            src_ref=source,
            dst_ref=target,
            send_sem=send_sem,
            recv_sem=recv_sem,
            device_id={"sp": to[0], "tp": to[1]},
            device_id_type=MESH,
        )
        started.append((flag, copy))
        return copy

    def send(source, target, send_sem, recv_sem, to, flag=None, keep=None):
        if keep is not None:

            @pl.when(keep)
            def _():
                pltpu.make_async_copy(source, target, recv_sem).start()

            flag = jnp.logical_not(keep)
        copy = plan(source, target, send_sem, recv_sem, to, flag)
        if flag is None:
            copy.start()
        else:
            pl.when(flag)(copy.start)

    def arrived(target, sem):
        pltpu.make_async_copy(target, target, sem).wait()

    load_tokens.wait()
    mine = tok_recv.at[zl, 0, c]
    send(tok_own, own_slot, tok_send.at[0], mine, dev(at_layer(2), x, y, zh))
    send(tok_own, own_slot, tok_send.at[1], mine, dev(at_layer(1), x, y, zh))
    send(
        tok_own, own_slot, tok_send.at[2], tok_recv.at[zl, 1, c], dev(z, x, flip(y), zh)
    )
    send(tok_own, own_slot, tok_send.at[3], mine, dev(z, x, y, flip(c)), flag=far)
    load_drift.wait()
    for i in range(1, 4):
        send(
            drift_in.at[2],
            drift_in.at[zl],
            drift_send.at[i - 1],
            drift_recv.at[zl],
            dev(at_layer(i), x, y, c),
            flag=near,
        )

    for copy in loads_small:
        copy.wait()
    gain = gain_in[...].astype(f32)[None, :]

    def normalize(parity, to_t):
        start = pl.multiple_of((parity * tp + to_t) * rows, rows)
        wide = tok_all[pl.ds(start, rows), :].astype(f32)
        scale = lax.rsqrt(jnp.mean(wide * wide, axis=1, keepdims=True) + norm_floor)
        normed[pl.ds(start, rows), :] = (wide * scale * gain).astype(bf16)

    to_x = dev(z, flip(x), y, c)
    to_core = dev(z, x, y, flip(c))
    to_half = dev(at_layer(2), x, y, c)

    def plan_first(p):
        _, own, full = pieces[p]
        sem = w_recv.at[p, s]
        middle = dev(1 + c * (layers - 3), x, y, c)
        end = dev(c * (layers - 1), x, y, c)
        beside = dev(at_layer(1), x, y, c)
        target = full.at[s]
        return (
            plan(own.at[flip(c)], target, w_send.at[p, 0], sem, middle, far),
            plan(own.at[c], target, w_send.at[p, 1], sem, end, far),
            plan(own.at[flip(zl)], target, w_send.at[p, 1], sem, beside, near),
        )

    def plan_pass(p, dz, across):
        block = 2 * at_layer(dz) + (flip(x) if across else x)
        full = pieces[p][2].at[block]
        sem = w_recv.at[p, block]
        i = (10 if across else 6) + dz
        onward = [plan(full, full, w_send.at[p, i], sem, to_core, near)]
        if not across:
            onward.insert(0, plan(full, full, w_send.at[p, 2 + dz], sem, to_x, near))

        def run():
            arrived(full, sem)
            for copy in onward:
                copy.start()

        return run

    def plan_token(parity, c_src, i, onward):
        slot = token_slot(parity, 2 * y + c_src)
        sem = tok_recv.at[parity, 0, c_src]
        out_sem = tok_recv.at[parity, 1, c_src]
        to_y = dev(z, x, flip(y), c)
        copies = []
        if onward:
            copies.append(
                plan(slot, slot, tok_send.at[4 + i], sem, dev(at_layer(1), x, y, c), far)
            )
        copies.append(
            plan(slot, slot, tok_send.at[6 + i], out_sem, to_y, far if onward else None)
        )

        def run(forward=True):
            arrived(slot, sem)
            if forward:
                for copy in copies:
                    copy.start()

        return run

    def out_chunk(zb, xb, cb, i):
        return out_all.at[zb, xb, cb, pl.ds(i * chunk, chunk)]

    def plan_out(zb, xb, i, base, to):
        piece = out_chunk(zb, xb, c, i)
        sem = out_recv.at[zb, xb, c, i]
        return [
            plan(piece, piece, out_send.at[base + k, i], sem, target)
            for k, target in enumerate(to)
        ]

    firsts = [plan_first(p) for p in range(3)]
    direct = [[plan_pass(p, dz, False) for dz in range(layers)] for p in range(3)]
    cross = [[plan_pass(p, dz, True) for dz in range(layers)] for p in range(3)]
    token_a = [plan_token(zl, k, k, True) for k in range(2)]
    token_b = [plan_token(flip(zl), k, 2 + k, False) for k in range(2)]
    out_own = [plan_out(zh, x, i, 0, (to_x, to_core)) for i in range(2)]
    out_half = [plan_out(zh, x, i, 2, (to_half,))[0] for i in range(2)]

    out_near_x = [plan_out(zh, flip(x), i, 3, (to_core,)) for i in range(2)]
    out_far = [plan_out(flip(zh), x, i, 4, (to_x, to_core)) for i in range(2)]
    out_far_x = [plan_out(flip(zh), flip(x), i, 6, (to_core,)) for i in range(2)]

    def out_from_x():
        for i in range(2):
            arrived(out_chunk(zh, flip(x), c, i), out_recv.at[zh, flip(x), c, i])
            out_near_x[i][0].start()

    def out_from_half():
        for i in range(2):
            arrived(out_chunk(flip(zh), x, c, i), out_recv.at[flip(zh), x, c, i])
            for copy in out_far[i]:
                copy.start()

    def out_start():
        for copy in loads_out:
            copy.wait()
        for pair in out_own:
            for copy in pair:
                copy.start()

    for p in range(3):
        for j in range(2):
            loads_own[p][j].wait()

    @pl.when(near)
    def _():
        firsts[0][2].start()
        for p in range(3):
            direct[p][0]()
        out_start()
        for run in token_a:
            run(False)
        for run in token_b:
            run()

    @pl.when(far)
    def _():
        for copy in firsts[0][:2]:
            copy.start()
        out_start()
        for run in token_a:
            run()
        for i in range(2):
            firsts[1][i].start()
        for i in range(2):
            firsts[2][i].start()
        for copy in out_half:
            copy.start()
        for run in token_b:
            run()

    for parity in range(2):
        for c_src in range(2):
            normalize(parity, 2 * y + c_src)

    @pl.when(near)
    def _():
        direct[0][1]()
        firsts[1][2].start()
        firsts[2][2].start()
        for dz in range(2, layers):
            direct[0][dz]()
        for p in range(3):
            cross[p][0]()

    for parity in range(2):
        for c_src in range(2):
            to_t = 2 * flip(y) + c_src
            arrived(token_slot(parity, to_t), tok_recv.at[parity, 1, c_src])
            normalize(parity, to_t)

    all_normed = normed[...]
    gate_in = dot_nt(all_normed, igate_in[...])
    gate_forget = dot_nt(all_normed, fgate_in[...])
    pick = lax.broadcasted_iota(jnp.int32, gate_in.shape, 1) == head
    pick_bias = lax.broadcasted_iota(jnp.int32, bias_in.shape, 1) == head
    bias = jnp.sum(jnp.where(pick_bias, bias_in[...], 0.0), axis=1, keepdims=True)
    forget_all = jnp.sum(jnp.where(pick, gate_forget, 0.0), axis=1, keepdims=True) + bias
    input_all = jnp.sum(jnp.where(pick, gate_in, 0.0), axis=1, keepdims=True)
    row_id = lax.broadcasted_iota(jnp.int32, (span, span), 0)
    col_id = lax.broadcasted_iota(jnp.int32, (span, span), 1)
    causal = row_id >= col_id
    eye = row_id == col_id
    gates = []
    for j in range(2):
        arrived(drift_in.at[j], drift_recv.at[j])
        offset = drift_in[j, pl.ds(head, 1), :][:, :1]
        pre = forget_all[j * span : (j + 1) * span] + offset
        in_col = input_all[j * span : (j + 1) * span]
        lf_col = jnp.minimum(pre, 0.0) - jnp.log1p(jnp.exp(-jnp.abs(pre)))
        lf_row = jnp.sum(jnp.where(eye, lf_col, 0.0), axis=0, keepdims=True)
        in_row = jnp.sum(jnp.where(eye, in_col, 0.0), axis=0, keepdims=True)
        b_col = jnp.sum(jnp.where(causal, lf_row, 0.0), axis=1, keepdims=True)
        b_row = jnp.sum(jnp.where(row_id <= col_id, lf_col, 0.0), axis=0, keepdims=True)
        total = jnp.sum(lf_col, axis=0, keepdims=True)
        write = total - b_col + in_col
        top = jnp.max(write, axis=0, keepdims=True)
        write_scale = jnp.exp(write - top)
        log_pair = jnp.where(causal, b_col - b_row + in_row, lowest_log)
        peak = jnp.max(log_pair, axis=1, keepdims=True)
        decay = jnp.where(causal, jnp.exp(log_pair - peak), 0.0)
        gates.append((b_col, total, top, write_scale, peak, decay))


    @pl.when(near)
    def _():
        direct[1][1]()
        for dz in range(1, layers):
            cross[0][dz]()
        for dz in range(2, layers):
            direct[1][dz]()

    cols = (slice(0, dk), slice(dk, dk + dv), slice(dk + dv, 2 * dk + dv))

    def products(p):
        first = True
        for xx in (x, flip(x)):
            for dz in range(layers):
                block = 2 * at_layer(dz) + xx
                full = pieces[p][2].at[block]
                pl.when(far)(functools.partial(arrived, full, w_recv.at[p, block]))
                at = pl.ds(pl.multiple_of(block * depth, depth), depth)
                term = jnp.dot(normed[:, at], full[...], preferred_element_type=f32)
                acc[:, cols[p]] = term if first else acc[:, cols[p]] + term
                first = False

    products(0)

    @pl.when(near)
    def _():
        direct[2][1]()
        for dz in range(1, layers):
            cross[1][dz]()
        for dz in range(2, layers):
            direct[2][dz]()
        for copy in out_half:
            copy.start()

    products(1)
    spans = [4 * c + 2 * j + x for j in range(2)]
    keys = (acc[:, cols[0]] * (dk**-0.5)).astype(bf16)
    values = acc[:, cols[1]].astype(bf16)
    for j in range(2):
        b_col, total, top, write_scale, peak, decay = gates[j]
        at = slice(j * span, (j + 1) * span)
        key_scaled = keys[at].astype(f32) * write_scale
        state_all[spans[j]] = jnp.dot(
            key_scaled.T.astype(bf16), values[at], preferred_element_type=f32
        ).astype(bf16)
        mine = spans[j]
        aux_all[mine, 0:1, :] = jnp.broadcast_to(total, (1, dk))
        aux_all[mine, 1:2, :] = jnp.broadcast_to(top, (1, dk))
        aux_all[mine, 2:3, :] = jnp.sum(key_scaled, axis=0, keepdims=True)
        aux_all[mine, 3:, :] = jnp.zeros((aux_all.shape[1] - 3, dk), f32)
    late = c == 1
    early = c == 0
    for k, (to, flag) in enumerate(
        (
            (dev(z, flip(x), y, c), None),
            (dev(z, flip(x), y, flip(c)), early),
            (dev(z, x, y, flip(c)), early),
        )
    ):
        for j in range(2):
            mine = spans[j]
            send(
                aux_all.at[mine],
                aux_all.at[mine],
                aux_send.at[k, j],
                aux_recv.at[mine],
                to,
                flag=flag,
            )
            send(
                state_all.at[mine],
                state_all.at[mine],
                state_send.at[k, j],
                state_recv.at[mine],
                to,
                flag=flag,
            )

    @pl.when(near)
    def _():
        for dz in range(1, layers):
            cross[2][dz]()

    products(2)
    out_from_half()
    queries = acc[:, cols[2]].astype(bf16)
    intra = []
    for j in range(2):
        b_col, total, top, write_scale, peak, decay = gates[j]
        at = slice(j * span, (j + 1) * span)
        weights = dot_nt(queries[at], keys[at]) * decay
        numer = jnp.dot(weights.astype(bf16), values[at], preferred_element_type=f32)
        denom = jnp.sum(weights, axis=1, keepdims=True)
        intra.append((numer, denom))

    out_from_x()
    for j in range(2):
        theirs = 4 * c + 2 * j + flip(x)
        arrived(aux_all.at[theirs], aux_recv.at[theirs])
        arrived(state_all.at[theirs], state_recv.at[theirs])

    @pl.when(late)
    def _():
        for m in range(layers):
            arrived(aux_all.at[m], aux_recv.at[m])
            arrived(state_all.at[m], state_recv.at[m])

    span_rows = aux_all[:, 0, :]
    top_rows = aux_all[:, 1, :]
    vec_rows = aux_all[:, 2, :]
    place = lax.broadcasted_iota(jnp.int32, span_rows.shape, 0)
    gain_row = head_gain_in[pl.ds(pl.multiple_of(head * dv, dv), dv)].astype(f32)[None, :]
    for j in range(2):
        b_col, total, top, write_scale, peak, decay = gates[j]
        numer, denom = intra[j]
        at = slice(j * span, (j + 1) * span)
        before = place < spans[j]
        logs = top_rows
        for m in range(1, n):
            between = (place < m) & (spans[j] > m)
            logs = logs + jnp.where(between, span_rows[m : m + 1, :], 0.0)
        logs = jnp.where(before, logs, lowest_log)
        entry = jnp.max(logs, axis=0, keepdims=True)
        weight = jnp.where(before, jnp.exp(logs - entry), 0.0)
        vec = jnp.sum(weight * vec_rows, axis=0, keepdims=True)
        mat = jnp.zeros((dk, dv), f32)
        for m in range(n - 1):
            mat = mat + weight[m : m + 1, :1] * state_all[m].astype(f32)
        carried = b_col + entry[:, :1]
        new_top = jnp.maximum(peak, carried)
        w_intra = jnp.exp(peak - new_top)
        w_carry = jnp.exp(carried - new_top)
        numer = w_intra * numer + w_carry * jnp.dot(
            queries[at], mat.astype(bf16), preferred_element_type=f32
        )
        denom = w_intra * denom + w_carry * jnp.sum(
            queries[at].astype(f32) * vec, axis=1, keepdims=True
        )
        hidden = numer / jnp.maximum(jnp.abs(denom), jnp.exp(-new_top))
        heads[j] = (
            hidden
            * lax.rsqrt(jnp.mean(hidden * hidden, axis=1, keepdims=True) + norm_floor)
            * gain_row
        ).astype(bf16)
        for d in range(2):
            send(
                heads.at[j],
                heads_in.at[z],
                heads_send.at[j, d],
                heads_recv.at[z],
                dev(2 * c + d, x, y, j),
                keep=near & (zl == d) & (c == j),
            )

    for i in range(2):
        arrived(out_chunk(flip(zh), flip(x), c, i), out_recv.at[flip(zh), flip(x), c, i])
        out_far_x[i][0].start()
    for zb in range(2):
        for xb in range(2):
            for i in range(2):
                arrived(out_chunk(zb, xb, flip(c), i), out_recv.at[zb, xb, flip(c), i])
    for m in range(layers):
        arrived(heads_in.at[m], heads_recv.at[m])

    features = out_all.shape[3]
    home = 2 * zh + c
    for zb in range(2):
        for xb in range(2):
            total = jnp.zeros((span, features), f32)
            for m in range(layers):
                total = total + dot_nt(
                    heads_in[m], out_all[zb, xb, m // 2, :, (m % 2) * dv : (m % 2 + 1) * dv]
                )
            part[zb, :, xb * features : (xb + 1) * features] = total.astype(bf16)
        for yy in range(2):
            for cc in range(2):
                send(
                    part.at[zb, pl.ds((2 * yy + cc) * rows, rows)],
                    final_in.at[zl, y, zb],
                    final_send.at[zb, yy, cc],
                    final_recv.at[zl, y, zb],
                    dev(home, x, yy, cc),
                    keep=(zl == c) & (y == yy) & (c == cc),
                )
    wide = 2 * features
    for zb in range(2):
        for zz in range(2):
            total = jnp.zeros((rows, wide), f32)
            for yy in range(2):
                arrived(final_in.at[zz, yy, zb], final_recv.at[zz, yy, zb])
                total = total + final_in[zz, yy, zb].astype(f32)
            at = (zz + 2 * zb) * wide
            out[:, at : at + wide] = total.astype(bf16)

    for flag, copy in started:
        if flag is None:
            copy.wait_send()
        else:
            pl.when(flag)(copy.wait_send)


def on_device_layers(
    n,
    tp,
    tokens,
    pre_gain,
    w_query,
    w_key,
    w_value,
    w_igate,
    w_fgate,
    forget_bias,
    gate_drift,
    head_gain,
    w_out,
):
    heads = w_igate.shape[1]
    rows, width = tokens.shape
    span = rows * tp
    if (
        heads != 2 * tp
        or n != heads
        or gate_drift.shape[0] != span
        or span > drift_span
    ):
        return on_device(
            tokens,
            pre_gain,
            w_query,
            w_key,
            w_value,
            w_igate,
            w_fgate,
            forget_bias,
            gate_drift,
            head_gain,
            w_out,
        )
    layers = n // 2
    depth = w_query.shape[0]
    dk = w_query.shape[1] // 2
    dv = w_value.shape[1] // 2
    features = w_out.shape[0]
    anywhere = pl.BlockSpec(memory_space=pl.ANY)
    dma = pltpu.SemaphoreType.DMA
    vmem = pltpu.VMEM
    return pl.pallas_call(
        functools.partial(layer_kernel, n, tp),
        out_shape=jax.ShapeDtypeStruct((rows, features * n), bf16),
        in_specs=[anywhere] * 11,
        out_specs=pl.BlockSpec(memory_space=pltpu.VMEM),
        scratch_shapes=[
            vmem((rows, width), bf16),
            vmem((2 * span, width), bf16),
            vmem((2 * span, width), bf16),
            vmem((width,), bf16),
            vmem((heads, width), bf16),
            vmem((heads, width), bf16),
            vmem((1, heads), f32),
            vmem((heads * dv,), bf16),
            vmem((3, heads, span), f32),
            vmem((2, depth, dk), bf16),
            vmem((2, depth, dv), bf16),
            vmem((2, depth, dk), bf16),
            vmem((n, depth, dk), bf16),
            vmem((n, depth, dv), bf16),
            vmem((n, depth, dk), bf16),
            vmem((2, 2, 2, features, 2 * dv), bf16),
            vmem((2 * span, 2 * dk + dv), f32),
            vmem((n, dk, dv), bf16),
            vmem((n, 8, dk), f32),
            vmem((2, span, dv), bf16),
            vmem((layers, span, dv), bf16),
            vmem((2, span, 2 * features), bf16),
            vmem((2, 2, 2, rows, 2 * features), bf16),
            dma((15,)),
            dma((10,)),
            dma((2, 2, 2)),
            dma((3,)),
            dma((2,)),
            dma((3, 6 + 2 * layers)),
            dma((3, n)),
            dma((7, 2)),
            dma((2, 2, 2, 2)),
            dma((3, 2)),
            dma((n,)),
            dma((3, 2)),
            dma((n,)),
            dma((2, 2)),
            dma((layers,)),
            dma((2, 2, 2)),
            dma((2, 2, 2)),
        ],
        compiler_params=pltpu.CompilerParams(collective_id=0, has_side_effects=True),
    )(
        tokens,
        pre_gain,
        w_key,
        w_value,
        w_query,
        w_igate.T,
        w_fgate.T,
        forget_bias[None, :],
        gate_drift.T,
        head_gain,
        w_out,
    )


def solution(mesh):
    in_specs = (
        P(("sp", "tp"), None),
        P(),
        P("sp", "tp"),
        P("sp", "tp"),
        P("sp", "tp"),
        P(),
        P(),
        P(),
        P("sp", None),
        P(),
        P("sp", "tp"),
    )
    out_specs = P(("sp", "tp"), None)
    body = on_device
    if mesh.shape["sp"] == 2 * mesh.shape["tp"] and mesh.shape["tp"] == 4:
        body = functools.partial(on_device_layers, mesh.shape["sp"], mesh.shape["tp"])
    return jax.shard_map(
        body, mesh=mesh, in_specs=in_specs, out_specs=out_specs, check_vma=False
    )
```

```python
import functools

import jax
import jax.numpy as jnp
from jax import lax
from jax.experimental import pallas as pl
from jax.experimental.pallas import tpu as pltpu
from jax.sharding import PartitionSpec as P

BLOCK = 64


norm_floor = 0.1
lowest_log = -1e30
highest = lax.Precision.HIGHEST


def prefix(value, axis, combine, identity):
    peers, position = (lax.axis_size(axis), lax.axis_index(axis))
    everything = jax.tree.map(
        lambda part, kind: lax.all_gather(part.astype(kind), axis),
        value,
        jax.tree.map(lambda a: jnp.bfloat16 if a.dtype == jnp.float32 else a.dtype, value),
    )
    start = jax.tree.map(
        lambda part, zero: jnp.broadcast_to(jnp.asarray(zero, part.dtype), part.shape),
        value,
        identity,
    )

    def step(k, before):
        reached = k < position
        new = combine(
            before, jax.tree.map(lambda part, own: part[k].astype(own.dtype), everything, value)
        )
        return jax.tree.map(lambda a, b: jnp.where(reached, a, b), new, before)

    return lax.fori_loop(0, peers, step, start)


def advance(memory, summary):
    old_mat, old_vec, old_top = memory
    span_log, span_top, span_mat, span_vec = summary
    new_top = jnp.maximum(span_log + old_top, span_top)
    kept_part = jnp.exp(span_log + old_top - new_top)
    fresh_part = jnp.exp(span_top - new_top)
    return (
        kept_part[:, None, None] * old_mat + fresh_part[:, None, None] * span_mat,
        kept_part[:, None] * old_vec + fresh_part[:, None] * span_vec,
        new_top,
    )


def prefix_states(initial, summary):

    def stepper(memory, one_block):
        return (advance(memory, one_block), memory)

    return lax.scan(stepper, initial, summary)


def join_devices(earlier, later_part):
    early_log, early_mat, early_vec, early_top = earlier
    late_log, late_mat, late_vec, late_top = later_part
    new_top = jnp.maximum(late_log + early_top, late_top)
    kept_part = jnp.exp(late_log + early_top - new_top)
    fresh_part = jnp.exp(late_top - new_top)
    return (
        early_log + late_log,
        kept_part[:, None, None] * early_mat + fresh_part[:, None, None] * late_mat,
        kept_part[:, None] * early_vec + fresh_part[:, None] * late_vec,
        new_top,
    )


def blend_parts(first_part, second_part):
    numer_first, denom_first, peak_first = first_part
    numer_second, denom_second, peak_second = second_part
    new_top = jnp.maximum(peak_first, peak_second)
    weight_first = jnp.exp(peak_first - new_top)
    weight_second = jnp.exp(peak_second - new_top)
    return (
        weight_first[..., None] * numer_first + weight_second[..., None] * numer_second,
        weight_first * denom_first + weight_second * denom_second,
        new_top,
    )


def on_device(
    tokens,
    pre_gain,
    w_query,
    w_key,
    w_value,
    w_igate,
    w_fgate,
    forget_bias,
    gate_drift,
    head_gain,
    w_out,
):
    tp_size = lax.axis_size("tp")
    head_count = w_igate.shape[1]
    local_heads = head_count // tp_size
    first_head = lax.axis_index("tp") * local_heads
    key_width = w_query.shape[1] // local_heads
    value_width = w_value.shape[1] // local_heads
    token_wide = tokens.astype(jnp.float32)
    scaled = token_wide * lax.rsqrt(
        jnp.mean(token_wide * token_wide, axis=1, keepdims=True) + norm_floor
    )
    normed = (scaled * pre_gain.astype(jnp.float32)).astype(jnp.bfloat16)
    gate_cols = jnp.concatenate(
        [
            lax.dynamic_slice_in_dim(w_igate, first_head, local_heads, 1),
            lax.dynamic_slice_in_dim(w_fgate, first_head, local_heads, 1),
        ],
        axis=1,
    )
    key_scale = key_width ** (-0.5)
    wq_full, wk_full, wv_full = (
        lax.all_gather(w_query, "sp", axis=0, tiled=True),
        lax.all_gather(w_key, "sp", axis=0, tiled=True),
        lax.all_gather(w_value, "sp", axis=0, tiled=True),
    )
    row_piece = lax.all_gather(normed, "tp", axis=0, tiled=True)
    queries_part = jnp.dot(row_piece, wq_full, preferred_element_type=jnp.float32).astype(
        jnp.bfloat16
    )
    keys_part = (
        jnp.dot(row_piece, wk_full, preferred_element_type=jnp.float32) * key_scale
    ).astype(jnp.bfloat16)
    values_part = jnp.dot(row_piece, wv_full, preferred_element_type=jnp.float32).astype(
        jnp.bfloat16
    )
    gate_part = jnp.dot(row_piece, gate_cols, preferred_element_type=jnp.float32)
    group_len = queries_part.shape[0]
    blocks = group_len // BLOCK
    log_input = gate_part[:, :local_heads]
    forget_pre = gate_part[:, local_heads:] + lax.dynamic_slice_in_dim(
        forget_bias, first_head, local_heads, 0
    )
    log_forget = jax.nn.log_sigmoid(
        forget_pre + lax.dynamic_slice_in_dim(gate_drift, first_head, local_heads, 1)
    )
    query_blk = queries_part.reshape(blocks, BLOCK, local_heads, key_width)
    key_blk = keys_part.reshape(blocks, BLOCK, local_heads, key_width)
    value_blk = values_part.reshape(blocks, BLOCK, local_heads, value_width)
    input_blk = log_input.reshape(blocks, BLOCK, local_heads).transpose(0, 2, 1)
    forget_blk = log_forget.reshape(blocks, BLOCK, local_heads).transpose(0, 2, 1)
    within = jnp.cumsum(forget_blk, axis=2)
    causal = jnp.arange(BLOCK)[:, None] >= jnp.arange(BLOCK)[None, :]
    log_pair = jnp.where(
        causal, within[..., :, None] - within[..., None, :] + input_blk[..., None, :], -jnp.inf
    )
    peak_intra = jnp.max(log_pair, axis=3)
    scores = jnp.einsum("nshd,nrhd->nhsr", query_blk, key_blk, preferred_element_type=jnp.float32)
    weights = scores * jnp.exp(log_pair - peak_intra[..., None])
    numer_intra = jnp.einsum(
        "nhsr,nrhv->nhsv",
        weights.astype(jnp.bfloat16),
        value_blk,
        preferred_element_type=jnp.float32,
    )
    denom_intra = jnp.sum(weights, axis=3)
    span_log = within[..., -1]
    log_write = span_log[..., None] - within + input_blk
    span_top = jnp.max(log_write, axis=2)
    write_scale = jnp.exp(log_write - span_top[..., None])
    key_scaled = key_blk.astype(jnp.float32) * write_scale.transpose(0, 2, 1)[..., None]
    value_wide = value_blk.astype(jnp.float32)
    span_mat = jnp.einsum("nrhv,nrhd->nhvd", value_wide, key_scaled, precision=highest)
    span_vec = jnp.sum(key_scaled, axis=1)
    summary = (span_log, span_top, span_mat, span_vec)
    empty_state = (
        jnp.zeros((local_heads, value_width, key_width), jnp.float32),
        jnp.zeros((local_heads, key_width), jnp.float32),
        jnp.full((local_heads,), lowest_log, jnp.float32),
    )
    local_end, local_starts = prefix_states(empty_state, summary)
    device_summary = (jnp.sum(span_log, axis=0),) + local_end
    identity_all = (jnp.zeros((local_heads,), jnp.float32),) + empty_state
    incoming = prefix(device_summary, "sp", join_devices, identity_all)
    query_wide = query_blk.astype(jnp.float32)
    intra_part = (numer_intra, denom_intra, peak_intra)
    start_mat, start_vec, start_top = local_starts
    local_part = (
        jnp.einsum("nhvd,nshd->nhsv", start_mat, query_wide, precision=highest),
        jnp.einsum("nhd,nshd->nhs", start_vec, query_wide, precision=highest),
        within + start_top[..., None],
    )
    numerator, denominator, peak_log = blend_parts(local_part, intra_part)
    entry_log, entry_mat, entry_vec, entry_top = incoming
    before_log = jnp.concatenate(
        [jnp.zeros((1, local_heads), jnp.float32), jnp.cumsum(span_log, axis=0)[:-1]], axis=0
    )
    from_left = (
        jnp.einsum("hvd,nshd->nhsv", entry_mat, query_wide, precision=highest),
        jnp.einsum("hd,nshd->nhs", entry_vec, query_wide, precision=highest),
        within + (before_log + entry_top[None, :])[..., None],
    )
    numerator, denominator, peak_log = blend_parts((numerator, denominator, peak_log), from_left)
    hidden = numerator / jnp.maximum(jnp.abs(denominator), jnp.exp(-peak_log))[..., None]
    hidden = hidden.transpose(0, 2, 1, 3).reshape(group_len, local_heads, value_width)
    head_gains = lax.dynamic_slice_in_dim(
        head_gain, first_head * value_width, local_heads * value_width, 0
    )
    head_gains = head_gains.astype(jnp.float32).reshape(local_heads, value_width)
    normed_heads = (
        hidden
        * lax.rsqrt(jnp.mean(hidden * hidden, axis=2, keepdims=True) + norm_floor)
        * head_gains
    )
    normed_heads = normed_heads.astype(jnp.bfloat16).reshape(group_len, local_heads * value_width)
    out_slab = lax.all_gather(w_out, "sp", axis=0, tiled=True)
    return lax.psum_scatter(
        lax.dot_general(
            normed_heads, out_slab, (((1,), (1,)), ((), ())), preferred_element_type=jnp.float32
        ).astype(jnp.bfloat16),
        "tp",
        scatter_dimension=0,
        tiled=True,
    )


drift_span = 128
MESH = pl.DeviceIdType.MESH
f32 = jnp.float32
bf16 = jnp.bfloat16


def dot_nt(a, b):
    return lax.dot_general(a, b, (((1,), (1,)), ((), ())), preferred_element_type=f32)


def layer_kernel(
    n,
    tp,
    tokens,
    pre_gain,
    w_key,
    w_value,
    w_query,
    w_igate,
    w_fgate,
    forget_bias,
    drift,
    head_gain,
    w_out,
    out,
    tok_own,
    tok_all,
    normed,
    gain_in,
    igate_in,
    fgate_in,
    bias_in,
    head_gain_in,
    drift_in,
    key_own,
    value_own,
    query_own,
    key_all,
    value_all,
    query_all,
    out_all,
    acc,
    state_all,
    aux_all,
    heads,
    heads_in,
    part,
    load_sems,
    tok_send,
    tok_recv,
    drift_send,
    drift_recv,
    w_send,
    w_recv,
    out_send,
    out_recv,
    state_send,
    state_recv,
    aux_send,
    aux_recv,
    heads_send,
    heads_recv,
    final_send,
    final_recv,
):
    s = lax.axis_index("sp")
    t = lax.axis_index("tp")
    layers = n // 2
    z = s // 2
    x = s % 2
    y = t // 2
    c = t % 2
    zh = z // 2
    zl = z % 2
    near = zh == c
    far = jnp.logical_not(near)
    head = layers * y + z
    rows = tok_own.shape[0]
    span = rows * tp
    length = 2 * span
    depth = key_own.shape[1]
    dk = key_own.shape[2]
    dv = value_own.shape[2]

    def flip(value):
        return 1 - value

    def at_layer(dz):
        if dz == 0:
            return z
        if dz == 1:
            return 2 * zh + flip(zl)
        if dz == 2:
            return 2 * flip(zh) + zl
        return 2 * flip(zh) + flip(zl)

    def dev(zz, xx, yy, cc):
        return 2 * zz + xx, 2 * yy + cc

    def load(source, target, sem):
        copy = pltpu.make_async_copy(source, target, sem)
        copy.start()
        return copy

    pieces = (
        (w_key, key_own, key_all),
        (w_value, value_own, value_all),
        (w_query, query_own, query_all),
    )

    def token_slot(parity, to_t):
        start = pl.multiple_of((parity * tp + to_t) * rows, rows)
        return tok_all.at[pl.ds(start, rows)]

    own_slot = token_slot(zl, t)
    load_tokens = load(tokens, tok_own, load_sems.at[0])
    loads_own = []
    for p, (w_hbm, own, full) in enumerate(pieces):
        width = own.shape[2]
        loads_own.append(
            [
                load(
                    w_hbm.at[:, pl.ds(j * width, width)],
                    own.at[j],
                    load_sems.at[1 + 2 * p + j],
                )
                for j in range(2)
            ]
        )
    chunk = out_all.shape[3] // 2
    loads_out = [
        load(
            w_out.at[pl.ds(i * chunk, chunk)],
            out_all.at[zh, x, c, pl.ds(i * chunk, chunk)],
            load_sems.at[7 + i],
        )
        for i in range(2)
    ]
    small = (
        (pre_gain, gain_in),
        (w_igate, igate_in),
        (w_fgate, fgate_in),
        (forget_bias, bias_in),
        (head_gain, head_gain_in),
    )
    loads_small = [load(a, b, load_sems.at[9 + i]) for i, (a, b) in enumerate(small)]

    @pl.when(near)
    def _():
        pltpu.make_async_copy(tokens, own_slot, tok_recv.at[zl, 0, c]).start()
        pltpu.make_async_copy(drift, drift_in.at[zl], drift_recv.at[zl]).start()
        for p, (w_hbm, own, full) in enumerate(pieces):
            width = own.shape[2]
            for j in range(2):

                @pl.when(zl == j)
                def _():
                    pltpu.make_async_copy(
                        w_hbm.at[:, pl.ds(j * width, width)], full.at[s], w_recv.at[p, s]
                    ).start()

    load_drift = load(drift, drift_in.at[2], load_sems.at[14])

    barrier = pltpu.get_barrier_semaphore()
    me = s * tp + t
    for i in range(1, n * tp):
        other = lax.rem(me + i, n * tp)
        pl.semaphore_signal(
            barrier,
            inc=1,
            device_id={"sp": other // tp, "tp": lax.rem(other, tp)},
            device_id_type=MESH,
        )

    @pl.when(c == 0)
    def _():
        state_all[layers:, :, :] = jnp.zeros((layers, dk, dv), bf16)
        aux_all[layers:, :, :] = jnp.zeros((layers, aux_all.shape[1], dk), f32)

    pl.semaphore_wait(barrier, n * tp - 1)

    started = []

    def plan(source, target, send_sem, recv_sem, to, flag=None):
        copy = pltpu.make_async_remote_copy(
            src_ref=source,
            dst_ref=target,
            send_sem=send_sem,
            recv_sem=recv_sem,
            device_id={"sp": to[0], "tp": to[1]},
            device_id_type=MESH,
        )
        started.append((flag, copy))
        return copy

    def send(source, target, send_sem, recv_sem, to, flag=None, keep=None):
        if keep is not None:

            @pl.when(keep)
            def _():
                pltpu.make_async_copy(source, target, recv_sem).start()

            flag = jnp.logical_not(keep)
        copy = plan(source, target, send_sem, recv_sem, to, flag)
        if flag is None:
            copy.start()
        else:
            pl.when(flag)(copy.start)

    def arrived(target, sem):
        pltpu.make_async_copy(target, target, sem).wait()

    load_tokens.wait()
    mine = tok_recv.at[zl, 0, c]
    send(tok_own, own_slot, tok_send.at[0], mine, dev(at_layer(2), x, y, zh))
    send(tok_own, own_slot, tok_send.at[1], mine, dev(at_layer(1), x, y, zh))
    send(
        tok_own, own_slot, tok_send.at[2], tok_recv.at[zl, 1, c], dev(z, x, flip(y), zh)
    )
    send(tok_own, own_slot, tok_send.at[3], mine, dev(z, x, y, flip(c)), flag=far)
    load_drift.wait()
    for i in range(1, 4):
        send(
            drift_in.at[2],
            drift_in.at[zl],
            drift_send.at[i - 1],
            drift_recv.at[zl],
            dev(at_layer(i), x, y, c),
            flag=near,
        )

    for copy in loads_small:
        copy.wait()
    gain = gain_in[...].astype(f32)[None, :]

    def normalize(parity, to_t):
        start = pl.multiple_of((parity * tp + to_t) * rows, rows)
        wide = tok_all[pl.ds(start, rows), :].astype(f32)
        scale = lax.rsqrt(jnp.mean(wide * wide, axis=1, keepdims=True) + norm_floor)
        normed[pl.ds(start, rows), :] = (wide * scale * gain).astype(bf16)

    to_x = dev(z, flip(x), y, c)
    to_core = dev(z, x, y, flip(c))
    to_half = dev(at_layer(2), x, y, c)

    def plan_first(p):
        _, own, full = pieces[p]
        sem = w_recv.at[p, s]
        middle = dev(1 + c * (layers - 3), x, y, c)
        end = dev(c * (layers - 1), x, y, c)
        beside = dev(at_layer(1), x, y, c)
        target = full.at[s]
        return (
            plan(own.at[flip(c)], target, w_send.at[p, 0], sem, middle, far),
            plan(own.at[c], target, w_send.at[p, 1], sem, end, far),
            plan(own.at[flip(zl)], target, w_send.at[p, 1], sem, beside, near),
        )

    def plan_pass(p, dz, across):
        block = 2 * at_layer(dz) + (flip(x) if across else x)
        full = pieces[p][2].at[block]
        sem = w_recv.at[p, block]
        i = (10 if across else 6) + dz
        onward = [plan(full, full, w_send.at[p, i], sem, to_core, near)]
        if not across:
            onward.insert(0, plan(full, full, w_send.at[p, 2 + dz], sem, to_x, near))

        def run():
            arrived(full, sem)
            for copy in onward:
                copy.start()

        return run

    def plan_token(parity, c_src, i, onward):
        slot = token_slot(parity, 2 * y + c_src)
        sem = tok_recv.at[parity, 0, c_src]
        out_sem = tok_recv.at[parity, 1, c_src]
        to_y = dev(z, x, flip(y), c)
        copies = []
        if onward:
            copies.append(
                plan(slot, slot, tok_send.at[4 + i], sem, dev(at_layer(1), x, y, c), far)
            )
        copies.append(
            plan(slot, slot, tok_send.at[6 + i], out_sem, to_y, far if onward else None)
        )

        def run(forward=True):
            arrived(slot, sem)
            if forward:
                for copy in copies:
                    copy.start()

        return run

    def out_chunk(zb, xb, cb, i):
        return out_all.at[zb, xb, cb, pl.ds(i * chunk, chunk)]

    def plan_out(zb, xb, i, base, to):
        piece = out_chunk(zb, xb, c, i)
        sem = out_recv.at[zb, xb, c, i]
        return [
            plan(piece, piece, out_send.at[base + k, i], sem, target)
            for k, target in enumerate(to)
        ]

    firsts = [plan_first(p) for p in range(3)]
    direct = [[plan_pass(p, dz, False) for dz in range(layers)] for p in range(3)]
    cross = [[plan_pass(p, dz, True) for dz in range(layers)] for p in range(3)]
    token_a = [plan_token(zl, k, k, True) for k in range(2)]
    token_b = [plan_token(flip(zl), k, 2 + k, False) for k in range(2)]
    out_own = [plan_out(zh, x, i, 0, (to_x, to_core)) for i in range(2)]
    out_half = [plan_out(zh, x, i, 2, (to_half,))[0] for i in range(2)]

    out_near_x = [plan_out(zh, flip(x), i, 3, (to_core,)) for i in range(2)]
    out_far = [plan_out(flip(zh), x, i, 4, (to_x, to_core)) for i in range(2)]
    out_far_x = [plan_out(flip(zh), flip(x), i, 6, (to_core,)) for i in range(2)]

    def out_from_x():
        for i in range(2):
            arrived(out_chunk(zh, flip(x), c, i), out_recv.at[zh, flip(x), c, i])
            out_near_x[i][0].start()

    def out_from_half(i):
        arrived(out_chunk(flip(zh), x, c, i), out_recv.at[flip(zh), x, c, i])
        for copy in out_far[i]:
            copy.start()

    def out_start():
        for copy in loads_out:
            copy.wait()
        for pair in out_own:
            for copy in pair:
                copy.start()

    for p in range(3):
        for j in range(2):
            loads_own[p][j].wait()

    @pl.when(near)
    def _():
        firsts[1][2].start()
        for p in (1, 0, 2):
            direct[p][0]()
        out_start()
        for run in token_a:
            run(False)
        for run in token_b:
            run()

    @pl.when(far)
    def _():
        firsts[1][1].start()
        firsts[1][0].start()
        out_start()
        for run in token_a:
            run()
        for p in (0, 2):
            for i in (1, 0):
                firsts[p][i].start()
        for copy in out_half:
            copy.start()
        for run in token_b:
            run()

    for parity in range(2):
        for c_src in range(2):
            normalize(parity, 2 * y + c_src)

    @pl.when(near)
    def _():
        firsts[0][2].start()
        firsts[2][2].start()
        direct[1][1]()
        for dz in range(2, layers):
            direct[1][dz]()
        for p in (1, 0, 2):
            cross[p][0]()

    for parity in range(2):
        for c_src in range(2):
            to_t = 2 * flip(y) + c_src
            arrived(token_slot(parity, to_t), tok_recv.at[parity, 1, c_src])
            normalize(parity, to_t)

    all_normed = normed[...]
    gate_in = dot_nt(all_normed, igate_in[...])
    gate_forget = dot_nt(all_normed, fgate_in[...])
    pick = lax.broadcasted_iota(jnp.int32, gate_in.shape, 1) == head
    pick_bias = lax.broadcasted_iota(jnp.int32, bias_in.shape, 1) == head
    bias = jnp.sum(jnp.where(pick_bias, bias_in[...], 0.0), axis=1, keepdims=True)
    forget_all = jnp.sum(jnp.where(pick, gate_forget, 0.0), axis=1, keepdims=True) + bias
    input_all = jnp.sum(jnp.where(pick, gate_in, 0.0), axis=1, keepdims=True)
    row_id = lax.broadcasted_iota(jnp.int32, (span, span), 0)
    col_id = lax.broadcasted_iota(jnp.int32, (span, span), 1)
    causal = row_id >= col_id
    eye = row_id == col_id
    gates = []
    for j in range(2):
        arrived(drift_in.at[j], drift_recv.at[j])
        offset = drift_in[j, pl.ds(head, 1), :][:, :1]
        pre = forget_all[j * span : (j + 1) * span] + offset
        in_col = input_all[j * span : (j + 1) * span]
        lf_col = jnp.minimum(pre, 0.0) - jnp.log1p(jnp.exp(-jnp.abs(pre)))
        lf_row = jnp.sum(jnp.where(eye, lf_col, 0.0), axis=0, keepdims=True)
        in_row = jnp.sum(jnp.where(eye, in_col, 0.0), axis=0, keepdims=True)
        b_col = jnp.sum(jnp.where(causal, lf_row, 0.0), axis=1, keepdims=True)
        b_row = jnp.sum(jnp.where(row_id <= col_id, lf_col, 0.0), axis=0, keepdims=True)
        total = jnp.sum(lf_col, axis=0, keepdims=True)
        write = total - b_col + in_col
        top = jnp.max(write, axis=0, keepdims=True)
        write_scale = jnp.exp(write - top)
        log_pair = jnp.where(causal, b_col - b_row + in_row, lowest_log)
        peak = jnp.max(log_pair, axis=1, keepdims=True)
        decay = jnp.where(causal, jnp.exp(log_pair - peak), 0.0)
        gates.append((b_col, total, top, write_scale, peak, decay))


    @pl.when(near)
    def _():
        for dz in range(1, layers):
            direct[0][dz]()
        for dz in range(1, layers):
            cross[1][dz]()
        for dz in range(1, layers):
            direct[2][dz]()
        for copy in out_half:
            copy.start()

    cols = (slice(0, dk), slice(dk, dk + dv), slice(dk + dv, 2 * dk + dv))

    def products(p):
        full = pieces[p][2]

        @pl.when(far)
        def _():
            for block in range(n):
                arrived(full.at[block], w_recv.at[p, block])

        flat = full[...].reshape(n * depth, full.shape[2])
        acc[:, cols[p]] = jnp.dot(normed[...], flat, preferred_element_type=f32)

    products(1)

    @pl.when(near)
    def _():
        for dz in range(1, layers):
            cross[0][dz]()

    products(0)

    spans = [4 * c + 2 * j + x for j in range(2)]
    keys = (acc[:, cols[0]] * (dk**-0.5)).astype(bf16)
    values = acc[:, cols[1]].astype(bf16)
    for j in range(2):
        b_col, total, top, write_scale, peak, decay = gates[j]
        at = slice(j * span, (j + 1) * span)
        key_scaled = keys[at].astype(f32) * write_scale
        state_all[spans[j]] = jnp.dot(
            key_scaled.T.astype(bf16), values[at], preferred_element_type=f32
        ).astype(bf16)
        mine = spans[j]
        aux_all[mine, 0:1, :] = jnp.broadcast_to(total, (1, dk))
        aux_all[mine, 1:2, :] = jnp.broadcast_to(top, (1, dk))
        aux_all[mine, 2:3, :] = jnp.sum(key_scaled, axis=0, keepdims=True)
        aux_all[mine, 3:, :] = jnp.zeros((aux_all.shape[1] - 3, dk), f32)
    late = c == 1
    early = c == 0
    for k, (to, flag) in enumerate(
        (
            (dev(z, flip(x), y, c), None),
            (dev(z, flip(x), y, flip(c)), early),
            (dev(z, x, y, flip(c)), early),
        )
    ):
        for j in range(2):
            mine = spans[j]
            send(
                aux_all.at[mine],
                aux_all.at[mine],
                aux_send.at[k, j],
                aux_recv.at[mine],
                to,
                flag=flag,
            )
            send(
                state_all.at[mine],
                state_all.at[mine],
                state_send.at[k, j],
                state_recv.at[mine],
                to,
                flag=flag,
            )

    @pl.when(near)
    def _():
        for dz in range(1, layers):
            cross[2][dz]()

    products(2)
    queries = acc[:, cols[2]].astype(bf16)
    intra = []
    for j in range(2):
        b_col, total, top, write_scale, peak, decay = gates[j]
        at = slice(j * span, (j + 1) * span)
        weights = dot_nt(queries[at], keys[at]) * decay
        numer = jnp.dot(weights.astype(bf16), values[at], preferred_element_type=f32)
        denom = jnp.sum(weights, axis=1, keepdims=True)
        intra.append((numer, denom))

    out_from_half(0)
    for j in range(2):
        theirs = 4 * c + 2 * j + flip(x)
        arrived(aux_all.at[theirs], aux_recv.at[theirs])
        arrived(state_all.at[theirs], state_recv.at[theirs])

    @pl.when(late)
    def _():
        for m in range(layers):
            arrived(aux_all.at[m], aux_recv.at[m])
            arrived(state_all.at[m], state_recv.at[m])

    span_rows = aux_all[:, 0, :]
    top_rows = aux_all[:, 1, :]
    vec_rows = aux_all[:, 2, :]
    place = lax.broadcasted_iota(jnp.int32, span_rows.shape, 0)
    gain_row = head_gain_in[pl.ds(pl.multiple_of(head * dv, dv), dv)].astype(f32)[None, :]
    for j in range(2):
        b_col, total, top, write_scale, peak, decay = gates[j]
        numer, denom = intra[j]
        at = slice(j * span, (j + 1) * span)
        before = place < spans[j]
        logs = top_rows
        for m in range(1, n):
            between = (place < m) & (spans[j] > m)
            logs = logs + jnp.where(between, span_rows[m : m + 1, :], 0.0)
        logs = jnp.where(before, logs, lowest_log)
        entry = jnp.max(logs, axis=0, keepdims=True)
        weight = jnp.where(before, jnp.exp(logs - entry), 0.0)
        vec = jnp.sum(weight * vec_rows, axis=0, keepdims=True)
        mat = jnp.zeros((dk, dv), f32)
        for m in range(n - 1):
            mat = mat + weight[m : m + 1, :1] * state_all[m].astype(f32)
        carried = b_col + entry[:, :1]
        new_top = jnp.maximum(peak, carried)
        w_intra = jnp.exp(peak - new_top)
        w_carry = jnp.exp(carried - new_top)
        numer = w_intra * numer + w_carry * jnp.dot(
            queries[at], mat.astype(bf16), preferred_element_type=f32
        )
        denom = w_intra * denom + w_carry * jnp.sum(
            queries[at].astype(f32) * vec, axis=1, keepdims=True
        )
        hidden = numer / jnp.maximum(jnp.abs(denom), jnp.exp(-new_top))
        heads[j] = (
            hidden
            * lax.rsqrt(jnp.mean(hidden * hidden, axis=1, keepdims=True) + norm_floor)
            * gain_row
        ).astype(bf16)
        for d in range(2):
            send(
                heads.at[j],
                heads_in.at[z],
                heads_send.at[j, d],
                heads_recv.at[z],
                dev(2 * c + d, x, y, j),
                keep=near & (zl == d) & (c == j),
            )

    out_from_x()
    out_from_half(1)
    features = out_all.shape[3]
    home = 2 * zh + c
    wide = 2 * features

    def landing(yy, zz, zb):
        start = pl.multiple_of((zz + 2 * zb) * wide, wide)
        return out.at[yy, :, pl.ds(start, wide)]

    def out_arrived(zb):
        for xb in range(2):
            for i in range(2):
                arrived(out_chunk(zb, xb, flip(c), i), out_recv.at[zb, xb, flip(c), i])

    def heads_arrived(half):
        for i in range(2):
            arrived(heads_in.at[2 * half + i], heads_recv.at[2 * half + i])

    def project(zb, xb, half):
        total = jnp.zeros((span, features), f32)
        for i in range(2):
            total = total + dot_nt(
                heads_in[2 * half + i], out_all[zb, xb, half, :, i * dv : (i + 1) * dv]
            )
        return total

    def share(zb):
        for yy in range(2):
            for cc in range(2):
                send(
                    part.at[zb, pl.ds((2 * yy + cc) * rows, rows)],
                    landing(y, zl, zb),
                    final_send.at[zb, yy, cc],
                    final_recv.at[zl, y, zb],
                    dev(home, x, yy, cc),
                    keep=(zl == c) & (y == yy) & (c == cc),
                )

    out_arrived(zh)
    heads_arrived(zh)
    early_part = [project(zh, xb, zh) for xb in range(2)]
    for i in range(2):
        arrived(out_chunk(flip(zh), flip(x), c, i), out_recv.at[flip(zh), flip(x), c, i])
        out_far_x[i][0].start()
    heads_arrived(flip(zh))
    for xb in range(2):
        total = early_part[xb] + project(zh, xb, flip(zh))
        part[zh, :, xb * features : (xb + 1) * features] = total.astype(bf16)
    share(zh)
    out_arrived(flip(zh))
    for xb in range(2):
        total = project(flip(zh), xb, zh) + project(flip(zh), xb, flip(zh))
        part[flip(zh), :, xb * features : (xb + 1) * features] = total.astype(bf16)
    share(flip(zh))
    for zb in range(2):
        for zz in range(2):
            for yy in range(2):
                arrived(landing(yy, zz, zb), final_recv.at[zz, yy, zb])

    for flag, copy in started:
        if flag is None:
            copy.wait_send()
        else:
            pl.when(flag)(copy.wait_send)


def on_device_layers(
    n,
    tp,
    tokens,
    pre_gain,
    w_query,
    w_key,
    w_value,
    w_igate,
    w_fgate,
    forget_bias,
    gate_drift,
    head_gain,
    w_out,
):
    heads = w_igate.shape[1]
    rows, width = tokens.shape
    span = rows * tp
    if (
        heads != 2 * tp
        or n != heads
        or gate_drift.shape[0] != span
        or span > drift_span
    ):
        return on_device(
            tokens,
            pre_gain,
            w_query,
            w_key,
            w_value,
            w_igate,
            w_fgate,
            forget_bias,
            gate_drift,
            head_gain,
            w_out,
        )
    layers = n // 2
    depth = w_query.shape[0]
    dk = w_query.shape[1] // 2
    dv = w_value.shape[1] // 2
    features = w_out.shape[0]
    anywhere = pl.BlockSpec(memory_space=pl.ANY)
    dma = pltpu.SemaphoreType.DMA
    vmem = pltpu.VMEM
    parts = pl.pallas_call(
        functools.partial(layer_kernel, n, tp),
        out_shape=pltpu.VMEM((2, rows, features * n), bf16),
        in_specs=[anywhere] * 11,
        out_specs=anywhere,
        scratch_shapes=[
            vmem((rows, width), bf16),
            vmem((2 * span, width), bf16),
            vmem((2 * span, width), bf16),
            vmem((width,), bf16),
            vmem((heads, width), bf16),
            vmem((heads, width), bf16),
            vmem((1, heads), f32),
            vmem((heads * dv,), bf16),
            vmem((3, heads, span), f32),
            vmem((2, depth, dk), bf16),
            vmem((2, depth, dv), bf16),
            vmem((2, depth, dk), bf16),
            vmem((n, depth, dk), bf16),
            vmem((n, depth, dv), bf16),
            vmem((n, depth, dk), bf16),
            vmem((2, 2, 2, features, 2 * dv), bf16),
            vmem((2 * span, 2 * dk + dv), f32),
            vmem((n, dk, dv), bf16),
            vmem((n, 8, dk), f32),
            vmem((2, span, dv), bf16),
            vmem((layers, span, dv), bf16),
            vmem((2, span, 2 * features), bf16),
            dma((15,)),
            dma((10,)),
            dma((2, 2, 2)),
            dma((3,)),
            dma((2,)),
            dma((3, 6 + 2 * layers)),
            dma((3, n)),
            dma((7, 2)),
            dma((2, 2, 2, 2)),
            dma((3, 2)),
            dma((n,)),
            dma((3, 2)),
            dma((n,)),
            dma((2, 2)),
            dma((layers,)),
            dma((2, 2, 2)),
            dma((2, 2, 2)),
        ],
        compiler_params=pltpu.CompilerParams(collective_id=0, has_side_effects=True),
    )(
        tokens,
        pre_gain,
        w_key,
        w_value,
        w_query,
        w_igate.T,
        w_fgate.T,
        forget_bias[None, :],
        gate_drift.T,
        head_gain,
        w_out,
    )
    return jnp.sum(parts.astype(f32), axis=0).astype(bf16)


def solution(mesh):
    in_specs = (
        P(("sp", "tp"), None),
        P(),
        P("sp", "tp"),
        P("sp", "tp"),
        P("sp", "tp"),
        P(),
        P(),
        P(),
        P("sp", None),
        P(),
        P("sp", "tp"),
    )
    out_specs = P(("sp", "tp"), None)
    body = on_device
    if mesh.shape["sp"] == 2 * mesh.shape["tp"] and mesh.shape["tp"] == 4:
        body = functools.partial(on_device_layers, mesh.shape["sp"], mesh.shape["tp"])
    return jax.shard_map(
        body, mesh=mesh, in_specs=in_specs, out_specs=out_specs, check_vma=False
    )
```

```python
import functools

import jax
import jax.numpy as jnp
from jax import lax
from jax.experimental import pallas as pl
from jax.experimental.pallas import tpu as pltpu
from jax.sharding import PartitionSpec as P

BLOCK = 64


norm_floor = 0.1
lowest_log = -1e30
highest = lax.Precision.HIGHEST


def prefix(value, axis, combine, identity):
    peers, position = (lax.axis_size(axis), lax.axis_index(axis))
    everything = jax.tree.map(
        lambda part, kind: lax.all_gather(part.astype(kind), axis),
        value,
        jax.tree.map(lambda a: jnp.bfloat16 if a.dtype == jnp.float32 else a.dtype, value),
    )
    start = jax.tree.map(
        lambda part, zero: jnp.broadcast_to(jnp.asarray(zero, part.dtype), part.shape),
        value,
        identity,
    )

    def step(k, before):
        reached = k < position
        new = combine(
            before, jax.tree.map(lambda part, own: part[k].astype(own.dtype), everything, value)
        )
        return jax.tree.map(lambda a, b: jnp.where(reached, a, b), new, before)

    return lax.fori_loop(0, peers, step, start)


def advance(memory, summary):
    old_mat, old_vec, old_top = memory
    span_log, span_top, span_mat, span_vec = summary
    new_top = jnp.maximum(span_log + old_top, span_top)
    kept_part = jnp.exp(span_log + old_top - new_top)
    fresh_part = jnp.exp(span_top - new_top)
    return (
        kept_part[:, None, None] * old_mat + fresh_part[:, None, None] * span_mat,
        kept_part[:, None] * old_vec + fresh_part[:, None] * span_vec,
        new_top,
    )


def prefix_states(initial, summary):

    def stepper(memory, one_block):
        return (advance(memory, one_block), memory)

    return lax.scan(stepper, initial, summary)


def join_devices(earlier, later_part):
    early_log, early_mat, early_vec, early_top = earlier
    late_log, late_mat, late_vec, late_top = later_part
    new_top = jnp.maximum(late_log + early_top, late_top)
    kept_part = jnp.exp(late_log + early_top - new_top)
    fresh_part = jnp.exp(late_top - new_top)
    return (
        early_log + late_log,
        kept_part[:, None, None] * early_mat + fresh_part[:, None, None] * late_mat,
        kept_part[:, None] * early_vec + fresh_part[:, None] * late_vec,
        new_top,
    )


def blend_parts(first_part, second_part):
    numer_first, denom_first, peak_first = first_part
    numer_second, denom_second, peak_second = second_part
    new_top = jnp.maximum(peak_first, peak_second)
    weight_first = jnp.exp(peak_first - new_top)
    weight_second = jnp.exp(peak_second - new_top)
    return (
        weight_first[..., None] * numer_first + weight_second[..., None] * numer_second,
        weight_first * denom_first + weight_second * denom_second,
        new_top,
    )


def on_device(
    tokens,
    pre_gain,
    w_query,
    w_key,
    w_value,
    w_igate,
    w_fgate,
    forget_bias,
    gate_drift,
    head_gain,
    w_out,
):
    tp_size = lax.axis_size("tp")
    head_count = w_igate.shape[1]
    local_heads = head_count // tp_size
    first_head = lax.axis_index("tp") * local_heads
    key_width = w_query.shape[1] // local_heads
    value_width = w_value.shape[1] // local_heads
    token_wide = tokens.astype(jnp.float32)
    scaled = token_wide * lax.rsqrt(
        jnp.mean(token_wide * token_wide, axis=1, keepdims=True) + norm_floor
    )
    normed = (scaled * pre_gain.astype(jnp.float32)).astype(jnp.bfloat16)
    gate_cols = jnp.concatenate(
        [
            lax.dynamic_slice_in_dim(w_igate, first_head, local_heads, 1),
            lax.dynamic_slice_in_dim(w_fgate, first_head, local_heads, 1),
        ],
        axis=1,
    )
    key_scale = key_width ** (-0.5)
    wq_full, wk_full, wv_full = (
        lax.all_gather(w_query, "sp", axis=0, tiled=True),
        lax.all_gather(w_key, "sp", axis=0, tiled=True),
        lax.all_gather(w_value, "sp", axis=0, tiled=True),
    )
    row_piece = lax.all_gather(normed, "tp", axis=0, tiled=True)
    queries_part = jnp.dot(row_piece, wq_full, preferred_element_type=jnp.float32).astype(
        jnp.bfloat16
    )
    keys_part = (
        jnp.dot(row_piece, wk_full, preferred_element_type=jnp.float32) * key_scale
    ).astype(jnp.bfloat16)
    values_part = jnp.dot(row_piece, wv_full, preferred_element_type=jnp.float32).astype(
        jnp.bfloat16
    )
    gate_part = jnp.dot(row_piece, gate_cols, preferred_element_type=jnp.float32)
    group_len = queries_part.shape[0]
    blocks = group_len // BLOCK
    log_input = gate_part[:, :local_heads]
    forget_pre = gate_part[:, local_heads:] + lax.dynamic_slice_in_dim(
        forget_bias, first_head, local_heads, 0
    )
    log_forget = jax.nn.log_sigmoid(
        forget_pre + lax.dynamic_slice_in_dim(gate_drift, first_head, local_heads, 1)
    )
    query_blk = queries_part.reshape(blocks, BLOCK, local_heads, key_width)
    key_blk = keys_part.reshape(blocks, BLOCK, local_heads, key_width)
    value_blk = values_part.reshape(blocks, BLOCK, local_heads, value_width)
    input_blk = log_input.reshape(blocks, BLOCK, local_heads).transpose(0, 2, 1)
    forget_blk = log_forget.reshape(blocks, BLOCK, local_heads).transpose(0, 2, 1)
    within = jnp.cumsum(forget_blk, axis=2)
    causal = jnp.arange(BLOCK)[:, None] >= jnp.arange(BLOCK)[None, :]
    log_pair = jnp.where(
        causal, within[..., :, None] - within[..., None, :] + input_blk[..., None, :], -jnp.inf
    )
    peak_intra = jnp.max(log_pair, axis=3)
    scores = jnp.einsum("nshd,nrhd->nhsr", query_blk, key_blk, preferred_element_type=jnp.float32)
    weights = scores * jnp.exp(log_pair - peak_intra[..., None])
    numer_intra = jnp.einsum(
        "nhsr,nrhv->nhsv",
        weights.astype(jnp.bfloat16),
        value_blk,
        preferred_element_type=jnp.float32,
    )
    denom_intra = jnp.sum(weights, axis=3)
    span_log = within[..., -1]
    log_write = span_log[..., None] - within + input_blk
    span_top = jnp.max(log_write, axis=2)
    write_scale = jnp.exp(log_write - span_top[..., None])
    key_scaled = key_blk.astype(jnp.float32) * write_scale.transpose(0, 2, 1)[..., None]
    value_wide = value_blk.astype(jnp.float32)
    span_mat = jnp.einsum("nrhv,nrhd->nhvd", value_wide, key_scaled, precision=highest)
    span_vec = jnp.sum(key_scaled, axis=1)
    summary = (span_log, span_top, span_mat, span_vec)
    empty_state = (
        jnp.zeros((local_heads, value_width, key_width), jnp.float32),
        jnp.zeros((local_heads, key_width), jnp.float32),
        jnp.full((local_heads,), lowest_log, jnp.float32),
    )
    local_end, local_starts = prefix_states(empty_state, summary)
    device_summary = (jnp.sum(span_log, axis=0),) + local_end
    identity_all = (jnp.zeros((local_heads,), jnp.float32),) + empty_state
    incoming = prefix(device_summary, "sp", join_devices, identity_all)
    query_wide = query_blk.astype(jnp.float32)
    intra_part = (numer_intra, denom_intra, peak_intra)
    start_mat, start_vec, start_top = local_starts
    local_part = (
        jnp.einsum("nhvd,nshd->nhsv", start_mat, query_wide, precision=highest),
        jnp.einsum("nhd,nshd->nhs", start_vec, query_wide, precision=highest),
        within + start_top[..., None],
    )
    numerator, denominator, peak_log = blend_parts(local_part, intra_part)
    entry_log, entry_mat, entry_vec, entry_top = incoming
    before_log = jnp.concatenate(
        [jnp.zeros((1, local_heads), jnp.float32), jnp.cumsum(span_log, axis=0)[:-1]], axis=0
    )
    from_left = (
        jnp.einsum("hvd,nshd->nhsv", entry_mat, query_wide, precision=highest),
        jnp.einsum("hd,nshd->nhs", entry_vec, query_wide, precision=highest),
        within + (before_log + entry_top[None, :])[..., None],
    )
    numerator, denominator, peak_log = blend_parts((numerator, denominator, peak_log), from_left)
    hidden = numerator / jnp.maximum(jnp.abs(denominator), jnp.exp(-peak_log))[..., None]
    hidden = hidden.transpose(0, 2, 1, 3).reshape(group_len, local_heads, value_width)
    head_gains = lax.dynamic_slice_in_dim(
        head_gain, first_head * value_width, local_heads * value_width, 0
    )
    head_gains = head_gains.astype(jnp.float32).reshape(local_heads, value_width)
    normed_heads = (
        hidden
        * lax.rsqrt(jnp.mean(hidden * hidden, axis=2, keepdims=True) + norm_floor)
        * head_gains
    )
    normed_heads = normed_heads.astype(jnp.bfloat16).reshape(group_len, local_heads * value_width)
    out_slab = lax.all_gather(w_out, "sp", axis=0, tiled=True)
    return lax.psum_scatter(
        lax.dot_general(
            normed_heads, out_slab, (((1,), (1,)), ((), ())), preferred_element_type=jnp.float32
        ).astype(jnp.bfloat16),
        "tp",
        scatter_dimension=0,
        tiled=True,
    )


drift_span = 128
MESH = pl.DeviceIdType.MESH
f32 = jnp.float32
bf16 = jnp.bfloat16


def dot_nt(a, b):
    return lax.dot_general(a, b, (((1,), (1,)), ((), ())), preferred_element_type=f32)


def layer_kernel(
    n,
    tp,
    tokens,
    pre_gain,
    w_key,
    w_value,
    w_query,
    w_igate,
    w_fgate,
    forget_bias,
    drift,
    head_gain,
    w_out,
    out,
    tok_own,
    tok_all,
    normed,
    gain_in,
    igate_in,
    fgate_in,
    bias_in,
    head_gain_in,
    drift_in,
    key_own,
    value_own,
    query_own,
    key_all,
    value_all,
    query_all,
    out_all,
    acc,
    state_all,
    aux_all,
    heads,
    heads_in,
    part,
    load_sems,
    tok_send,
    tok_recv,
    drift_send,
    drift_recv,
    w_send,
    w_recv,
    out_send,
    out_recv,
    state_send,
    state_recv,
    aux_send,
    aux_recv,
    heads_send,
    heads_recv,
    final_send,
    final_recv,
):
    s = lax.axis_index("sp")
    t = lax.axis_index("tp")
    layers = n // 2
    z = s // 2
    x = s % 2
    y = t // 2
    c = t % 2
    zh = z // 2
    zl = z % 2
    near = zh == c
    far = jnp.logical_not(near)
    head = layers * y + z
    rows = tok_own.shape[0]
    span = rows * tp
    length = 2 * span
    depth = key_own.shape[1]
    dk = key_own.shape[2]
    dv = value_own.shape[2]

    def flip(value):
        return 1 - value

    def at_layer(dz):
        if dz == 0:
            return z
        if dz == 1:
            return 2 * zh + flip(zl)
        if dz == 2:
            return 2 * flip(zh) + zl
        return 2 * flip(zh) + flip(zl)

    def dev(zz, xx, yy, cc):
        return 2 * zz + xx, 2 * yy + cc

    def load(source, target, sem):
        copy = pltpu.make_async_copy(source, target, sem)
        copy.start()
        return copy

    pieces = (
        (w_key, key_own, key_all),
        (w_value, value_own, value_all),
        (w_query, query_own, query_all),
    )

    def token_slot(parity, to_t):
        start = pl.multiple_of((parity * tp + to_t) * rows, rows)
        return tok_all.at[pl.ds(start, rows)]

    own_slot = token_slot(zl, t)
    load_tokens = load(tokens, tok_own, load_sems.at[0])
    loads_own = []
    for p, (w_hbm, own, full) in enumerate(pieces):
        width = own.shape[2]
        loads_own.append(
            [
                load(
                    w_hbm.at[:, pl.ds(j * width, width)],
                    own.at[j],
                    load_sems.at[1 + p],
                )
                for j in range(2)
            ]
        )
    chunk = out_all.shape[3] // 2
    loads_out = [
        load(
            w_out.at[pl.ds(i * chunk, chunk)],
            out_all.at[zh, x, c, pl.ds(i * chunk, chunk)],
            load_sems.at[4],
        )
        for i in range(2)
    ]
    small = (
        (pre_gain, gain_in),
        (w_igate, igate_in),
        (w_fgate, fgate_in),
        (forget_bias, bias_in),
        (head_gain, head_gain_in),
    )
    loads_small = [load(a, b, load_sems.at[5 + i]) for i, (a, b) in enumerate(small)]

    @pl.when(near)
    def _():
        pltpu.make_async_copy(tokens, own_slot, tok_recv.at[zl, 0, c]).start()
        pltpu.make_async_copy(drift, drift_in.at[zl], drift_recv.at[zl]).start()
        for p, (w_hbm, own, full) in enumerate(pieces):
            width = own.shape[2]
            for j in range(2):

                @pl.when(zl == j)
                def _():
                    pltpu.make_async_copy(
                        w_hbm.at[:, pl.ds(j * width, width)], full.at[s], w_recv.at[p, s]
                    ).start()

    load_drift = load(drift, drift_in.at[2], load_sems.at[10])

    barrier = pltpu.get_barrier_semaphore()
    me = s * tp + t
    for i in range(1, n * tp):
        other = lax.rem(me + i, n * tp)
        pl.semaphore_signal(
            barrier,
            inc=1,
            device_id={"sp": other // tp, "tp": lax.rem(other, tp)},
            device_id_type=MESH,
        )

    @pl.when(c == 0)
    def _():
        state_all[layers:, :, :] = jnp.zeros((layers, dk, dv), bf16)
        aux_all[layers:, :, :] = jnp.zeros((layers, aux_all.shape[1], dk), f32)

    pl.semaphore_wait(barrier, n * tp - 1)

    def plan(source, target, send_sem, recv_sem, to, flag=None):
        copy = pltpu.make_async_remote_copy(
            src_ref=source,
            dst_ref=target,
            send_sem=send_sem,
            recv_sem=recv_sem,
            device_id={"sp": to[0], "tp": to[1]},
            device_id_type=MESH,
        )
        return copy

    def send(source, target, send_sem, recv_sem, to, flag=None, keep=None):
        if keep is not None:

            @pl.when(keep)
            def _():
                pltpu.make_async_copy(source, target, recv_sem).start()

            flag = jnp.logical_not(keep)
        copy = plan(source, target, send_sem, recv_sem, to, flag)
        if flag is None:
            copy.start()
        else:
            pl.when(flag)(copy.start)

    def arrived(target, sem):
        pltpu.make_async_copy(target, target, sem).wait()

    load_tokens.wait()
    mine = tok_recv.at[zl, 0, c]
    send(tok_own, own_slot, tok_send.at[0], mine, dev(at_layer(2), x, y, zh))
    send(tok_own, own_slot, tok_send.at[0], mine, dev(at_layer(1), x, y, zh))
    send(
        tok_own, own_slot, tok_send.at[0], tok_recv.at[zl, 1, c], dev(z, x, flip(y), zh)
    )
    send(tok_own, own_slot, tok_send.at[0], mine, dev(z, x, y, flip(c)), flag=far)
    load_drift.wait()
    for i in range(1, 4):
        send(
            drift_in.at[2],
            drift_in.at[zl],
            drift_send.at[0],
            drift_recv.at[zl],
            dev(at_layer(i), x, y, c),
            flag=near,
        )

    for copy in loads_small:
        copy.wait()
    gain = gain_in[...].astype(f32)[None, :]

    def normalize(parity, to_t):
        start = pl.multiple_of((parity * tp + to_t) * rows, rows)
        wide = tok_all[pl.ds(start, rows), :].astype(f32)
        scale = lax.rsqrt(jnp.mean(wide * wide, axis=1, keepdims=True) + norm_floor)
        normed[pl.ds(start, rows), :] = (wide * scale * gain).astype(bf16)

    to_x = dev(z, flip(x), y, c)
    to_core = dev(z, x, y, flip(c))
    to_half = dev(at_layer(2), x, y, c)

    def plan_first(p):
        _, own, full = pieces[p]
        sem = w_recv.at[p, s]
        middle = dev(1 + c * (layers - 3), x, y, c)
        end = dev(c * (layers - 1), x, y, c)
        beside = dev(at_layer(1), x, y, c)
        target = full.at[s]
        return (
            plan(own.at[flip(c)], target, w_send.at[p, 0], sem, middle, far),
            plan(own.at[c], target, w_send.at[p, 0], sem, end, far),
            plan(own.at[flip(zl)], target, w_send.at[p, 0], sem, beside, near),
        )

    def plan_pass(p, dz, across):
        block = 2 * at_layer(dz) + (flip(x) if across else x)
        full = pieces[p][2].at[block]
        sem = w_recv.at[p, block]
        to_far = w_recv.at[p, 0]
        onward = [plan(full, full, w_send.at[p, 2], to_far, to_core, near)]
        if not across:
            onward.insert(0, plan(full, full, w_send.at[p, 1], sem, to_x, near))

        def run():
            arrived(full, sem)
            for copy in onward:
                copy.start()

        return run

    def plan_token(parity, c_src, i, onward):
        slot = token_slot(parity, 2 * y + c_src)
        sem = tok_recv.at[parity, 0, c_src]
        out_sem = tok_recv.at[parity, 1, c_src]
        to_y = dev(z, x, flip(y), c)
        copies = []
        if onward:
            copies.append(
                plan(slot, slot, tok_send.at[1], sem, dev(at_layer(1), x, y, c), far)
            )
        copies.append(
            plan(slot, slot, tok_send.at[1], out_sem, to_y, far if onward else None)
        )

        def run(forward=True):
            arrived(slot, sem)
            if forward:
                for copy in copies:
                    copy.start()

        return run

    def out_chunk(zb, xb, cb, i):
        return out_all.at[zb, xb, cb, pl.ds(i * chunk, chunk)]

    def plan_out(zb, xb, i, to):
        piece = out_chunk(zb, xb, c, i)
        targets = {
            "half": (out_send.at[0], out_recv.at[i], to_half),
            "x": (out_send.at[1], out_recv.at[2], to_x),
            "far_x": (out_send.at[1], out_recv.at[3 + i], to_x),
            "core": (out_send.at[2], out_recv.at[5 + zb], to_core),
        }
        return [plan(piece, piece, targets[k][0], targets[k][1], targets[k][2]) for k in to]

    firsts = [plan_first(p) for p in range(3)]
    direct = [[plan_pass(p, dz, False) for dz in range(layers)] for p in range(3)]
    cross = [[plan_pass(p, dz, True) for dz in range(layers)] for p in range(3)]
    token_a = [plan_token(zl, k, k, True) for k in range(2)]
    token_b = [plan_token(flip(zl), k, 2 + k, False) for k in range(2)]
    out_own = [plan_out(zh, x, i, ("x", "core")) for i in range(2)]
    out_half = [plan_out(zh, x, i, ("half",))[0] for i in range(2)]

    out_near_x = [plan_out(zh, flip(x), i, ("core",)) for i in range(2)]
    out_far = [plan_out(flip(zh), x, i, ("far_x", "core")) for i in range(2)]
    out_far_x = [plan_out(flip(zh), flip(x), i, ("core",)) for i in range(2)]

    def out_from_x():
        arrived(out_all.at[zh, flip(x), c], out_recv.at[2])
        for i in range(2):
            out_near_x[i][0].start()

    def out_from_half(i):
        arrived(out_chunk(flip(zh), x, c, i), out_recv.at[i])
        for copy in out_far[i]:
            copy.start()

    def out_start():
        arrived(out_all.at[zh, x, c], load_sems.at[4])
        for pair in out_own:
            for copy in pair:
                copy.start()

    for p in range(3):
        arrived(pieces[p][1], load_sems.at[1 + p])

    @pl.when(near)
    def _():
        firsts[1][2].start()
        for p in (1, 0, 2):
            direct[p][0]()
        out_start()
        for run in token_a:
            run(False)
        for run in token_b:
            run()

    @pl.when(far)
    def _():
        firsts[1][1].start()
        firsts[1][0].start()
        out_start()
        for run in token_a:
            run()
        for i in (1, 0):
            firsts[0][i].start()
        arrived(pieces[0][1], w_send.at[0, 0])
        for i in (1, 0):
            firsts[2][i].start()
        for run in token_b:
            run()
        arrived(pieces[2][1], w_send.at[2, 0])
        for copy in out_half:
            copy.start()

    for parity in range(2):
        for c_src in range(2):
            normalize(parity, 2 * y + c_src)

    @pl.when(near)
    def _():
        firsts[0][2].start()
        firsts[2][2].start()
        direct[1][1]()
        for dz in range(2, layers):
            direct[1][dz]()
        for p in (1, 0, 2):
            cross[p][0]()

    for parity in range(2):
        for c_src in range(2):
            to_t = 2 * flip(y) + c_src
            arrived(token_slot(parity, to_t), tok_recv.at[parity, 1, c_src])
            normalize(parity, to_t)

    all_normed = normed[...]
    gate_in = dot_nt(all_normed, igate_in[...])
    gate_forget = dot_nt(all_normed, fgate_in[...])
    pick = lax.broadcasted_iota(jnp.int32, gate_in.shape, 1) == head
    pick_bias = lax.broadcasted_iota(jnp.int32, bias_in.shape, 1) == head
    bias = jnp.sum(jnp.where(pick_bias, bias_in[...], 0.0), axis=1, keepdims=True)
    forget_all = jnp.sum(jnp.where(pick, gate_forget, 0.0), axis=1, keepdims=True) + bias
    input_all = jnp.sum(jnp.where(pick, gate_in, 0.0), axis=1, keepdims=True)
    row_id = lax.broadcasted_iota(jnp.int32, (span, span), 0)
    col_id = lax.broadcasted_iota(jnp.int32, (span, span), 1)
    causal = row_id >= col_id
    eye = row_id == col_id
    gates = []
    for j in range(2):
        arrived(drift_in.at[j], drift_recv.at[j])
        offset = drift_in[j, pl.ds(head, 1), :][:, :1]
        pre = forget_all[j * span : (j + 1) * span] + offset
        in_col = input_all[j * span : (j + 1) * span]
        lf_col = jnp.minimum(pre, 0.0) - jnp.log1p(jnp.exp(-jnp.abs(pre)))
        lf_row = jnp.sum(jnp.where(eye, lf_col, 0.0), axis=0, keepdims=True)
        in_row = jnp.sum(jnp.where(eye, in_col, 0.0), axis=0, keepdims=True)
        b_col = jnp.sum(jnp.where(causal, lf_row, 0.0), axis=1, keepdims=True)
        b_row = jnp.sum(jnp.where(row_id <= col_id, lf_col, 0.0), axis=0, keepdims=True)
        total = jnp.sum(lf_col, axis=0, keepdims=True)
        write = total - b_col + in_col
        top = jnp.max(write, axis=0, keepdims=True)
        write_scale = jnp.exp(write - top)
        log_pair = jnp.where(causal, b_col - b_row + in_row, lowest_log)
        peak = jnp.max(log_pair, axis=1, keepdims=True)
        decay = jnp.where(causal, jnp.exp(log_pair - peak), 0.0)
        gates.append((b_col, total, top, write_scale, peak, decay))


    @pl.when(near)
    def _():
        for dz in range(1, layers):
            direct[0][dz]()
        for dz in range(1, layers):
            cross[1][dz]()
        for dz in range(1, layers):
            direct[2][dz]()
        for copy in out_half:
            copy.start()

    cols = (slice(0, dk), slice(dk, dk + dv), slice(dk + dv, 2 * dk + dv))

    def products(p):
        full = pieces[p][2]

        @pl.when(far)
        def _():
            arrived(full, w_recv.at[p, 0])

        flat = full[...].reshape(n * depth, full.shape[2])
        acc[:, cols[p]] = jnp.dot(normed[...], flat, preferred_element_type=f32)

    products(1)

    @pl.when(near)
    def _():
        for dz in range(1, layers):
            cross[0][dz]()

    products(0)

    spans = [4 * c + 2 * j + x for j in range(2)]
    keys = (acc[:, cols[0]] * (dk**-0.5)).astype(bf16)
    values = acc[:, cols[1]].astype(bf16)
    for j in range(2):
        b_col, total, top, write_scale, peak, decay = gates[j]
        at = slice(j * span, (j + 1) * span)
        key_scaled = keys[at].astype(f32) * write_scale
        state_all[spans[j]] = jnp.dot(
            key_scaled.T.astype(bf16), values[at], preferred_element_type=f32
        ).astype(bf16)
        mine = spans[j]
        aux_all[mine, 0:1, :] = jnp.broadcast_to(total, (1, dk))
        aux_all[mine, 1:2, :] = jnp.broadcast_to(top, (1, dk))
        aux_all[mine, 2:3, :] = jnp.sum(key_scaled, axis=0, keepdims=True)
        aux_all[mine, 3:, :] = jnp.zeros((aux_all.shape[1] - 3, dk), f32)
    late = c == 1
    early = c == 0
    for k, (to, flag) in enumerate(
        (
            (dev(z, flip(x), y, c), None),
            (dev(z, flip(x), y, flip(c)), early),
            (dev(z, x, y, flip(c)), early),
        )
    ):
        group = 0 if k == 0 else 1
        for j in range(2):
            mine = spans[j]
            send(
                aux_all.at[mine],
                aux_all.at[mine],
                aux_send.at[0],
                aux_recv.at[group],
                to,
                flag=flag,
            )
            send(
                state_all.at[mine],
                state_all.at[mine],
                state_send.at[0],
                state_recv.at[group],
                to,
                flag=flag,
            )

    @pl.when(near)
    def _():
        for dz in range(1, layers):
            cross[2][dz]()

    products(2)
    queries = acc[:, cols[2]].astype(bf16)
    intra = []
    for j in range(2):
        b_col, total, top, write_scale, peak, decay = gates[j]
        at = slice(j * span, (j + 1) * span)
        weights = dot_nt(queries[at], keys[at]) * decay
        numer = jnp.dot(weights.astype(bf16), values[at], preferred_element_type=f32)
        denom = jnp.sum(weights, axis=1, keepdims=True)
        intra.append((numer, denom))

    pl.when(near)(functools.partial(out_from_half, 0))
    arrived(aux_all.at[pl.ds(0, 2)], aux_recv.at[0])
    arrived(state_all.at[pl.ds(0, 2)], state_recv.at[0])

    @pl.when(late)
    def _():
        arrived(aux_all.at[pl.ds(0, layers)], aux_recv.at[1])
        arrived(state_all.at[pl.ds(0, layers)], state_recv.at[1])

    span_rows = aux_all[:, 0, :]
    top_rows = aux_all[:, 1, :]
    vec_rows = aux_all[:, 2, :]
    place = lax.broadcasted_iota(jnp.int32, span_rows.shape, 0)
    gain_row = head_gain_in[pl.ds(pl.multiple_of(head * dv, dv), dv)].astype(f32)[None, :]
    for j in range(2):
        b_col, total, top, write_scale, peak, decay = gates[j]
        numer, denom = intra[j]
        at = slice(j * span, (j + 1) * span)
        before = place < spans[j]
        logs = top_rows
        for m in range(1, n):
            between = (place < m) & (spans[j] > m)
            logs = logs + jnp.where(between, span_rows[m : m + 1, :], 0.0)
        logs = jnp.where(before, logs, lowest_log)
        entry = jnp.max(logs, axis=0, keepdims=True)
        weight = jnp.where(before, jnp.exp(logs - entry), 0.0)
        vec = jnp.sum(weight * vec_rows, axis=0, keepdims=True)
        mat = jnp.zeros((dk, dv), f32)
        for m in range(n - 1):
            mat = mat + weight[m : m + 1, :1] * state_all[m].astype(f32)
        carried = b_col + entry[:, :1]
        new_top = jnp.maximum(peak, carried)
        w_intra = jnp.exp(peak - new_top)
        w_carry = jnp.exp(carried - new_top)
        numer = w_intra * numer + w_carry * jnp.dot(
            queries[at], mat.astype(bf16), preferred_element_type=f32
        )
        denom = w_intra * denom + w_carry * jnp.sum(
            queries[at].astype(f32) * vec, axis=1, keepdims=True
        )
        hidden = numer / jnp.maximum(jnp.abs(denom), jnp.exp(-new_top))
        heads[j] = (
            hidden
            * lax.rsqrt(jnp.mean(hidden * hidden, axis=1, keepdims=True) + norm_floor)
            * gain_row
        ).astype(bf16)
        for d in range(2):
            send(
                heads.at[j],
                heads_in.at[z],
                heads_send.at[0],
                heads_recv.at[zh],
                dev(2 * c + d, x, y, j),
                keep=near & (zl == d) & (c == j),
            )

    out_from_x()
    pl.when(far)(functools.partial(out_from_half, 0))
    out_from_half(1)
    features = out_all.shape[3]
    home = 2 * zh + c
    wide = 2 * features

    def landing(yy, zz, zb):
        start = pl.multiple_of((zz + 2 * zb) * wide, wide)
        return out.at[yy, :, pl.ds(start, wide)]

    def out_arrived(zb):
        arrived(out_all.at[zb, :, flip(c)], out_recv.at[5 + zb])

    def heads_arrived(half):
        arrived(heads_in.at[pl.ds(2 * half, 2)], heads_recv.at[half])

    def project(zb, xb, half):
        total = jnp.zeros((span, features), f32)
        for i in range(2):
            total = total + dot_nt(
                heads_in[2 * half + i], out_all[zb, xb, half, :, i * dv : (i + 1) * dv]
            )
        return total

    def share(zb):
        for yy in range(2):
            for cc in range(2):
                send(
                    part.at[zb, pl.ds((2 * yy + cc) * rows, rows)],
                    landing(y, zl, zb),
                    final_send.at[0],
                    final_recv.at[0],
                    dev(home, x, yy, cc),
                    keep=(zl == c) & (y == yy) & (c == cc),
                )

    out_arrived(zh)
    heads_arrived(zh)
    early_part = [project(zh, xb, zh) for xb in range(2)]
    for i in range(2):
        arrived(out_chunk(flip(zh), flip(x), c, i), out_recv.at[3 + i])
        out_far_x[i][0].start()
    heads_arrived(flip(zh))
    for xb in range(2):
        total = early_part[xb] + project(zh, xb, flip(zh))
        part[zh, :, xb * features : (xb + 1) * features] = total.astype(bf16)
    share(zh)
    out_arrived(flip(zh))
    for xb in range(2):
        total = project(flip(zh), xb, zh) + project(flip(zh), xb, flip(zh))
        part[flip(zh), :, xb * features : (xb + 1) * features] = total.astype(bf16)
    share(flip(zh))
    arrived(out, final_recv.at[0])

    def drained(ref, sem, flag=None):
        if flag is None:
            arrived(ref, sem)
        else:
            pl.when(flag)(functools.partial(arrived, ref, sem))

    drained(tok_all.at[pl.ds(0, 4 * rows)], tok_send.at[0], far)
    drained(tok_all.at[pl.ds(0, 6 * rows)], tok_send.at[1], far)
    drained(tok_all.at[pl.ds(0, 3 * rows)], tok_send.at[0], near)
    drained(tok_all.at[pl.ds(0, 2 * rows)], tok_send.at[1], near)
    drained(drift_in, drift_send.at[0], near)
    for p in range(3):
        _, own, full = pieces[p]
        if p == 1:
            drained(own, w_send.at[p, 0], far)
        drained(own.at[0], w_send.at[p, 0], near)
        drained(full.at[pl.ds(0, layers)], w_send.at[p, 1], near)
        drained(full, w_send.at[p, 2], near)
    drained(out_all.at[0, 0, 0], out_send.at[0])
    drained(out_all.at[0, 0], out_send.at[1])
    drained(out_all.at[0], out_send.at[2])
    for ref, sem in ((state_all, state_send.at[0]), (aux_all, aux_send.at[0])):
        drained(ref.at[pl.ds(0, 6)], sem, early)
        drained(ref.at[pl.ds(0, 2)], sem, late)
    drained(heads_in.at[pl.ds(0, 3)], heads_send.at[0], near)
    drained(heads_in, heads_send.at[0], far)
    at_home = zl == c
    drained(part, final_send.at[0], jnp.logical_not(at_home))
    drained(part.at[:, pl.ds(0, 3 * rows)], final_send.at[0], at_home)


def on_device_layers(
    n,
    tp,
    tokens,
    pre_gain,
    w_query,
    w_key,
    w_value,
    w_igate,
    w_fgate,
    forget_bias,
    gate_drift,
    head_gain,
    w_out,
):
    heads = w_igate.shape[1]
    rows, width = tokens.shape
    span = rows * tp
    if (
        heads != 2 * tp
        or n != heads
        or gate_drift.shape[0] != span
        or span > drift_span
    ):
        return on_device(
            tokens,
            pre_gain,
            w_query,
            w_key,
            w_value,
            w_igate,
            w_fgate,
            forget_bias,
            gate_drift,
            head_gain,
            w_out,
        )
    layers = n // 2
    depth = w_query.shape[0]
    dk = w_query.shape[1] // 2
    dv = w_value.shape[1] // 2
    features = w_out.shape[0]
    anywhere = pl.BlockSpec(memory_space=pl.ANY)
    dma = pltpu.SemaphoreType.DMA
    vmem = pltpu.VMEM
    parts = pl.pallas_call(
        functools.partial(layer_kernel, n, tp),
        out_shape=pltpu.VMEM((2, rows, features * n), bf16),
        in_specs=[anywhere] * 11,
        out_specs=anywhere,
        scratch_shapes=[
            vmem((rows, width), bf16),
            vmem((2 * span, width), bf16),
            vmem((2 * span, width), bf16),
            vmem((width,), bf16),
            vmem((heads, width), bf16),
            vmem((heads, width), bf16),
            vmem((1, heads), f32),
            vmem((heads * dv,), bf16),
            vmem((3, heads, span), f32),
            vmem((2, depth, dk), bf16),
            vmem((2, depth, dv), bf16),
            vmem((2, depth, dk), bf16),
            vmem((n, depth, dk), bf16),
            vmem((n, depth, dv), bf16),
            vmem((n, depth, dk), bf16),
            vmem((2, 2, 2, features, 2 * dv), bf16),
            vmem((2 * span, 2 * dk + dv), f32),
            vmem((n, dk, dv), bf16),
            vmem((n, 8, dk), f32),
            vmem((2, span, dv), bf16),
            vmem((layers, span, dv), bf16),
            vmem((2, span, 2 * features), bf16),
            dma((11,)),
            dma((2,)),
            dma((2, 2, 2)),
            dma((1,)),
            dma((2,)),
            dma((3, 3)),
            dma((3, n)),
            dma((3,)),
            dma((7,)),
            dma((1,)),
            dma((2,)),
            dma((1,)),
            dma((2,)),
            dma((1,)),
            dma((2,)),
            dma((1,)),
            dma((1,)),
        ],
        compiler_params=pltpu.CompilerParams(collective_id=0, has_side_effects=True),
    )(
        tokens,
        pre_gain,
        w_key,
        w_value,
        w_query,
        w_igate.T,
        w_fgate.T,
        forget_bias[None, :],
        gate_drift.T,
        head_gain,
        w_out,
    )
    return jnp.sum(parts.astype(f32), axis=0).astype(bf16)


def solution(mesh):
    in_specs = (
        P(("sp", "tp"), None),
        P(),
        P("sp", "tp"),
        P("sp", "tp"),
        P("sp", "tp"),
        P(),
        P(),
        P(),
        P("sp", None),
        P(),
        P("sp", "tp"),
    )
    out_specs = P(("sp", "tp"), None)
    body = on_device
    if mesh.shape["sp"] == 2 * mesh.shape["tp"] and mesh.shape["tp"] == 4:
        body = functools.partial(on_device_layers, mesh.shape["sp"], mesh.shape["tp"])
    return jax.shard_map(
        body, mesh=mesh, in_specs=in_specs, out_specs=out_specs, check_vma=False
    )
```

```python
import functools

import jax
import jax.numpy as jnp
from jax import lax
from jax.experimental import pallas as pl
from jax.experimental.pallas import tpu as pltpu
from jax.sharding import PartitionSpec as P

BLOCK = 64


norm_floor = 0.1
lowest_log = -1e30
highest = lax.Precision.HIGHEST


def prefix(value, axis, combine, identity):
    peers, position = (lax.axis_size(axis), lax.axis_index(axis))
    everything = jax.tree.map(
        lambda part, kind: lax.all_gather(part.astype(kind), axis),
        value,
        jax.tree.map(lambda a: jnp.bfloat16 if a.dtype == jnp.float32 else a.dtype, value),
    )
    start = jax.tree.map(
        lambda part, zero: jnp.broadcast_to(jnp.asarray(zero, part.dtype), part.shape),
        value,
        identity,
    )

    def step(k, before):
        reached = k < position
        new = combine(
            before, jax.tree.map(lambda part, own: part[k].astype(own.dtype), everything, value)
        )
        return jax.tree.map(lambda a, b: jnp.where(reached, a, b), new, before)

    return lax.fori_loop(0, peers, step, start)


def advance(memory, summary):
    old_mat, old_vec, old_top = memory
    span_log, span_top, span_mat, span_vec = summary
    new_top = jnp.maximum(span_log + old_top, span_top)
    kept_part = jnp.exp(span_log + old_top - new_top)
    fresh_part = jnp.exp(span_top - new_top)
    return (
        kept_part[:, None, None] * old_mat + fresh_part[:, None, None] * span_mat,
        kept_part[:, None] * old_vec + fresh_part[:, None] * span_vec,
        new_top,
    )


def prefix_states(initial, summary):

    def stepper(memory, one_block):
        return (advance(memory, one_block), memory)

    return lax.scan(stepper, initial, summary)


def join_devices(earlier, later_part):
    early_log, early_mat, early_vec, early_top = earlier
    late_log, late_mat, late_vec, late_top = later_part
    new_top = jnp.maximum(late_log + early_top, late_top)
    kept_part = jnp.exp(late_log + early_top - new_top)
    fresh_part = jnp.exp(late_top - new_top)
    return (
        early_log + late_log,
        kept_part[:, None, None] * early_mat + fresh_part[:, None, None] * late_mat,
        kept_part[:, None] * early_vec + fresh_part[:, None] * late_vec,
        new_top,
    )


def blend_parts(first_part, second_part):
    numer_first, denom_first, peak_first = first_part
    numer_second, denom_second, peak_second = second_part
    new_top = jnp.maximum(peak_first, peak_second)
    weight_first = jnp.exp(peak_first - new_top)
    weight_second = jnp.exp(peak_second - new_top)
    return (
        weight_first[..., None] * numer_first + weight_second[..., None] * numer_second,
        weight_first * denom_first + weight_second * denom_second,
        new_top,
    )


def on_device(
    tokens,
    pre_gain,
    w_query,
    w_key,
    w_value,
    w_igate,
    w_fgate,
    forget_bias,
    gate_drift,
    head_gain,
    w_out,
):
    tp_size = lax.axis_size("tp")
    head_count = w_igate.shape[1]
    local_heads = head_count // tp_size
    first_head = lax.axis_index("tp") * local_heads
    key_width = w_query.shape[1] // local_heads
    value_width = w_value.shape[1] // local_heads
    token_wide = tokens.astype(jnp.float32)
    scaled = token_wide * lax.rsqrt(
        jnp.mean(token_wide * token_wide, axis=1, keepdims=True) + norm_floor
    )
    normed = (scaled * pre_gain.astype(jnp.float32)).astype(jnp.bfloat16)
    gate_cols = jnp.concatenate(
        [
            lax.dynamic_slice_in_dim(w_igate, first_head, local_heads, 1),
            lax.dynamic_slice_in_dim(w_fgate, first_head, local_heads, 1),
        ],
        axis=1,
    )
    key_scale = key_width ** (-0.5)
    wq_full, wk_full, wv_full = (
        lax.all_gather(w_query, "sp", axis=0, tiled=True),
        lax.all_gather(w_key, "sp", axis=0, tiled=True),
        lax.all_gather(w_value, "sp", axis=0, tiled=True),
    )
    row_piece = lax.all_gather(normed, "tp", axis=0, tiled=True)
    queries_part = jnp.dot(row_piece, wq_full, preferred_element_type=jnp.float32).astype(
        jnp.bfloat16
    )
    keys_part = (
        jnp.dot(row_piece, wk_full, preferred_element_type=jnp.float32) * key_scale
    ).astype(jnp.bfloat16)
    values_part = jnp.dot(row_piece, wv_full, preferred_element_type=jnp.float32).astype(
        jnp.bfloat16
    )
    gate_part = jnp.dot(row_piece, gate_cols, preferred_element_type=jnp.float32)
    group_len = queries_part.shape[0]
    blocks = group_len // BLOCK
    log_input = gate_part[:, :local_heads]
    forget_pre = gate_part[:, local_heads:] + lax.dynamic_slice_in_dim(
        forget_bias, first_head, local_heads, 0
    )
    log_forget = jax.nn.log_sigmoid(
        forget_pre + lax.dynamic_slice_in_dim(gate_drift, first_head, local_heads, 1)
    )
    query_blk = queries_part.reshape(blocks, BLOCK, local_heads, key_width)
    key_blk = keys_part.reshape(blocks, BLOCK, local_heads, key_width)
    value_blk = values_part.reshape(blocks, BLOCK, local_heads, value_width)
    input_blk = log_input.reshape(blocks, BLOCK, local_heads).transpose(0, 2, 1)
    forget_blk = log_forget.reshape(blocks, BLOCK, local_heads).transpose(0, 2, 1)
    within = jnp.cumsum(forget_blk, axis=2)
    causal = jnp.arange(BLOCK)[:, None] >= jnp.arange(BLOCK)[None, :]
    log_pair = jnp.where(
        causal, within[..., :, None] - within[..., None, :] + input_blk[..., None, :], -jnp.inf
    )
    peak_intra = jnp.max(log_pair, axis=3)
    scores = jnp.einsum("nshd,nrhd->nhsr", query_blk, key_blk, preferred_element_type=jnp.float32)
    weights = scores * jnp.exp(log_pair - peak_intra[..., None])
    numer_intra = jnp.einsum(
        "nhsr,nrhv->nhsv",
        weights.astype(jnp.bfloat16),
        value_blk,
        preferred_element_type=jnp.float32,
    )
    denom_intra = jnp.sum(weights, axis=3)
    span_log = within[..., -1]
    log_write = span_log[..., None] - within + input_blk
    span_top = jnp.max(log_write, axis=2)
    write_scale = jnp.exp(log_write - span_top[..., None])
    key_scaled = key_blk.astype(jnp.float32) * write_scale.transpose(0, 2, 1)[..., None]
    value_wide = value_blk.astype(jnp.float32)
    span_mat = jnp.einsum("nrhv,nrhd->nhvd", value_wide, key_scaled, precision=highest)
    span_vec = jnp.sum(key_scaled, axis=1)
    summary = (span_log, span_top, span_mat, span_vec)
    empty_state = (
        jnp.zeros((local_heads, value_width, key_width), jnp.float32),
        jnp.zeros((local_heads, key_width), jnp.float32),
        jnp.full((local_heads,), lowest_log, jnp.float32),
    )
    local_end, local_starts = prefix_states(empty_state, summary)
    device_summary = (jnp.sum(span_log, axis=0),) + local_end
    identity_all = (jnp.zeros((local_heads,), jnp.float32),) + empty_state
    incoming = prefix(device_summary, "sp", join_devices, identity_all)
    query_wide = query_blk.astype(jnp.float32)
    intra_part = (numer_intra, denom_intra, peak_intra)
    start_mat, start_vec, start_top = local_starts
    local_part = (
        jnp.einsum("nhvd,nshd->nhsv", start_mat, query_wide, precision=highest),
        jnp.einsum("nhd,nshd->nhs", start_vec, query_wide, precision=highest),
        within + start_top[..., None],
    )
    numerator, denominator, peak_log = blend_parts(local_part, intra_part)
    entry_log, entry_mat, entry_vec, entry_top = incoming
    before_log = jnp.concatenate(
        [jnp.zeros((1, local_heads), jnp.float32), jnp.cumsum(span_log, axis=0)[:-1]], axis=0
    )
    from_left = (
        jnp.einsum("hvd,nshd->nhsv", entry_mat, query_wide, precision=highest),
        jnp.einsum("hd,nshd->nhs", entry_vec, query_wide, precision=highest),
        within + (before_log + entry_top[None, :])[..., None],
    )
    numerator, denominator, peak_log = blend_parts((numerator, denominator, peak_log), from_left)
    hidden = numerator / jnp.maximum(jnp.abs(denominator), jnp.exp(-peak_log))[..., None]
    hidden = hidden.transpose(0, 2, 1, 3).reshape(group_len, local_heads, value_width)
    head_gains = lax.dynamic_slice_in_dim(
        head_gain, first_head * value_width, local_heads * value_width, 0
    )
    head_gains = head_gains.astype(jnp.float32).reshape(local_heads, value_width)
    normed_heads = (
        hidden
        * lax.rsqrt(jnp.mean(hidden * hidden, axis=2, keepdims=True) + norm_floor)
        * head_gains
    )
    normed_heads = normed_heads.astype(jnp.bfloat16).reshape(group_len, local_heads * value_width)
    out_slab = lax.all_gather(w_out, "sp", axis=0, tiled=True)
    return lax.psum_scatter(
        lax.dot_general(
            normed_heads, out_slab, (((1,), (1,)), ((), ())), preferred_element_type=jnp.float32
        ).astype(jnp.bfloat16),
        "tp",
        scatter_dimension=0,
        tiled=True,
    )


drift_span = 128
MESH = pl.DeviceIdType.MESH
f32 = jnp.float32
bf16 = jnp.bfloat16


def dot_nt(a, b):
    return lax.dot_general(a, b, (((1,), (1,)), ((), ())), preferred_element_type=f32)


def layer_kernel(
    n,
    tp,
    tokens,
    pre_gain,
    w_key,
    w_value,
    w_query,
    w_igate,
    w_fgate,
    forget_bias,
    drift,
    head_gain,
    w_out,
    out,
    tok_own,
    tok_all,
    normed,
    gain_in,
    igate_in,
    fgate_in,
    bias_in,
    head_gain_in,
    drift_in,
    key_own,
    value_own,
    query_own,
    key_all,
    value_all,
    query_all,
    out_all,
    acc,
    state_all,
    aux_all,
    heads,
    heads_in,
    part,
    load_sems,
    tok_send,
    tok_recv,
    drift_send,
    drift_recv,
    w_send,
    w_recv,
    out_send,
    out_recv,
    state_send,
    state_recv,
    aux_send,
    aux_recv,
    heads_send,
    heads_recv,
    final_send,
    final_recv,
):
    s = lax.axis_index("sp")
    t = lax.axis_index("tp")
    layers = n // 2
    z = s // 2
    x = s % 2
    y = t // 2
    c = t % 2
    zh = z // 2
    zl = z % 2
    near = zh == c
    far = jnp.logical_not(near)
    head = layers * y + z
    rows = tok_own.shape[0]
    span = rows * tp
    length = 2 * span
    depth = key_own.shape[1]
    dk = key_own.shape[2]
    dv = value_own.shape[2]

    def flip(value):
        return 1 - value

    def at_layer(dz):
        if dz == 0:
            return z
        if dz == 1:
            return 2 * zh + flip(zl)
        if dz == 2:
            return 2 * flip(zh) + zl
        return 2 * flip(zh) + flip(zl)

    def dev(zz, xx, yy, cc):
        return 2 * zz + xx, 2 * yy + cc

    barrier = pltpu.get_barrier_semaphore()
    to_sibling = dev(z, x, y, flip(c))
    partners = [dev(z, flip(x), y, cc) for cc in range(2)]
    for dz in range(layers):
        for yy in (y, flip(y)) if dz < 2 else (y,):
            partners += [dev(at_layer(dz), x, yy, cc) for cc in range(2)]
    partners[2:4] = [to_sibling]
    for ss, tt in partners:
        pl.semaphore_signal(
            barrier,
            inc=1,
            device_id={"sp": ss, "tp": tt},
            device_id_type=MESH,
        )

    def load(source, target, sem):
        copy = pltpu.make_async_copy(source, target, sem)
        copy.start()
        return copy

    pieces = (
        (w_key, key_own, key_all),
        (w_value, value_own, value_all),
        (w_query, query_own, query_all),
    )

    def token_slot(parity, to_t):
        start = pl.multiple_of((parity * tp + to_t) * rows, rows)
        return tok_all.at[pl.ds(start, rows)]

    own_slot = token_slot(zl, t)
    load_tokens = load(tokens, tok_own, load_sems.at[0])
    loads_own = []
    for p, (w_hbm, own, full) in enumerate(pieces):
        width = own.shape[2]
        loads_own.append(
            [
                load(
                    w_hbm.at[:, pl.ds(j * width, width)],
                    own.at[j],
                    load_sems.at[1 + p],
                )
                for j in range(2)
            ]
        )
    chunk = out_all.shape[3] // 2
    loads_out = [
        load(
            w_out.at[pl.ds(i * chunk, chunk)],
            out_all.at[zh, x, c, pl.ds(i * chunk, chunk)],
            load_sems.at[4],
        )
        for i in range(2)
    ]
    small = (
        (pre_gain, gain_in),
        (w_igate, igate_in),
        (w_fgate, fgate_in),
        (forget_bias, bias_in),
        (head_gain, head_gain_in),
    )
    loads_small = [load(a, b, load_sems.at[5 + i]) for i, (a, b) in enumerate(small)]

    @pl.when(near)
    def _():
        pltpu.make_async_copy(tokens, own_slot, tok_recv.at[zl, 0, c]).start()
        pltpu.make_async_copy(drift, drift_in.at[zl], drift_recv.at[zl]).start()
        for p, (w_hbm, own, full) in enumerate(pieces):
            width = own.shape[2]
            for j in range(2):

                @pl.when(zl == j)
                def _():
                    pltpu.make_async_copy(
                        w_hbm.at[:, pl.ds(j * width, width)], full.at[s], w_recv.at[p, s]
                    ).start()

    load_drift = load(drift, drift_in.at[2], load_sems.at[10])

    @pl.when(c == 0)
    def _():
        state_all[layers:, :, :] = jnp.zeros((layers, dk, dv), bf16)
        aux_all[layers:, :, :] = jnp.zeros((layers, aux_all.shape[1], dk), f32)

    pl.semaphore_wait(barrier, len(partners))

    def plan(source, target, send_sem, recv_sem, to, flag=None):
        copy = pltpu.make_async_remote_copy(
            src_ref=source,
            dst_ref=target,
            send_sem=send_sem,
            recv_sem=recv_sem,
            device_id={"sp": to[0], "tp": to[1]},
            device_id_type=MESH,
        )
        return copy

    def send(source, target, send_sem, recv_sem, to, flag=None, keep=None):
        if keep is not None:

            @pl.when(keep)
            def _():
                pltpu.make_async_copy(source, target, recv_sem).start()

            flag = jnp.logical_not(keep)
        copy = plan(source, target, send_sem, recv_sem, to, flag)
        if flag is None:
            copy.start()
        else:
            pl.when(flag)(copy.start)

    def arrived(target, sem):
        pltpu.make_async_copy(target, target, sem).wait()

    load_tokens.wait()
    mine = tok_recv.at[zl, 0, c]
    send(tok_own, own_slot, tok_send.at[0], mine, dev(at_layer(2), x, y, zh))
    send(tok_own, own_slot, tok_send.at[0], mine, dev(at_layer(1), x, y, zh))
    send(
        tok_own, own_slot, tok_send.at[0], tok_recv.at[zl, 1, c], dev(z, x, flip(y), zh)
    )
    send(tok_own, own_slot, tok_send.at[0], mine, dev(z, x, y, flip(c)), flag=far)
    load_drift.wait()
    for i in range(1, 4):
        send(
            drift_in.at[2],
            drift_in.at[zl],
            drift_send.at[0],
            drift_recv.at[zl],
            dev(at_layer(i), x, y, c),
            flag=near,
        )

    for copy in loads_small:
        copy.wait()
    gain = gain_in[...].astype(f32)[None, :]

    def normalize(parity, to_t):
        start = pl.multiple_of((parity * tp + to_t) * rows, rows)
        wide = tok_all[pl.ds(start, rows), :].astype(f32)
        scale = lax.rsqrt(jnp.mean(wide * wide, axis=1, keepdims=True) + norm_floor)
        normed[pl.ds(start, rows), :] = (wide * scale * gain).astype(bf16)

    to_x = dev(z, flip(x), y, c)
    to_core = dev(z, x, y, flip(c))
    to_half = dev(at_layer(2), x, y, c)

    def plan_first(p):
        _, own, full = pieces[p]
        sem = w_recv.at[p, s]
        middle = dev(1 + c * (layers - 3), x, y, c)
        end = dev(c * (layers - 1), x, y, c)
        beside = dev(at_layer(1), x, y, c)
        target = full.at[s]
        return (
            plan(own.at[flip(c)], target, w_send.at[p, 0], sem, middle, far),
            plan(own.at[c], target, w_send.at[p, 0], sem, end, far),
            plan(own.at[flip(zl)], target, w_send.at[p, 0], sem, beside, near),
        )

    def plan_pass(p, dz, across):
        block = 2 * at_layer(dz) + (flip(x) if across else x)
        full = pieces[p][2].at[block]
        sem = w_recv.at[p, block]
        to_far = w_recv.at[p, 0]
        onward = [plan(full, full, w_send.at[p, 2], to_far, to_core, near)]
        if not across:
            onward.insert(0, plan(full, full, w_send.at[p, 1], sem, to_x, near))

        def run():
            arrived(full, sem)
            for copy in onward:
                copy.start()

        return run

    def plan_token(parity, c_src, i, onward):
        slot = token_slot(parity, 2 * y + c_src)
        sem = tok_recv.at[parity, 0, c_src]
        out_sem = tok_recv.at[parity, 1, c_src]
        to_y = dev(z, x, flip(y), c)
        copies = []
        if onward:
            copies.append(
                plan(slot, slot, tok_send.at[1], sem, dev(at_layer(1), x, y, c), far)
            )
        copies.append(
            plan(slot, slot, tok_send.at[1], out_sem, to_y, far if onward else None)
        )

        def run(forward=True):
            arrived(slot, sem)
            if forward:
                for copy in copies:
                    copy.start()

        return run

    def out_chunk(zb, xb, cb, i):
        return out_all.at[zb, xb, cb, pl.ds(i * chunk, chunk)]

    def plan_out(zb, xb, i, to):
        piece = out_chunk(zb, xb, c, i)
        targets = {
            "half": (out_send.at[0], out_recv.at[i], to_half),
            "x": (out_send.at[1], out_recv.at[2], to_x),
            "far_x": (out_send.at[1], out_recv.at[3 + i], to_x),
            "core": (out_send.at[2], out_recv.at[5 + 2 * zb + xb], to_core),
        }
        return [plan(piece, piece, targets[k][0], targets[k][1], targets[k][2]) for k in to]

    firsts = [plan_first(p) for p in range(3)]
    direct = [[plan_pass(p, dz, False) for dz in range(layers)] for p in range(3)]
    cross = [[plan_pass(p, dz, True) for dz in range(layers)] for p in range(3)]
    token_a = [plan_token(zl, k, k, True) for k in range(2)]
    token_b = [plan_token(flip(zl), k, 2 + k, False) for k in range(2)]
    out_own = [plan_out(zh, x, i, ("x", "core")) for i in range(2)]
    out_half = [plan_out(zh, x, i, ("half",))[0] for i in range(2)]

    out_near_x = [plan_out(zh, flip(x), i, ("core",)) for i in range(2)]
    out_far = [plan_out(flip(zh), x, i, ("far_x", "core")) for i in range(2)]
    out_far_x = [plan_out(flip(zh), flip(x), i, ("core",)) for i in range(2)]

    def out_from_x():
        arrived(out_all.at[zh, flip(x), c], out_recv.at[2])
        for i in range(2):
            out_near_x[i][0].start()

    def out_from_half(i):
        arrived(out_chunk(flip(zh), x, c, i), out_recv.at[i])
        for copy in out_far[i]:
            copy.start()

    def out_start():
        arrived(out_all.at[zh, x, c], load_sems.at[4])
        for pair in out_own:
            for copy in pair:
                copy.start()

    for p in range(3):
        arrived(pieces[p][1], load_sems.at[1 + p])

    @pl.when(near)
    def _():
        firsts[1][2].start()
        for p in (1, 0, 2):
            direct[p][0]()
        out_start()
        for run in token_a:
            run(False)
        for run in token_b:
            run()

    @pl.when(far)
    def _():
        firsts[1][1].start()
        firsts[1][0].start()
        firsts[0][1].start()
        firsts[0][0].start()
        out_start()
        for run in token_a:
            run()
        for i in (1, 0):
            firsts[2][i].start()
        for run in token_b:
            run()
        arrived(pieces[0][1], w_send.at[0, 0])
        arrived(pieces[2][1], w_send.at[2, 0])
        for copy in out_half:
            copy.start()

    for parity in range(2):
        for c_src in range(2):
            normalize(parity, 2 * y + c_src)

    @pl.when(near)
    def _():
        firsts[0][2].start()
        firsts[2][2].start()
        direct[1][1]()
        for dz in range(2, layers):
            direct[1][dz]()
        for p in (1, 0, 2):
            cross[p][0]()

    for parity in range(2):
        for c_src in range(2):
            to_t = 2 * flip(y) + c_src
            arrived(token_slot(parity, to_t), tok_recv.at[parity, 1, c_src])
            normalize(parity, to_t)

    all_normed = normed[...]
    gate_in = dot_nt(all_normed, igate_in[...])
    gate_forget = dot_nt(all_normed, fgate_in[...])
    pick = lax.broadcasted_iota(jnp.int32, gate_in.shape, 1) == head
    pick_bias = lax.broadcasted_iota(jnp.int32, bias_in.shape, 1) == head
    bias = jnp.sum(jnp.where(pick_bias, bias_in[...], 0.0), axis=1, keepdims=True)
    forget_all = jnp.sum(jnp.where(pick, gate_forget, 0.0), axis=1, keepdims=True) + bias
    input_all = jnp.sum(jnp.where(pick, gate_in, 0.0), axis=1, keepdims=True)
    row_id = lax.broadcasted_iota(jnp.int32, (span, span), 0)
    col_id = lax.broadcasted_iota(jnp.int32, (span, span), 1)
    causal = row_id >= col_id
    eye = row_id == col_id
    gates = []
    for j in range(2):
        arrived(drift_in.at[j], drift_recv.at[j])
        offset = drift_in[j, pl.ds(head, 1), :][:, :1]
        pre = forget_all[j * span : (j + 1) * span] + offset
        in_col = input_all[j * span : (j + 1) * span]
        lf_col = jnp.minimum(pre, 0.0) - jnp.log1p(jnp.exp(-jnp.abs(pre)))
        lf_row = jnp.sum(jnp.where(eye, lf_col, 0.0), axis=0, keepdims=True)
        in_row = jnp.sum(jnp.where(eye, in_col, 0.0), axis=0, keepdims=True)
        b_col = jnp.sum(jnp.where(causal, lf_row, 0.0), axis=1, keepdims=True)
        b_row = jnp.sum(jnp.where(row_id <= col_id, lf_col, 0.0), axis=0, keepdims=True)
        total = jnp.sum(lf_col, axis=0, keepdims=True)
        write = total - b_col + in_col
        top = jnp.max(write, axis=0, keepdims=True)
        write_scale = jnp.exp(write - top)
        log_pair = jnp.where(causal, b_col - b_row + in_row, lowest_log)
        peak = jnp.max(log_pair, axis=1, keepdims=True)
        decay = jnp.where(causal, jnp.exp(log_pair - peak), 0.0)
        gates.append((b_col, total, top, write_scale, peak, decay))


    @pl.when(near)
    def _():
        for dz in range(1, layers):
            direct[0][dz]()
        for dz in range(1, layers):
            cross[1][dz]()
        for dz in range(1, layers):
            direct[2][dz]()
        for copy in out_half:
            copy.start()

    cols = (slice(0, dk), slice(dk, dk + dv), slice(dk + dv, 2 * dk + dv))

    def products(p):
        full = pieces[p][2]

        @pl.when(far)
        def _():
            arrived(full, w_recv.at[p, 0])

        flat = full[...].reshape(n * depth, full.shape[2])
        acc[:, cols[p]] = jnp.dot(normed[...], flat, preferred_element_type=f32)

    products(1)

    @pl.when(near)
    def _():
        for dz in range(1, layers):
            cross[0][dz]()

    products(0)

    spans = [4 * c + 2 * j + x for j in range(2)]
    keys = (acc[:, cols[0]] * (dk**-0.5)).astype(bf16)
    values = acc[:, cols[1]].astype(bf16)
    for j in range(2):
        b_col, total, top, write_scale, peak, decay = gates[j]
        at = slice(j * span, (j + 1) * span)
        key_scaled = keys[at].astype(f32) * write_scale
        state_all[spans[j]] = jnp.dot(
            key_scaled.T.astype(bf16), values[at], preferred_element_type=f32
        ).astype(bf16)
        mine = spans[j]
        aux_all[mine, 0:1, :] = jnp.broadcast_to(total, (1, dk))
        aux_all[mine, 1:2, :] = jnp.broadcast_to(top, (1, dk))
        aux_all[mine, 2:3, :] = jnp.sum(key_scaled, axis=0, keepdims=True)
        aux_all[mine, 3:, :] = jnp.zeros((aux_all.shape[1] - 3, dk), f32)
    late = c == 1
    early = c == 0
    for k, (to, flag) in enumerate(
        (
            (dev(z, flip(x), y, c), None),
            (dev(z, flip(x), y, flip(c)), early),
            (dev(z, x, y, flip(c)), early),
        )
    ):
        group = 0 if k == 0 else 1
        for j in range(2):
            mine = spans[j]
            send(
                aux_all.at[mine],
                aux_all.at[mine],
                aux_send.at[0],
                aux_recv.at[group],
                to,
                flag=flag,
            )
            send(
                state_all.at[mine],
                state_all.at[mine],
                state_send.at[0],
                state_recv.at[group],
                to,
                flag=flag,
            )

    @pl.when(near)
    def _():
        for dz in range(1, layers):
            cross[2][dz]()

    products(2)
    queries = acc[:, cols[2]].astype(bf16)
    intra = []
    for j in range(2):
        b_col, total, top, write_scale, peak, decay = gates[j]
        at = slice(j * span, (j + 1) * span)
        weights = dot_nt(queries[at], keys[at]) * decay
        numer = jnp.dot(weights.astype(bf16), values[at], preferred_element_type=f32)
        denom = jnp.sum(weights, axis=1, keepdims=True)
        intra.append((numer, denom))

    pl.when(near)(functools.partial(out_from_half, 0))
    arrived(aux_all.at[pl.ds(0, 2)], aux_recv.at[0])
    arrived(state_all.at[pl.ds(0, 2)], state_recv.at[0])

    @pl.when(late)
    def _():
        arrived(aux_all.at[pl.ds(0, layers)], aux_recv.at[1])
        arrived(state_all.at[pl.ds(0, layers)], state_recv.at[1])

    span_rows = aux_all[:, 0, :]
    top_rows = aux_all[:, 1, :]
    vec_rows = aux_all[:, 2, :]
    place = lax.broadcasted_iota(jnp.int32, span_rows.shape, 0)
    gain_row = head_gain_in[pl.ds(pl.multiple_of(head * dv, dv), dv)].astype(f32)[None, :]
    for j in range(2):
        b_col, total, top, write_scale, peak, decay = gates[j]
        numer, denom = intra[j]
        at = slice(j * span, (j + 1) * span)
        before = place < spans[j]
        logs = top_rows
        for m in range(1, n):
            between = (place < m) & (spans[j] > m)
            logs = logs + jnp.where(between, span_rows[m : m + 1, :], 0.0)
        logs = jnp.where(before, logs, lowest_log)
        entry = jnp.max(logs, axis=0, keepdims=True)
        weight = jnp.where(before, jnp.exp(logs - entry), 0.0)
        vec = jnp.sum(weight * vec_rows, axis=0, keepdims=True)
        mat = jnp.zeros((dk, dv), f32)
        for m in range(n - 1):
            mat = mat + weight[m : m + 1, :1] * state_all[m].astype(f32)
        carried = b_col + entry[:, :1]
        new_top = jnp.maximum(peak, carried)
        w_intra = jnp.exp(peak - new_top)
        w_carry = jnp.exp(carried - new_top)
        numer = w_intra * numer + w_carry * jnp.dot(
            queries[at], mat.astype(bf16), preferred_element_type=f32
        )
        denom = w_intra * denom + w_carry * jnp.sum(
            queries[at].astype(f32) * vec, axis=1, keepdims=True
        )
        hidden = numer / jnp.maximum(jnp.abs(denom), jnp.exp(-new_top))
        heads[j] = (
            hidden
            * lax.rsqrt(jnp.mean(hidden * hidden, axis=1, keepdims=True) + norm_floor)
            * gain_row
        ).astype(bf16)
        for d in range(2):
            send(
                heads.at[j],
                heads_in.at[z],
                heads_send.at[0],
                heads_recv.at[zh],
                dev(2 * c + d, x, y, j),
                keep=near & (zl == d) & (c == j),
            )

    out_from_x()
    pl.when(far)(functools.partial(out_from_half, 0))
    out_from_half(1)
    features = out_all.shape[3]
    home = 2 * zh + c
    wide = 2 * features

    def landing(yy, zz, zb, xb):
        start = pl.multiple_of((zz + 2 * zb) * wide + xb * features, features)
        return out.at[yy, :, pl.ds(start, features)]

    def out_arrived(zb, xb):
        arrived(out_all.at[zb, xb, flip(c)], out_recv.at[5 + 2 * zb + xb])

    def heads_arrived(half):
        arrived(heads_in.at[pl.ds(2 * half, 2)], heads_recv.at[half])

    def project(zb, xb, half):
        total = jnp.zeros((span, features), f32)
        for i in range(2):
            total = total + dot_nt(
                heads_in[2 * half + i], out_all[zb, xb, half, :, i * dv : (i + 1) * dv]
            )
        return total

    def share(zb, xb, total):
        part[zb, xb] = total.astype(bf16)
        for yy in range(2):
            for cc in range(2):
                send(
                    part.at[zb, xb, pl.ds((2 * yy + cc) * rows, rows)],
                    landing(y, zl, zb, xb),
                    final_send.at[0],
                    final_recv.at[0],
                    dev(home, x, yy, cc),
                    keep=(zl == c) & (y == yy) & (c == cc),
                )

    sides = (x, flip(x))
    for xb in sides:
        out_arrived(zh, xb)
    heads_arrived(zh)
    early_part = [project(zh, xb, zh) for xb in sides]
    for i in range(2):
        arrived(out_chunk(flip(zh), flip(x), c, i), out_recv.at[3 + i])
        out_far_x[i][0].start()
    heads_arrived(flip(zh))
    for k, xb in enumerate(sides):
        share(zh, xb, early_part[k] + project(zh, xb, flip(zh)))
    for xb in sides:
        out_arrived(flip(zh), xb)
        share(flip(zh), xb, project(flip(zh), xb, zh) + project(flip(zh), xb, flip(zh)))
    arrived(out, final_recv.at[0])

    def drained(ref, sem, flag=None):
        if flag is None:
            arrived(ref, sem)
        else:
            pl.when(flag)(functools.partial(arrived, ref, sem))

    drained(tok_all.at[pl.ds(0, 4 * rows)], tok_send.at[0], far)
    drained(tok_all.at[pl.ds(0, 6 * rows)], tok_send.at[1], far)
    drained(tok_all.at[pl.ds(0, 3 * rows)], tok_send.at[0], near)
    drained(tok_all.at[pl.ds(0, 2 * rows)], tok_send.at[1], near)
    drained(drift_in, drift_send.at[0], near)
    for p in range(3):
        _, own, full = pieces[p]
        if p == 1:
            drained(own, w_send.at[p, 0], far)
        drained(own.at[0], w_send.at[p, 0], near)
        drained(full.at[pl.ds(0, layers)], w_send.at[p, 1], near)
        drained(full, w_send.at[p, 2], near)
    drained(out_all.at[0, 0, 0], out_send.at[0])
    drained(out_all.at[0, 0], out_send.at[1])
    drained(out_all.at[0], out_send.at[2])
    for ref, sem in ((state_all, state_send.at[0]), (aux_all, aux_send.at[0])):
        drained(ref.at[pl.ds(0, 6)], sem, early)
        drained(ref.at[pl.ds(0, 2)], sem, late)
    drained(heads_in.at[pl.ds(0, 3)], heads_send.at[0], near)
    drained(heads_in, heads_send.at[0], far)
    at_home = zl == c
    drained(part, final_send.at[0], jnp.logical_not(at_home))
    drained(part.at[:, :, pl.ds(0, 3 * rows)], final_send.at[0], at_home)


def on_device_layers(
    n,
    tp,
    tokens,
    pre_gain,
    w_query,
    w_key,
    w_value,
    w_igate,
    w_fgate,
    forget_bias,
    gate_drift,
    head_gain,
    w_out,
):
    heads = w_igate.shape[1]
    rows, width = tokens.shape
    span = rows * tp
    if (
        heads != 2 * tp
        or n != heads
        or gate_drift.shape[0] != span
        or span > drift_span
    ):
        return on_device(
            tokens,
            pre_gain,
            w_query,
            w_key,
            w_value,
            w_igate,
            w_fgate,
            forget_bias,
            gate_drift,
            head_gain,
            w_out,
        )
    layers = n // 2
    depth = w_query.shape[0]
    dk = w_query.shape[1] // 2
    dv = w_value.shape[1] // 2
    features = w_out.shape[0]
    anywhere = pl.BlockSpec(memory_space=pl.ANY)
    dma = pltpu.SemaphoreType.DMA
    vmem = pltpu.VMEM
    parts = pl.pallas_call(
        functools.partial(layer_kernel, n, tp),
        out_shape=pltpu.VMEM((2, rows, features * n), bf16),
        in_specs=[anywhere] * 11,
        out_specs=anywhere,
        scratch_shapes=[
            vmem((rows, width), bf16),
            vmem((2 * span, width), bf16),
            vmem((2 * span, width), bf16),
            vmem((width,), bf16),
            vmem((heads, width), bf16),
            vmem((heads, width), bf16),
            vmem((1, heads), f32),
            vmem((heads * dv,), bf16),
            vmem((3, heads, span), f32),
            vmem((2, depth, dk), bf16),
            vmem((2, depth, dv), bf16),
            vmem((2, depth, dk), bf16),
            vmem((n, depth, dk), bf16),
            vmem((n, depth, dv), bf16),
            vmem((n, depth, dk), bf16),
            vmem((2, 2, 2, features, 2 * dv), bf16),
            vmem((2 * span, 2 * dk + dv), f32),
            vmem((n, dk, dv), bf16),
            vmem((n, 8, dk), f32),
            vmem((2, span, dv), bf16),
            vmem((layers, span, dv), bf16),
            vmem((2, 2, span, features), bf16),
            dma((11,)),
            dma((2,)),
            dma((2, 2, 2)),
            dma((1,)),
            dma((2,)),
            dma((3, 3)),
            dma((3, n)),
            dma((3,)),
            dma((9,)),
            dma((1,)),
            dma((2,)),
            dma((1,)),
            dma((2,)),
            dma((1,)),
            dma((2,)),
            dma((1,)),
            dma((1,)),
        ],
        compiler_params=pltpu.CompilerParams(collective_id=0, has_side_effects=True),
    )(
        tokens,
        pre_gain,
        w_key,
        w_value,
        w_query,
        w_igate.T,
        w_fgate.T,
        forget_bias[None, :],
        gate_drift.T,
        head_gain,
        w_out,
    )
    return jnp.sum(parts.astype(f32), axis=0).astype(bf16)


def solution(mesh):
    in_specs = (
        P(("sp", "tp"), None),
        P(),
        P("sp", "tp"),
        P("sp", "tp"),
        P("sp", "tp"),
        P(),
        P(),
        P(),
        P("sp", None),
        P(),
        P("sp", "tp"),
    )
    out_specs = P(("sp", "tp"), None)
    body = on_device
    if mesh.shape["sp"] == 2 * mesh.shape["tp"] and mesh.shape["tp"] == 4:
        body = functools.partial(on_device_layers, mesh.shape["sp"], mesh.shape["tp"])
    return jax.shard_map(
        body, mesh=mesh, in_specs=in_specs, out_specs=out_specs, check_vma=False
    )
```

```python
import functools

import jax
import jax.numpy as jnp
from jax import lax
from jax.experimental import pallas as pl
from jax.experimental.pallas import tpu as pltpu
from jax.sharding import PartitionSpec as P

BLOCK = 64


norm_floor = 0.1
lowest_log = -1e30
highest = lax.Precision.HIGHEST


def prefix(value, axis, combine, identity):
    peers, position = (lax.axis_size(axis), lax.axis_index(axis))
    everything = jax.tree.map(
        lambda part, kind: lax.all_gather(part.astype(kind), axis),
        value,
        jax.tree.map(lambda a: jnp.bfloat16 if a.dtype == jnp.float32 else a.dtype, value),
    )
    start = jax.tree.map(
        lambda part, zero: jnp.broadcast_to(jnp.asarray(zero, part.dtype), part.shape),
        value,
        identity,
    )

    def step(k, before):
        reached = k < position
        new = combine(
            before, jax.tree.map(lambda part, own: part[k].astype(own.dtype), everything, value)
        )
        return jax.tree.map(lambda a, b: jnp.where(reached, a, b), new, before)

    return lax.fori_loop(0, peers, step, start)


def advance(memory, summary):
    old_mat, old_vec, old_top = memory
    span_log, span_top, span_mat, span_vec = summary
    new_top = jnp.maximum(span_log + old_top, span_top)
    kept_part = jnp.exp(span_log + old_top - new_top)
    fresh_part = jnp.exp(span_top - new_top)
    return (
        kept_part[:, None, None] * old_mat + fresh_part[:, None, None] * span_mat,
        kept_part[:, None] * old_vec + fresh_part[:, None] * span_vec,
        new_top,
    )


def prefix_states(initial, summary):

    def stepper(memory, one_block):
        return (advance(memory, one_block), memory)

    return lax.scan(stepper, initial, summary)


def join_devices(earlier, later_part):
    early_log, early_mat, early_vec, early_top = earlier
    late_log, late_mat, late_vec, late_top = later_part
    new_top = jnp.maximum(late_log + early_top, late_top)
    kept_part = jnp.exp(late_log + early_top - new_top)
    fresh_part = jnp.exp(late_top - new_top)
    return (
        early_log + late_log,
        kept_part[:, None, None] * early_mat + fresh_part[:, None, None] * late_mat,
        kept_part[:, None] * early_vec + fresh_part[:, None] * late_vec,
        new_top,
    )


def blend_parts(first_part, second_part):
    numer_first, denom_first, peak_first = first_part
    numer_second, denom_second, peak_second = second_part
    new_top = jnp.maximum(peak_first, peak_second)
    weight_first = jnp.exp(peak_first - new_top)
    weight_second = jnp.exp(peak_second - new_top)
    return (
        weight_first[..., None] * numer_first + weight_second[..., None] * numer_second,
        weight_first * denom_first + weight_second * denom_second,
        new_top,
    )


def on_device(
    tokens,
    pre_gain,
    w_query,
    w_key,
    w_value,
    w_igate,
    w_fgate,
    forget_bias,
    gate_drift,
    head_gain,
    w_out,
):
    tp_size = lax.axis_size("tp")
    head_count = w_igate.shape[1]
    local_heads = head_count // tp_size
    first_head = lax.axis_index("tp") * local_heads
    key_width = w_query.shape[1] // local_heads
    value_width = w_value.shape[1] // local_heads
    token_wide = tokens.astype(jnp.float32)
    scaled = token_wide * lax.rsqrt(
        jnp.mean(token_wide * token_wide, axis=1, keepdims=True) + norm_floor
    )
    normed = (scaled * pre_gain.astype(jnp.float32)).astype(jnp.bfloat16)
    gate_cols = jnp.concatenate(
        [
            lax.dynamic_slice_in_dim(w_igate, first_head, local_heads, 1),
            lax.dynamic_slice_in_dim(w_fgate, first_head, local_heads, 1),
        ],
        axis=1,
    )
    key_scale = key_width ** (-0.5)
    wq_full, wk_full, wv_full = (
        lax.all_gather(w_query, "sp", axis=0, tiled=True),
        lax.all_gather(w_key, "sp", axis=0, tiled=True),
        lax.all_gather(w_value, "sp", axis=0, tiled=True),
    )
    row_piece = lax.all_gather(normed, "tp", axis=0, tiled=True)
    queries_part = jnp.dot(row_piece, wq_full, preferred_element_type=jnp.float32).astype(
        jnp.bfloat16
    )
    keys_part = (
        jnp.dot(row_piece, wk_full, preferred_element_type=jnp.float32) * key_scale
    ).astype(jnp.bfloat16)
    values_part = jnp.dot(row_piece, wv_full, preferred_element_type=jnp.float32).astype(
        jnp.bfloat16
    )
    gate_part = jnp.dot(row_piece, gate_cols, preferred_element_type=jnp.float32)
    group_len = queries_part.shape[0]
    blocks = group_len // BLOCK
    log_input = gate_part[:, :local_heads]
    forget_pre = gate_part[:, local_heads:] + lax.dynamic_slice_in_dim(
        forget_bias, first_head, local_heads, 0
    )
    log_forget = jax.nn.log_sigmoid(
        forget_pre + lax.dynamic_slice_in_dim(gate_drift, first_head, local_heads, 1)
    )
    query_blk = queries_part.reshape(blocks, BLOCK, local_heads, key_width)
    key_blk = keys_part.reshape(blocks, BLOCK, local_heads, key_width)
    value_blk = values_part.reshape(blocks, BLOCK, local_heads, value_width)
    input_blk = log_input.reshape(blocks, BLOCK, local_heads).transpose(0, 2, 1)
    forget_blk = log_forget.reshape(blocks, BLOCK, local_heads).transpose(0, 2, 1)
    within = jnp.cumsum(forget_blk, axis=2)
    causal = jnp.arange(BLOCK)[:, None] >= jnp.arange(BLOCK)[None, :]
    log_pair = jnp.where(
        causal, within[..., :, None] - within[..., None, :] + input_blk[..., None, :], -jnp.inf
    )
    peak_intra = jnp.max(log_pair, axis=3)
    scores = jnp.einsum("nshd,nrhd->nhsr", query_blk, key_blk, preferred_element_type=jnp.float32)
    weights = scores * jnp.exp(log_pair - peak_intra[..., None])
    numer_intra = jnp.einsum(
        "nhsr,nrhv->nhsv",
        weights.astype(jnp.bfloat16),
        value_blk,
        preferred_element_type=jnp.float32,
    )
    denom_intra = jnp.sum(weights, axis=3)
    span_log = within[..., -1]
    log_write = span_log[..., None] - within + input_blk
    span_top = jnp.max(log_write, axis=2)
    write_scale = jnp.exp(log_write - span_top[..., None])
    key_scaled = key_blk.astype(jnp.float32) * write_scale.transpose(0, 2, 1)[..., None]
    value_wide = value_blk.astype(jnp.float32)
    span_mat = jnp.einsum("nrhv,nrhd->nhvd", value_wide, key_scaled, precision=highest)
    span_vec = jnp.sum(key_scaled, axis=1)
    summary = (span_log, span_top, span_mat, span_vec)
    empty_state = (
        jnp.zeros((local_heads, value_width, key_width), jnp.float32),
        jnp.zeros((local_heads, key_width), jnp.float32),
        jnp.full((local_heads,), lowest_log, jnp.float32),
    )
    local_end, local_starts = prefix_states(empty_state, summary)
    device_summary = (jnp.sum(span_log, axis=0),) + local_end
    identity_all = (jnp.zeros((local_heads,), jnp.float32),) + empty_state
    incoming = prefix(device_summary, "sp", join_devices, identity_all)
    query_wide = query_blk.astype(jnp.float32)
    intra_part = (numer_intra, denom_intra, peak_intra)
    start_mat, start_vec, start_top = local_starts
    local_part = (
        jnp.einsum("nhvd,nshd->nhsv", start_mat, query_wide, precision=highest),
        jnp.einsum("nhd,nshd->nhs", start_vec, query_wide, precision=highest),
        within + start_top[..., None],
    )
    numerator, denominator, peak_log = blend_parts(local_part, intra_part)
    entry_log, entry_mat, entry_vec, entry_top = incoming
    before_log = jnp.concatenate(
        [jnp.zeros((1, local_heads), jnp.float32), jnp.cumsum(span_log, axis=0)[:-1]], axis=0
    )
    from_left = (
        jnp.einsum("hvd,nshd->nhsv", entry_mat, query_wide, precision=highest),
        jnp.einsum("hd,nshd->nhs", entry_vec, query_wide, precision=highest),
        within + (before_log + entry_top[None, :])[..., None],
    )
    numerator, denominator, peak_log = blend_parts((numerator, denominator, peak_log), from_left)
    hidden = numerator / jnp.maximum(jnp.abs(denominator), jnp.exp(-peak_log))[..., None]
    hidden = hidden.transpose(0, 2, 1, 3).reshape(group_len, local_heads, value_width)
    head_gains = lax.dynamic_slice_in_dim(
        head_gain, first_head * value_width, local_heads * value_width, 0
    )
    head_gains = head_gains.astype(jnp.float32).reshape(local_heads, value_width)
    normed_heads = (
        hidden
        * lax.rsqrt(jnp.mean(hidden * hidden, axis=2, keepdims=True) + norm_floor)
        * head_gains
    )
    normed_heads = normed_heads.astype(jnp.bfloat16).reshape(group_len, local_heads * value_width)
    out_slab = lax.all_gather(w_out, "sp", axis=0, tiled=True)
    return lax.psum_scatter(
        lax.dot_general(
            normed_heads, out_slab, (((1,), (1,)), ((), ())), preferred_element_type=jnp.float32
        ).astype(jnp.bfloat16),
        "tp",
        scatter_dimension=0,
        tiled=True,
    )


drift_span = 128
MESH = pl.DeviceIdType.MESH
f32 = jnp.float32
bf16 = jnp.bfloat16


def dot_nt(a, b):
    return lax.dot_general(a, b, (((1,), (1,)), ((), ())), preferred_element_type=f32)


def layer_kernel(
    n,
    tp,
    tokens,
    pre_gain,
    w_key,
    w_value,
    w_query,
    w_igate,
    w_fgate,
    forget_bias,
    drift,
    head_gain,
    w_out,
    out,
    tok_own,
    tok_all,
    normed,
    gain_in,
    igate_in,
    fgate_in,
    bias_in,
    head_gain_in,
    drift_in,
    key_own,
    value_own,
    query_own,
    key_all,
    value_all,
    query_all,
    out_all,
    acc,
    state_all,
    aux_all,
    heads,
    heads_in,
    part,
    load_sems,
    tok_send,
    tok_recv,
    drift_send,
    drift_recv,
    w_send,
    pass_send,
    w_recv,
    out_send,
    out_recv,
    state_send,
    state_recv,
    aux_send,
    aux_recv,
    heads_send,
    heads_recv,
    final_send,
    final_recv,
):
    s = lax.axis_index("sp")
    t = lax.axis_index("tp")
    layers = n // 2
    z = s // 2
    x = s % 2
    y = t // 2
    c = t % 2
    zh = z // 2
    zl = z % 2
    near = zh == c
    far = jnp.logical_not(near)
    head = layers * y + z
    rows = tok_own.shape[0]
    span = rows * tp
    length = 2 * span
    depth = key_own.shape[1]
    dk = key_own.shape[2]
    dv = value_own.shape[2]

    def flip(value):
        return 1 - value

    def at_layer(dz):
        if dz == 0:
            return z
        if dz == 1:
            return 2 * zh + flip(zl)
        if dz == 2:
            return 2 * flip(zh) + zl
        return 2 * flip(zh) + flip(zl)

    def dev(zz, xx, yy, cc):
        return 2 * zz + xx, 2 * yy + cc

    barrier = pltpu.get_barrier_semaphore()
    to_sibling = dev(z, x, y, flip(c))
    partners = [dev(z, flip(x), y, cc) for cc in range(2)]
    for dz in range(layers):
        for yy in (y, flip(y)) if dz < 2 else (y,):
            partners += [dev(at_layer(dz), x, yy, cc) for cc in range(2)]
    partners[2:4] = [to_sibling]
    for ss, tt in partners:
        pl.semaphore_signal(
            barrier,
            inc=1,
            device_id={"sp": ss, "tp": tt},
            device_id_type=MESH,
        )

    def load(source, target, sem):
        copy = pltpu.make_async_copy(source, target, sem)
        copy.start()
        return copy

    pieces = (
        (w_key, key_own, key_all),
        (w_value, value_own, value_all),
        (w_query, query_own, query_all),
    )

    def token_slot(parity, to_t):
        start = pl.multiple_of((parity * tp + to_t) * rows, rows)
        return tok_all.at[pl.ds(start, rows)]

    own_slot = token_slot(zl, t)
    load_tokens = load(tokens, tok_own, load_sems.at[0])
    loads_own = []
    for p, (w_hbm, own, full) in enumerate(pieces):
        width = own.shape[2]
        loads_own.append(
            [
                load(
                    w_hbm.at[:, pl.ds(j * width, width)],
                    own.at[j],
                    load_sems.at[1 + p],
                )
                for j in range(2)
            ]
        )
    chunk = out_all.shape[3] // 2
    loads_out = [
        load(
            w_out.at[pl.ds(i * chunk, chunk)],
            out_all.at[zh, x, c, pl.ds(i * chunk, chunk)],
            load_sems.at[4],
        )
        for i in range(2)
    ]
    small = (
        (pre_gain, gain_in),
        (w_igate, igate_in),
        (w_fgate, fgate_in),
        (forget_bias, bias_in),
        (head_gain, head_gain_in),
    )
    loads_small = [load(a, b, load_sems.at[5 + i]) for i, (a, b) in enumerate(small)]

    @pl.when(near)
    def _():
        pltpu.make_async_copy(tokens, own_slot, tok_recv.at[zl, 0, c]).start()
        pltpu.make_async_copy(drift, drift_in.at[zl], drift_recv.at[0]).start()
        for p, (w_hbm, own, full) in enumerate(pieces):
            width = own.shape[2]
            for j in range(2):

                @pl.when(zl == j)
                def _():
                    pltpu.make_async_copy(
                        w_hbm.at[:, pl.ds(j * width, width)], full.at[s], w_recv.at[p, 0]
                    ).start()

    load_drift = load(drift, drift_in.at[2], load_sems.at[10])

    @pl.when(c == 0)
    def _():
        state_all[layers:, :, :] = jnp.zeros((layers, dk, dv), bf16)
        aux_all[layers:, :, :] = jnp.zeros((layers, aux_all.shape[1], dk), f32)

    pl.semaphore_wait(barrier, len(partners))

    def plan(source, target, send_sem, recv_sem, to, flag=None):
        copy = pltpu.make_async_remote_copy(
            src_ref=source,
            dst_ref=target,
            send_sem=send_sem,
            recv_sem=recv_sem,
            device_id={"sp": to[0], "tp": to[1]},
            device_id_type=MESH,
        )
        return copy

    def send(source, target, send_sem, recv_sem, to, flag=None, keep=None):
        if keep is not None:

            @pl.when(keep)
            def _():
                pltpu.make_async_copy(source, target, recv_sem).start()

            flag = jnp.logical_not(keep)
        copy = plan(source, target, send_sem, recv_sem, to, flag)
        if flag is None:
            copy.start()
        else:
            pl.when(flag)(copy.start)

    def arrived(target, sem):
        pltpu.make_async_copy(target, target, sem).wait()

    load_tokens.wait()
    mine = tok_recv.at[zl, 0, c]
    send(tok_own, own_slot, tok_send.at[0], mine, dev(at_layer(2), x, y, zh))
    send(tok_own, own_slot, tok_send.at[0], mine, dev(at_layer(1), x, y, zh))
    send(
        tok_own, own_slot, tok_send.at[0], tok_recv.at[zl, 1, c], dev(z, x, flip(y), zh)
    )
    send(tok_own, own_slot, tok_send.at[0], mine, dev(z, x, y, flip(c)), flag=far)
    load_drift.wait()
    for i in range(1, 4):
        send(
            drift_in.at[2],
            drift_in.at[zl],
            drift_send.at[0],
            drift_recv.at[0],
            dev(at_layer(i), x, y, c),
            flag=near,
        )

    for copy in loads_small:
        copy.wait()
    gain = gain_in[...].astype(f32)[None, :]

    def normalize(parity, to_t):
        start = pl.multiple_of((parity * tp + to_t) * rows, rows)
        wide = tok_all[pl.ds(start, rows), :].astype(f32)
        scale = lax.rsqrt(jnp.mean(wide * wide, axis=1, keepdims=True) + norm_floor)
        normed[pl.ds(start, rows), :] = (wide * scale * gain).astype(bf16)

    to_x = dev(z, flip(x), y, c)
    to_core = dev(z, x, y, flip(c))
    to_half = dev(at_layer(2), x, y, c)

    def plan_first(p):
        _, own, full = pieces[p]
        sem = w_recv.at[p, 2]
        side_sem = w_recv.at[p, 1]
        middle = dev(1 + c * (layers - 3), x, y, c)
        end = dev(c * (layers - 1), x, y, c)
        beside = dev(at_layer(1), x, y, c)
        target = full.at[s]
        return (
            plan(own.at[flip(c)], target, w_send.at[p], sem, middle, far),
            plan(own.at[c], target, w_send.at[p], sem, end, far),
            plan(own.at[flip(zl)], target, w_send.at[p], side_sem, beside, near),
        )

    def plan_pass(p, dzs, across):
        blocks = [2 * at_layer(dz) + (flip(x) if across else x) for dz in dzs]
        refs = [pieces[p][2].at[block] for block in blocks]
        sem = w_recv.at[p, (3 if dzs[0] == 0 else 4) if across else min(dzs[0], 2)]
        across_sem = w_recv.at[p, 3 if dzs[0] == 0 else 4]
        to_far = w_recv.at[p, 0]
        onward = []
        for full in refs:
            if not across:
                onward.append(plan(full, full, pass_send.at[0], across_sem, to_x, near))
            onward.append(plan(full, full, pass_send.at[1], to_far, to_core, near))

        def run():
            arrived(pieces[p][2].at[pl.ds(0, len(refs))], sem)
            for copy in onward:
                copy.start()

        return run

    def plan_token(parity, c_src, i, onward):
        slot = token_slot(parity, 2 * y + c_src)
        sem = tok_recv.at[parity, 0, c_src]
        out_sem = tok_recv.at[parity, 1, c_src]
        to_y = dev(z, x, flip(y), c)
        copies = []
        if onward:
            copies.append(
                plan(slot, slot, tok_send.at[1], sem, dev(at_layer(1), x, y, c), far)
            )
        copies.append(
            plan(slot, slot, tok_send.at[1], out_sem, to_y, far if onward else None)
        )

        def run(forward=True):
            arrived(slot, sem)
            if forward:
                for copy in copies:
                    copy.start()

        return run

    def out_chunk(zb, xb, cb, i):
        return out_all.at[zb, xb, cb, pl.ds(i * chunk, chunk)]

    def plan_out(zb, xb, i, to):
        piece = out_chunk(zb, xb, c, i)
        targets = {
            "half": (out_send.at[0], out_recv.at[i], to_half),
            "x": (out_send.at[1], out_recv.at[2], to_x),
            "far_x": (out_send.at[1], out_recv.at[3 + i], to_x),
            "core": (out_send.at[2], out_recv.at[5 + 2 * zb + xb], to_core),
        }
        return [plan(piece, piece, targets[k][0], targets[k][1], targets[k][2]) for k in to]

    firsts = [plan_first(p) for p in range(3)]
    direct = [[plan_pass(p, dzs, False) for dzs in ((0,), (1,), (2, 3))] for p in range(3)]
    cross = [[plan_pass(p, dzs, True) for dzs in ((0,), (1, 2, 3))] for p in range(3)]
    token_a = [plan_token(zl, k, k, True) for k in range(2)]
    token_b = [plan_token(flip(zl), k, 2 + k, False) for k in range(2)]
    out_own = [plan_out(zh, x, i, ("x", "core")) for i in range(2)]
    out_half = [plan_out(zh, x, i, ("half",))[0] for i in range(2)]

    out_near_x = [plan_out(zh, flip(x), i, ("core",)) for i in range(2)]
    out_far = [plan_out(flip(zh), x, i, ("far_x", "core")) for i in range(2)]
    out_far_x = [plan_out(flip(zh), flip(x), i, ("core",)) for i in range(2)]

    def out_from_x():
        arrived(out_all.at[zh, flip(x), c], out_recv.at[2])
        for i in range(2):
            out_near_x[i][0].start()

    def out_from_half(i):
        arrived(out_chunk(flip(zh), x, c, i), out_recv.at[i])
        for copy in out_far[i]:
            copy.start()

    def out_start():
        arrived(out_all.at[zh, x, c], load_sems.at[4])
        for pair in out_own:
            for copy in pair:
                copy.start()

    for p in range(3):
        arrived(pieces[p][1], load_sems.at[1 + p])

    @pl.when(near)
    def _():
        firsts[1][2].start()
        for p in (1, 0, 2):
            direct[p][0]()
        out_start()
        for run in token_a:
            run(False)
        for run in token_b:
            run()

    @pl.when(far)
    def _():
        firsts[1][1].start()
        firsts[1][0].start()
        firsts[0][1].start()
        firsts[0][0].start()
        out_start()
        for run in token_a:
            run()
        for i in (1, 0):
            firsts[2][i].start()
        for run in token_b:
            run()
        arrived(pieces[0][1], w_send.at[0])
        arrived(pieces[2][1], w_send.at[2])
        for copy in out_half:
            copy.start()

    for parity in range(2):
        for c_src in range(2):
            normalize(parity, 2 * y + c_src)

    @pl.when(near)
    def _():
        firsts[0][2].start()
        firsts[2][2].start()
        direct[1][1]()
        direct[1][2]()
        for p in (1, 0, 2):
            cross[p][0]()

    for parity in range(2):
        for c_src in range(2):
            to_t = 2 * flip(y) + c_src
            arrived(token_slot(parity, to_t), tok_recv.at[parity, 1, c_src])
            normalize(parity, to_t)

    all_normed = normed[...]
    gate_in = dot_nt(all_normed, igate_in[...])
    gate_forget = dot_nt(all_normed, fgate_in[...])
    pick = lax.broadcasted_iota(jnp.int32, gate_in.shape, 1) == head
    pick_bias = lax.broadcasted_iota(jnp.int32, bias_in.shape, 1) == head
    bias = jnp.sum(jnp.where(pick_bias, bias_in[...], 0.0), axis=1, keepdims=True)
    forget_all = jnp.sum(jnp.where(pick, gate_forget, 0.0), axis=1, keepdims=True) + bias
    input_all = jnp.sum(jnp.where(pick, gate_in, 0.0), axis=1, keepdims=True)
    row_id = lax.broadcasted_iota(jnp.int32, (span, span), 0)
    col_id = lax.broadcasted_iota(jnp.int32, (span, span), 1)
    causal = row_id >= col_id
    eye = row_id == col_id
    arrived(drift_in.at[pl.ds(0, 2)], drift_recv.at[0])
    gates = []
    for j in range(2):
        offset = drift_in[j, pl.ds(head, 1), :][:, :1]
        pre = forget_all[j * span : (j + 1) * span] + offset
        in_col = input_all[j * span : (j + 1) * span]
        lf_col = jnp.minimum(pre, 0.0) - jnp.log1p(jnp.exp(-jnp.abs(pre)))
        lf_row = jnp.sum(jnp.where(eye, lf_col, 0.0), axis=0, keepdims=True)
        in_row = jnp.sum(jnp.where(eye, in_col, 0.0), axis=0, keepdims=True)
        b_col = jnp.sum(jnp.where(causal, lf_row, 0.0), axis=1, keepdims=True)
        b_row = jnp.sum(jnp.where(row_id <= col_id, lf_col, 0.0), axis=0, keepdims=True)
        total = jnp.sum(lf_col, axis=0, keepdims=True)
        write = total - b_col + in_col
        top = jnp.max(write, axis=0, keepdims=True)
        write_scale = jnp.exp(write - top)
        log_pair = jnp.where(causal, b_col - b_row + in_row, lowest_log)
        peak = jnp.max(log_pair, axis=1, keepdims=True)
        decay = jnp.where(causal, jnp.exp(log_pair - peak), 0.0)
        gates.append((b_col, total, top, write_scale, peak, decay))


    @pl.when(near)
    def _():
        direct[0][1]()
        direct[0][2]()
        cross[1][1]()
        direct[2][1]()
        direct[2][2]()
        for copy in out_half:
            copy.start()

    cols = (slice(0, dk), slice(dk, dk + dv), slice(dk + dv, 2 * dk + dv))

    def products(p):
        full = pieces[p][2]

        @pl.when(far)
        def _():
            arrived(full, w_recv.at[p, 0])

        flat = full[...].reshape(n * depth, full.shape[2])
        acc[:, cols[p]] = jnp.dot(normed[...], flat, preferred_element_type=f32)

    products(1)

    @pl.when(near)
    def _():
        cross[0][1]()

    products(0)

    spans = [4 * c + 2 * j + x for j in range(2)]
    keys = (acc[:, cols[0]] * (dk**-0.5)).astype(bf16)
    values = acc[:, cols[1]].astype(bf16)
    for j in range(2):
        b_col, total, top, write_scale, peak, decay = gates[j]
        at = slice(j * span, (j + 1) * span)
        key_scaled = keys[at].astype(f32) * write_scale
        state_all[spans[j]] = jnp.dot(
            key_scaled.T.astype(bf16), values[at], preferred_element_type=f32
        ).astype(bf16)
        mine = spans[j]
        aux_all[mine, 0:1, :] = jnp.broadcast_to(total, (1, dk))
        aux_all[mine, 1:2, :] = jnp.broadcast_to(top, (1, dk))
        aux_all[mine, 2:3, :] = jnp.sum(key_scaled, axis=0, keepdims=True)
        aux_all[mine, 3:, :] = jnp.zeros((aux_all.shape[1] - 3, dk), f32)
    late = c == 1
    early = c == 0
    for k, (to, flag) in enumerate(
        (
            (dev(z, flip(x), y, c), None),
            (dev(z, flip(x), y, flip(c)), early),
            (dev(z, x, y, flip(c)), early),
        )
    ):
        group = 0 if k == 0 else 1
        for j in range(2):
            mine = spans[j]
            send(
                aux_all.at[mine],
                aux_all.at[mine],
                aux_send.at[0],
                aux_recv.at[group],
                to,
                flag=flag,
            )
            send(
                state_all.at[mine],
                state_all.at[mine],
                state_send.at[0],
                state_recv.at[group],
                to,
                flag=flag,
            )

    @pl.when(near)
    def _():
        cross[2][1]()

    products(2)
    queries = acc[:, cols[2]].astype(bf16)
    intra = []
    for j in range(2):
        b_col, total, top, write_scale, peak, decay = gates[j]
        at = slice(j * span, (j + 1) * span)
        weights = dot_nt(queries[at], keys[at]) * decay
        numer = jnp.dot(weights.astype(bf16), values[at], preferred_element_type=f32)
        denom = jnp.sum(weights, axis=1, keepdims=True)
        intra.append((numer, denom))

    pl.when(near)(functools.partial(out_from_half, 0))
    arrived(aux_all.at[pl.ds(0, 2)], aux_recv.at[0])
    arrived(state_all.at[pl.ds(0, 2)], state_recv.at[0])

    @pl.when(late)
    def _():
        arrived(aux_all.at[pl.ds(0, layers)], aux_recv.at[1])
        arrived(state_all.at[pl.ds(0, layers)], state_recv.at[1])

    span_rows = aux_all[:, 0, :]
    top_rows = aux_all[:, 1, :]
    vec_rows = aux_all[:, 2, :]
    place = lax.broadcasted_iota(jnp.int32, span_rows.shape, 0)
    gain_row = head_gain_in[pl.ds(pl.multiple_of(head * dv, dv), dv)].astype(f32)[None, :]
    for j in range(2):
        b_col, total, top, write_scale, peak, decay = gates[j]
        numer, denom = intra[j]
        at = slice(j * span, (j + 1) * span)
        before = place < spans[j]
        logs = top_rows
        for m in range(1, n):
            between = (place < m) & (spans[j] > m)
            logs = logs + jnp.where(between, span_rows[m : m + 1, :], 0.0)
        logs = jnp.where(before, logs, lowest_log)
        entry = jnp.max(logs, axis=0, keepdims=True)
        weight = jnp.where(before, jnp.exp(logs - entry), 0.0)
        vec = jnp.sum(weight * vec_rows, axis=0, keepdims=True)
        mat = jnp.zeros((dk, dv), f32)
        for m in range(n - 1):
            mat = mat + weight[m : m + 1, :1] * state_all[m].astype(f32)
        carried = b_col + entry[:, :1]
        new_top = jnp.maximum(peak, carried)
        w_intra = jnp.exp(peak - new_top)
        w_carry = jnp.exp(carried - new_top)
        numer = w_intra * numer + w_carry * jnp.dot(
            queries[at], mat.astype(bf16), preferred_element_type=f32
        )
        denom = w_intra * denom + w_carry * jnp.sum(
            queries[at].astype(f32) * vec, axis=1, keepdims=True
        )
        hidden = numer / jnp.maximum(jnp.abs(denom), jnp.exp(-new_top))
        heads[j] = (
            hidden
            * lax.rsqrt(jnp.mean(hidden * hidden, axis=1, keepdims=True) + norm_floor)
            * gain_row
        ).astype(bf16)
        for d in range(2):
            send(
                heads.at[j],
                heads_in.at[z],
                heads_send.at[0],
                heads_recv.at[zh],
                dev(2 * c + d, x, y, j),
                keep=near & (zl == d) & (c == j),
            )

    out_from_x()
    pl.when(far)(functools.partial(out_from_half, 0))
    out_from_half(1)
    features = out_all.shape[3]
    home = 2 * zh + c
    wide = 2 * features

    def landing(yy, zz, zb, xb):
        start = pl.multiple_of((zz + 2 * zb) * wide + xb * features, features)
        return out.at[yy, :, pl.ds(start, features)]

    def out_arrived(zb, xb):
        arrived(out_all.at[zb, xb, flip(c)], out_recv.at[5 + 2 * zb + xb])

    def heads_arrived(half):
        arrived(heads_in.at[pl.ds(2 * half, 2)], heads_recv.at[half])

    def project(zb, xb, half):
        total = jnp.zeros((span, features), f32)
        for i in range(2):
            total = total + dot_nt(
                heads_in[2 * half + i], out_all[zb, xb, half, :, i * dv : (i + 1) * dv]
            )
        return total

    def share(zb, xb, total):
        part[zb, xb] = total.astype(bf16)
        for yy in range(2):
            for cc in range(2):
                send(
                    part.at[zb, xb, pl.ds((2 * yy + cc) * rows, rows)],
                    landing(y, zl, zb, xb),
                    final_send.at[0],
                    final_recv.at[0],
                    dev(home, x, yy, cc),
                    keep=(zl == c) & (y == yy) & (c == cc),
                )

    sides = (x, flip(x))
    for xb in sides:
        out_arrived(zh, xb)
    heads_arrived(zh)
    early_part = [project(zh, xb, zh) for xb in sides]
    for i in range(2):
        arrived(out_chunk(flip(zh), flip(x), c, i), out_recv.at[3 + i])
        out_far_x[i][0].start()
    heads_arrived(flip(zh))
    for k, xb in enumerate(sides):
        share(zh, xb, early_part[k] + project(zh, xb, flip(zh)))
    for xb in sides:
        out_arrived(flip(zh), xb)
        share(flip(zh), xb, project(flip(zh), xb, zh) + project(flip(zh), xb, flip(zh)))
    arrived(out, final_recv.at[0])

    def drained(ref, sem, flag=None):
        if flag is None:
            arrived(ref, sem)
        else:
            pl.when(flag)(functools.partial(arrived, ref, sem))

    drained(tok_all.at[pl.ds(0, 4 * rows)], tok_send.at[0], far)
    drained(tok_all.at[pl.ds(0, 6 * rows)], tok_send.at[1], far)
    drained(tok_all.at[pl.ds(0, 3 * rows)], tok_send.at[0], near)
    drained(tok_all.at[pl.ds(0, 2 * rows)], tok_send.at[1], near)
    drained(drift_in, drift_send.at[0], near)
    for p in range(3):
        _, own, full = pieces[p]
        if p == 1:
            drained(own, w_send.at[p], far)
        drained(own.at[0], w_send.at[p], near)
    drained(out_all.at[0], pass_send.at[0], near)
    drained(out_all, pass_send.at[1], near)
    drained(out_all.at[0, 0, 0], out_send.at[0])
    drained(out_all.at[0, 0], out_send.at[1])
    drained(out_all.at[0], out_send.at[2])
    for ref, sem in ((state_all, state_send.at[0]), (aux_all, aux_send.at[0])):
        drained(ref.at[pl.ds(0, 6)], sem, early)
        drained(ref.at[pl.ds(0, 2)], sem, late)
    drained(heads_in.at[pl.ds(0, 3)], heads_send.at[0], near)
    drained(heads_in, heads_send.at[0], far)
    at_home = zl == c
    drained(part, final_send.at[0], jnp.logical_not(at_home))
    drained(part.at[:, :, pl.ds(0, 3 * rows)], final_send.at[0], at_home)


def on_device_layers(
    n,
    tp,
    tokens,
    pre_gain,
    w_query,
    w_key,
    w_value,
    w_igate,
    w_fgate,
    forget_bias,
    gate_drift,
    head_gain,
    w_out,
):
    heads = w_igate.shape[1]
    rows, width = tokens.shape
    span = rows * tp
    if (
        heads != 2 * tp
        or n != heads
        or gate_drift.shape[0] != span
        or span > drift_span
    ):
        return on_device(
            tokens,
            pre_gain,
            w_query,
            w_key,
            w_value,
            w_igate,
            w_fgate,
            forget_bias,
            gate_drift,
            head_gain,
            w_out,
        )
    layers = n // 2
    depth = w_query.shape[0]
    dk = w_query.shape[1] // 2
    dv = w_value.shape[1] // 2
    features = w_out.shape[0]
    anywhere = pl.BlockSpec(memory_space=pl.ANY)
    dma = pltpu.SemaphoreType.DMA
    vmem = pltpu.VMEM
    parts = pl.pallas_call(
        functools.partial(layer_kernel, n, tp),
        out_shape=pltpu.VMEM((2, rows, features * n), bf16),
        in_specs=[anywhere] * 11,
        out_specs=anywhere,
        scratch_shapes=[
            vmem((rows, width), bf16),
            vmem((2 * span, width), bf16),
            vmem((2 * span, width), bf16),
            vmem((width,), bf16),
            vmem((heads, width), bf16),
            vmem((heads, width), bf16),
            vmem((1, heads), f32),
            vmem((heads * dv,), bf16),
            vmem((3, heads, span), f32),
            vmem((2, depth, dk), bf16),
            vmem((2, depth, dv), bf16),
            vmem((2, depth, dk), bf16),
            vmem((n, depth, dk), bf16),
            vmem((n, depth, dv), bf16),
            vmem((n, depth, dk), bf16),
            vmem((2, 2, 2, features, 2 * dv), bf16),
            vmem((2 * span, 2 * dk + dv), f32),
            vmem((n, dk, dv), bf16),
            vmem((n, 8, dk), f32),
            vmem((2, span, dv), bf16),
            vmem((layers, span, dv), bf16),
            vmem((2, 2, span, features), bf16),
            dma((11,)),
            dma((2,)),
            dma((2, 2, 2)),
            dma((1,)),
            dma((1,)),
            dma((3,)),
            dma((2,)),
            dma((3, 5)),
            dma((3,)),
            dma((9,)),
            dma((1,)),
            dma((2,)),
            dma((1,)),
            dma((2,)),
            dma((1,)),
            dma((2,)),
            dma((1,)),
            dma((1,)),
        ],
        compiler_params=pltpu.CompilerParams(collective_id=0, has_side_effects=True),
    )(
        tokens,
        pre_gain,
        w_key,
        w_value,
        w_query,
        w_igate.T,
        w_fgate.T,
        forget_bias[None, :],
        gate_drift.T,
        head_gain,
        w_out,
    )
    return jnp.sum(parts.astype(f32), axis=0).astype(bf16)


def solution(mesh):
    in_specs = (
        P(("sp", "tp"), None),
        P(),
        P("sp", "tp"),
        P("sp", "tp"),
        P("sp", "tp"),
        P(),
        P(),
        P(),
        P("sp", None),
        P(),
        P("sp", "tp"),
    )
    out_specs = P(("sp", "tp"), None)
    body = on_device
    if mesh.shape["sp"] == 2 * mesh.shape["tp"] and mesh.shape["tp"] == 4:
        body = functools.partial(on_device_layers, mesh.shape["sp"], mesh.shape["tp"])
    return jax.shard_map(
        body, mesh=mesh, in_specs=in_specs, out_specs=out_specs, check_vma=False
    )
```

```python
import functools

import jax
import jax.numpy as jnp
from jax import lax
from jax.experimental import pallas as pl
from jax.experimental.pallas import tpu as pltpu
from jax.sharding import PartitionSpec as P

BLOCK = 64


norm_floor = 0.1
lowest_log = -1e30
highest = lax.Precision.HIGHEST


def prefix(value, axis, combine, identity):
    peers, position = (lax.axis_size(axis), lax.axis_index(axis))
    everything = jax.tree.map(
        lambda part, kind: lax.all_gather(part.astype(kind), axis),
        value,
        jax.tree.map(lambda a: jnp.bfloat16 if a.dtype == jnp.float32 else a.dtype, value),
    )
    start = jax.tree.map(
        lambda part, zero: jnp.broadcast_to(jnp.asarray(zero, part.dtype), part.shape),
        value,
        identity,
    )

    def step(k, before):
        reached = k < position
        new = combine(
            before, jax.tree.map(lambda part, own: part[k].astype(own.dtype), everything, value)
        )
        return jax.tree.map(lambda a, b: jnp.where(reached, a, b), new, before)

    return lax.fori_loop(0, peers, step, start)


def advance(memory, summary):
    old_mat, old_vec, old_top = memory
    span_log, span_top, span_mat, span_vec = summary
    new_top = jnp.maximum(span_log + old_top, span_top)
    kept_part = jnp.exp(span_log + old_top - new_top)
    fresh_part = jnp.exp(span_top - new_top)
    return (
        kept_part[:, None, None] * old_mat + fresh_part[:, None, None] * span_mat,
        kept_part[:, None] * old_vec + fresh_part[:, None] * span_vec,
        new_top,
    )


def prefix_states(initial, summary):

    def stepper(memory, one_block):
        return (advance(memory, one_block), memory)

    return lax.scan(stepper, initial, summary)


def join_devices(earlier, later_part):
    early_log, early_mat, early_vec, early_top = earlier
    late_log, late_mat, late_vec, late_top = later_part
    new_top = jnp.maximum(late_log + early_top, late_top)
    kept_part = jnp.exp(late_log + early_top - new_top)
    fresh_part = jnp.exp(late_top - new_top)
    return (
        early_log + late_log,
        kept_part[:, None, None] * early_mat + fresh_part[:, None, None] * late_mat,
        kept_part[:, None] * early_vec + fresh_part[:, None] * late_vec,
        new_top,
    )


def blend_parts(first_part, second_part):
    numer_first, denom_first, peak_first = first_part
    numer_second, denom_second, peak_second = second_part
    new_top = jnp.maximum(peak_first, peak_second)
    weight_first = jnp.exp(peak_first - new_top)
    weight_second = jnp.exp(peak_second - new_top)
    return (
        weight_first[..., None] * numer_first + weight_second[..., None] * numer_second,
        weight_first * denom_first + weight_second * denom_second,
        new_top,
    )


def on_device(
    tokens,
    pre_gain,
    w_query,
    w_key,
    w_value,
    w_igate,
    w_fgate,
    forget_bias,
    gate_drift,
    head_gain,
    w_out,
):
    tp_size = lax.axis_size("tp")
    head_count = w_igate.shape[1]
    local_heads = head_count // tp_size
    first_head = lax.axis_index("tp") * local_heads
    key_width = w_query.shape[1] // local_heads
    value_width = w_value.shape[1] // local_heads
    token_wide = tokens.astype(jnp.float32)
    scaled = token_wide * lax.rsqrt(
        jnp.mean(token_wide * token_wide, axis=1, keepdims=True) + norm_floor
    )
    normed = (scaled * pre_gain.astype(jnp.float32)).astype(jnp.bfloat16)
    gate_cols = jnp.concatenate(
        [
            lax.dynamic_slice_in_dim(w_igate, first_head, local_heads, 1),
            lax.dynamic_slice_in_dim(w_fgate, first_head, local_heads, 1),
        ],
        axis=1,
    )
    key_scale = key_width ** (-0.5)
    wq_full, wk_full, wv_full = (
        lax.all_gather(w_query, "sp", axis=0, tiled=True),
        lax.all_gather(w_key, "sp", axis=0, tiled=True),
        lax.all_gather(w_value, "sp", axis=0, tiled=True),
    )
    row_piece = lax.all_gather(normed, "tp", axis=0, tiled=True)
    queries_part = jnp.dot(row_piece, wq_full, preferred_element_type=jnp.float32).astype(
        jnp.bfloat16
    )
    keys_part = (
        jnp.dot(row_piece, wk_full, preferred_element_type=jnp.float32) * key_scale
    ).astype(jnp.bfloat16)
    values_part = jnp.dot(row_piece, wv_full, preferred_element_type=jnp.float32).astype(
        jnp.bfloat16
    )
    gate_part = jnp.dot(row_piece, gate_cols, preferred_element_type=jnp.float32)
    group_len = queries_part.shape[0]
    blocks = group_len // BLOCK
    log_input = gate_part[:, :local_heads]
    forget_pre = gate_part[:, local_heads:] + lax.dynamic_slice_in_dim(
        forget_bias, first_head, local_heads, 0
    )
    log_forget = jax.nn.log_sigmoid(
        forget_pre + lax.dynamic_slice_in_dim(gate_drift, first_head, local_heads, 1)
    )
    query_blk = queries_part.reshape(blocks, BLOCK, local_heads, key_width)
    key_blk = keys_part.reshape(blocks, BLOCK, local_heads, key_width)
    value_blk = values_part.reshape(blocks, BLOCK, local_heads, value_width)
    input_blk = log_input.reshape(blocks, BLOCK, local_heads).transpose(0, 2, 1)
    forget_blk = log_forget.reshape(blocks, BLOCK, local_heads).transpose(0, 2, 1)
    within = jnp.cumsum(forget_blk, axis=2)
    causal = jnp.arange(BLOCK)[:, None] >= jnp.arange(BLOCK)[None, :]
    log_pair = jnp.where(
        causal, within[..., :, None] - within[..., None, :] + input_blk[..., None, :], -jnp.inf
    )
    peak_intra = jnp.max(log_pair, axis=3)
    scores = jnp.einsum("nshd,nrhd->nhsr", query_blk, key_blk, preferred_element_type=jnp.float32)
    weights = scores * jnp.exp(log_pair - peak_intra[..., None])
    numer_intra = jnp.einsum(
        "nhsr,nrhv->nhsv",
        weights.astype(jnp.bfloat16),
        value_blk,
        preferred_element_type=jnp.float32,
    )
    denom_intra = jnp.sum(weights, axis=3)
    span_log = within[..., -1]
    log_write = span_log[..., None] - within + input_blk
    span_top = jnp.max(log_write, axis=2)
    write_scale = jnp.exp(log_write - span_top[..., None])
    key_scaled = key_blk.astype(jnp.float32) * write_scale.transpose(0, 2, 1)[..., None]
    value_wide = value_blk.astype(jnp.float32)
    span_mat = jnp.einsum("nrhv,nrhd->nhvd", value_wide, key_scaled, precision=highest)
    span_vec = jnp.sum(key_scaled, axis=1)
    summary = (span_log, span_top, span_mat, span_vec)
    empty_state = (
        jnp.zeros((local_heads, value_width, key_width), jnp.float32),
        jnp.zeros((local_heads, key_width), jnp.float32),
        jnp.full((local_heads,), lowest_log, jnp.float32),
    )
    local_end, local_starts = prefix_states(empty_state, summary)
    device_summary = (jnp.sum(span_log, axis=0),) + local_end
    identity_all = (jnp.zeros((local_heads,), jnp.float32),) + empty_state
    incoming = prefix(device_summary, "sp", join_devices, identity_all)
    query_wide = query_blk.astype(jnp.float32)
    intra_part = (numer_intra, denom_intra, peak_intra)
    start_mat, start_vec, start_top = local_starts
    local_part = (
        jnp.einsum("nhvd,nshd->nhsv", start_mat, query_wide, precision=highest),
        jnp.einsum("nhd,nshd->nhs", start_vec, query_wide, precision=highest),
        within + start_top[..., None],
    )
    numerator, denominator, peak_log = blend_parts(local_part, intra_part)
    entry_log, entry_mat, entry_vec, entry_top = incoming
    before_log = jnp.concatenate(
        [jnp.zeros((1, local_heads), jnp.float32), jnp.cumsum(span_log, axis=0)[:-1]], axis=0
    )
    from_left = (
        jnp.einsum("hvd,nshd->nhsv", entry_mat, query_wide, precision=highest),
        jnp.einsum("hd,nshd->nhs", entry_vec, query_wide, precision=highest),
        within + (before_log + entry_top[None, :])[..., None],
    )
    numerator, denominator, peak_log = blend_parts((numerator, denominator, peak_log), from_left)
    hidden = numerator / jnp.maximum(jnp.abs(denominator), jnp.exp(-peak_log))[..., None]
    hidden = hidden.transpose(0, 2, 1, 3).reshape(group_len, local_heads, value_width)
    head_gains = lax.dynamic_slice_in_dim(
        head_gain, first_head * value_width, local_heads * value_width, 0
    )
    head_gains = head_gains.astype(jnp.float32).reshape(local_heads, value_width)
    normed_heads = (
        hidden
        * lax.rsqrt(jnp.mean(hidden * hidden, axis=2, keepdims=True) + norm_floor)
        * head_gains
    )
    normed_heads = normed_heads.astype(jnp.bfloat16).reshape(group_len, local_heads * value_width)
    out_slab = lax.all_gather(w_out, "sp", axis=0, tiled=True)
    return lax.psum_scatter(
        lax.dot_general(
            normed_heads, out_slab, (((1,), (1,)), ((), ())), preferred_element_type=jnp.float32
        ).astype(jnp.bfloat16),
        "tp",
        scatter_dimension=0,
        tiled=True,
    )


drift_span = 128
MESH = pl.DeviceIdType.MESH
f32 = jnp.float32
bf16 = jnp.bfloat16


def dot_nt(a, b):
    return lax.dot_general(a, b, (((1,), (1,)), ((), ())), preferred_element_type=f32)


def layer_kernel(
    n,
    tp,
    tokens,
    pre_gain,
    w_key,
    w_value,
    w_query,
    w_igate,
    w_fgate,
    forget_bias,
    drift,
    head_gain,
    w_out,
    out,
    tok_own,
    tok_all,
    normed,
    gain_in,
    igate_in,
    fgate_in,
    bias_in,
    head_gain_in,
    drift_in,
    key_own,
    value_own,
    query_own,
    key_all,
    value_all,
    query_all,
    out_all,
    acc,
    state_all,
    aux_all,
    heads,
    heads_in,
    part,
    load_sems,
    tok_send,
    tok_recv,
    drift_send,
    drift_recv,
    w_send,
    pass_send,
    w_recv,
    out_send,
    out_recv,
    state_send,
    state_recv,
    aux_send,
    aux_recv,
    heads_send,
    heads_recv,
    final_send,
    final_recv,
):
    s = lax.axis_index("sp")
    t = lax.axis_index("tp")
    layers = n // 2
    z = s // 2
    x = s % 2
    y = t // 2
    c = t % 2
    zh = z // 2
    zl = z % 2
    near = zh == c
    far = jnp.logical_not(near)
    head = layers * y + z
    rows = tok_own.shape[0]
    span = rows * tp
    length = 2 * span
    depth = key_own.shape[1]
    dk = key_own.shape[2]
    dv = value_own.shape[2]

    def flip(value):
        return 1 - value

    def at_layer(dz):
        if dz == 0:
            return z
        if dz == 1:
            return 2 * zh + flip(zl)
        if dz == 2:
            return 2 * flip(zh) + zl
        return 2 * flip(zh) + flip(zl)

    def dev(zz, xx, yy, cc):
        return 2 * zz + xx, 2 * yy + cc

    barrier = pltpu.get_barrier_semaphore()
    to_sibling = dev(z, x, y, flip(c))
    partners = [dev(z, flip(x), y, cc) for cc in range(2)]
    for dz in range(layers):
        for yy in (y, flip(y)) if dz < 2 else (y,):
            partners += [dev(at_layer(dz), x, yy, cc) for cc in range(2)]
    partners[2:4] = [to_sibling]
    for ss, tt in partners:
        pl.semaphore_signal(
            barrier,
            inc=1,
            device_id={"sp": ss, "tp": tt},
            device_id_type=MESH,
        )

    def load(source, target, sem):
        copy = pltpu.make_async_copy(source, target, sem)
        copy.start()
        return copy

    pieces = (
        (w_key, key_own, key_all),
        (w_value, value_own, value_all),
        (w_query, query_own, query_all),
    )

    def token_slot(parity, to_t):
        start = pl.multiple_of((parity * tp + to_t) * rows, rows)
        return tok_all.at[pl.ds(start, rows)]

    own_slot = token_slot(zl, t)
    load_tokens = load(tokens, tok_own, load_sems.at[0])
    loads_own = []
    for p, (w_hbm, own, full) in enumerate(pieces):
        width = own.shape[2]
        loads_own.append(
            [
                load(
                    w_hbm.at[:, pl.ds(j * width, width)],
                    own.at[j],
                    load_sems.at[1 + p],
                )
                for j in range(2)
            ]
        )
    chunk = out_all.shape[3] // 2
    loads_out = [
        load(
            w_out.at[pl.ds(i * chunk, chunk)],
            out_all.at[zh, x, c, pl.ds(i * chunk, chunk)],
            load_sems.at[4],
        )
        for i in range(2)
    ]
    small = (
        (pre_gain, gain_in),
        (w_igate, igate_in),
        (w_fgate, fgate_in),
        (forget_bias, bias_in),
        (head_gain, head_gain_in),
    )
    loads_small = [load(a, b, load_sems.at[5 + i]) for i, (a, b) in enumerate(small)]

    @pl.when(near)
    def _():
        pltpu.make_async_copy(tokens, own_slot, tok_recv.at[zl, 0, c]).start()
        pltpu.make_async_copy(drift, drift_in.at[zl], drift_recv.at[0]).start()
        for p, (w_hbm, own, full) in enumerate(pieces):
            width = own.shape[2]
            for j in range(2):

                @pl.when(zl == j)
                def _():
                    pltpu.make_async_copy(
                        w_hbm.at[:, pl.ds(j * width, width)], full.at[s], w_recv.at[p, 0]
                    ).start()

    load_drift = load(drift, drift_in.at[2], load_sems.at[10])

    @pl.when(c == 0)
    def _():
        state_all[layers:, :, :] = jnp.zeros((layers, dk, dv), bf16)
        aux_all[layers:, :, :] = jnp.zeros((layers, aux_all.shape[1], dk), f32)

    pl.semaphore_wait(barrier, len(partners))

    def plan(source, target, send_sem, recv_sem, to, flag=None):
        copy = pltpu.make_async_remote_copy(
            src_ref=source,
            dst_ref=target,
            send_sem=send_sem,
            recv_sem=recv_sem,
            device_id={"sp": to[0], "tp": to[1]},
            device_id_type=MESH,
        )
        return copy

    def send(source, target, send_sem, recv_sem, to, flag=None, keep=None):
        if keep is not None:

            @pl.when(keep)
            def _():
                pltpu.make_async_copy(source, target, recv_sem).start()

            flag = jnp.logical_not(keep)
        copy = plan(source, target, send_sem, recv_sem, to, flag)
        if flag is None:
            copy.start()
        else:
            pl.when(flag)(copy.start)

    def arrived(target, sem):
        pltpu.make_async_copy(target, target, sem).wait()

    load_tokens.wait()
    mine = tok_recv.at[zl, 0, c]
    send(tok_own, own_slot, tok_send.at[0], mine, dev(at_layer(2), x, y, zh))
    send(tok_own, own_slot, tok_send.at[0], mine, dev(at_layer(1), x, y, zh))
    send(
        tok_own, own_slot, tok_send.at[0], tok_recv.at[zl, 1, c], dev(z, x, flip(y), zh)
    )
    send(tok_own, own_slot, tok_send.at[0], mine, dev(z, x, y, flip(c)), flag=far)
    load_drift.wait()
    for i in range(1, 4):
        send(
            drift_in.at[2],
            drift_in.at[zl],
            drift_send.at[0],
            drift_recv.at[0],
            dev(at_layer(i), x, y, c),
            flag=near,
        )

    for copy in loads_small:
        copy.wait()
    gain = gain_in[...].astype(f32)[None, :]

    def normalize(parity, to_t):
        start = pl.multiple_of((parity * tp + to_t) * rows, rows)
        wide = tok_all[pl.ds(start, rows), :].astype(f32)
        scale = lax.rsqrt(jnp.mean(wide * wide, axis=1, keepdims=True) + norm_floor)
        normed[pl.ds(start, rows), :] = (wide * scale * gain).astype(bf16)

    to_x = dev(z, flip(x), y, c)
    to_core = dev(z, x, y, flip(c))
    to_half = dev(at_layer(2), x, y, c)

    def plan_first(p):
        _, own, full = pieces[p]
        sem = w_recv.at[p, 2]
        side_sem = w_recv.at[p, 1]
        middle = dev(1 + c * (layers - 3), x, y, c)
        end = dev(c * (layers - 1), x, y, c)
        beside = dev(at_layer(1), x, y, c)
        target = full.at[s]
        return (
            plan(own.at[flip(c)], target, w_send.at[p], sem, middle, far),
            plan(own.at[c], target, w_send.at[p], sem, end, far),
            plan(own.at[flip(zl)], target, w_send.at[p], side_sem, beside, near),
        )

    def plan_pass(p, dzs, across):
        blocks = [2 * at_layer(dz) + (flip(x) if across else x) for dz in dzs]
        refs = [pieces[p][2].at[block] for block in blocks]
        sem = w_recv.at[p, (3 if dzs[0] == 0 else 4) if across else min(dzs[0], 2)]
        across_sem = w_recv.at[p, 3 if dzs[0] == 0 else 4]
        to_far = w_recv.at[p, 0]
        onward = []
        for full in refs:
            if not across:
                onward.append(plan(full, full, pass_send.at[0], across_sem, to_x, near))
            onward.append(plan(full, full, pass_send.at[1], to_far, to_core, near))

        def run():
            arrived(pieces[p][2].at[pl.ds(0, len(refs))], sem)
            for copy in onward:
                copy.start()

        return run

    def plan_token(parity, c_src, i, onward):
        slot = token_slot(parity, 2 * y + c_src)
        sem = tok_recv.at[parity, 0, c_src]
        out_sem = tok_recv.at[parity, 1, c_src]
        to_y = dev(z, x, flip(y), c)
        copies = []
        if onward:
            copies.append(
                plan(slot, slot, tok_send.at[1], sem, dev(at_layer(1), x, y, c), far)
            )
        copies.append(
            plan(slot, slot, tok_send.at[1], out_sem, to_y, far if onward else None)
        )

        def run(forward=True):
            arrived(slot, sem)
            if forward:
                for copy in copies:
                    copy.start()

        return run

    def out_chunk(zb, xb, cb, i):
        return out_all.at[zb, xb, cb, pl.ds(i * chunk, chunk)]

    def plan_out(zb, xb, i, to):
        piece = out_chunk(zb, xb, c, i)
        targets = {
            "half": (out_send.at[0], out_recv.at[i], to_half),
            "x": (out_send.at[1], out_recv.at[2], to_x),
            "far_x": (out_send.at[1], out_recv.at[3 + i], to_x),
            "core": (out_send.at[2], out_recv.at[5 + 2 * zb + xb], to_core),
        }
        return [plan(piece, piece, targets[k][0], targets[k][1], targets[k][2]) for k in to]

    firsts = [plan_first(p) for p in range(3)]
    direct = [[plan_pass(p, dzs, False) for dzs in ((0,), (1,), (2, 3))] for p in range(3)]
    cross = [[plan_pass(p, dzs, True) for dzs in ((0,), (1, 2, 3))] for p in range(3)]
    token_a = [plan_token(zl, k, k, True) for k in range(2)]
    token_b = [plan_token(flip(zl), k, 2 + k, False) for k in range(2)]
    out_own = [plan_out(zh, x, i, ("x", "core")) for i in range(2)]
    out_half = [plan_out(zh, x, i, ("half",))[0] for i in range(2)]

    out_near_x = [plan_out(zh, flip(x), i, ("core",)) for i in range(2)]
    out_far = [plan_out(flip(zh), x, i, ("far_x", "core")) for i in range(2)]
    out_far_x = [plan_out(flip(zh), flip(x), i, ("core",)) for i in range(2)]

    def out_from_x():
        arrived(out_all.at[zh, flip(x), c], out_recv.at[2])
        for i in range(2):
            out_near_x[i][0].start()

    def out_from_half(i):
        arrived(out_chunk(flip(zh), x, c, i), out_recv.at[i])
        for copy in out_far[i]:
            copy.start()

    def out_start():
        arrived(out_all.at[zh, x, c], load_sems.at[4])
        for pair in out_own:
            for copy in pair:
                copy.start()

    for p in range(3):
        arrived(pieces[p][1], load_sems.at[1 + p])

    @pl.when(near)
    def _():
        firsts[1][2].start()
        for p in (1, 0, 2):
            direct[p][0]()
        out_start()
        for run in token_a:
            run(False)
        for run in token_b:
            run()

    @pl.when(far)
    def _():
        firsts[1][1].start()
        firsts[1][0].start()
        firsts[0][1].start()
        firsts[0][0].start()
        out_start()
        for run in token_a:
            run()
        for i in (1, 0):
            firsts[2][i].start()
        for run in token_b:
            run()
        arrived(pieces[0][1], w_send.at[0])
        for copy in out_half:
            copy.start()
        arrived(pieces[2][1], w_send.at[2])

    for parity in range(2):
        for c_src in range(2):
            normalize(parity, 2 * y + c_src)

    @pl.when(near)
    def _():
        firsts[0][2].start()
        firsts[2][2].start()
        direct[1][1]()
        direct[1][2]()
        for p in (1, 0, 2):
            cross[p][0]()

    for parity in range(2):
        for c_src in range(2):
            to_t = 2 * flip(y) + c_src
            arrived(token_slot(parity, to_t), tok_recv.at[parity, 1, c_src])
            normalize(parity, to_t)

    all_normed = normed[...]
    gate_in = dot_nt(all_normed, igate_in[...])
    gate_forget = dot_nt(all_normed, fgate_in[...])
    pick = lax.broadcasted_iota(jnp.int32, gate_in.shape, 1) == head
    pick_bias = lax.broadcasted_iota(jnp.int32, bias_in.shape, 1) == head
    bias = jnp.sum(jnp.where(pick_bias, bias_in[...], 0.0), axis=1, keepdims=True)
    forget_all = jnp.sum(jnp.where(pick, gate_forget, 0.0), axis=1, keepdims=True) + bias
    input_all = jnp.sum(jnp.where(pick, gate_in, 0.0), axis=1, keepdims=True)
    row_id = lax.broadcasted_iota(jnp.int32, (span, span), 0)
    col_id = lax.broadcasted_iota(jnp.int32, (span, span), 1)
    causal = row_id >= col_id
    eye = row_id == col_id
    arrived(drift_in.at[pl.ds(0, 2)], drift_recv.at[0])
    gates = []
    for j in range(2):
        offset = drift_in[j, pl.ds(head, 1), :][:, :1]
        pre = forget_all[j * span : (j + 1) * span] + offset
        in_col = input_all[j * span : (j + 1) * span]
        lf_col = jnp.minimum(pre, 0.0) - jnp.log1p(jnp.exp(-jnp.abs(pre)))
        lf_row = jnp.sum(jnp.where(eye, lf_col, 0.0), axis=0, keepdims=True)
        in_row = jnp.sum(jnp.where(eye, in_col, 0.0), axis=0, keepdims=True)
        b_col = jnp.sum(jnp.where(causal, lf_row, 0.0), axis=1, keepdims=True)
        b_row = jnp.sum(jnp.where(row_id <= col_id, lf_col, 0.0), axis=0, keepdims=True)
        total = jnp.sum(lf_col, axis=0, keepdims=True)
        write = total - b_col + in_col
        top = jnp.max(write, axis=0, keepdims=True)
        write_scale = jnp.exp(write - top)
        log_pair = jnp.where(causal, b_col - b_row + in_row, lowest_log)
        peak = jnp.max(log_pair, axis=1, keepdims=True)
        decay = jnp.where(causal, jnp.exp(log_pair - peak), 0.0)
        gates.append((b_col, total, top, write_scale, peak, decay))


    @pl.when(near)
    def _():
        direct[0][1]()
        direct[0][2]()
        cross[1][1]()
        direct[2][1]()
        direct[2][2]()
        for copy in out_half:
            copy.start()

    cols = (slice(0, dk), slice(dk, dk + dv), slice(dk + dv, 2 * dk + dv))

    def products(p):
        full = pieces[p][2]

        @pl.when(far)
        def _():
            arrived(full, w_recv.at[p, 0])

        flat = full[...].reshape(n * depth, full.shape[2])
        acc[:, cols[p]] = jnp.dot(normed[...], flat, preferred_element_type=f32)

    products(1)

    @pl.when(near)
    def _():
        cross[0][1]()

    products(0)

    spans = [4 * c + 2 * j + x for j in range(2)]
    keys = (acc[:, cols[0]] * (dk**-0.5)).astype(bf16)
    values = acc[:, cols[1]].astype(bf16)
    for j in range(2):
        b_col, total, top, write_scale, peak, decay = gates[j]
        at = slice(j * span, (j + 1) * span)
        key_scaled = keys[at].astype(f32) * write_scale
        state_all[spans[j]] = jnp.dot(
            key_scaled.T.astype(bf16), values[at], preferred_element_type=f32
        ).astype(bf16)
        mine = spans[j]
        aux_all[mine, 0:1, :] = jnp.broadcast_to(total, (1, dk))
        aux_all[mine, 1:2, :] = jnp.broadcast_to(top, (1, dk))
        aux_all[mine, 2:3, :] = jnp.sum(key_scaled, axis=0, keepdims=True)
        aux_all[mine, 3:, :] = jnp.zeros((aux_all.shape[1] - 3, dk), f32)
    late = c == 1
    early = c == 0
    for k, (to, flag) in enumerate(
        (
            (dev(z, flip(x), y, c), None),
            (dev(z, flip(x), y, flip(c)), early),
            (dev(z, x, y, flip(c)), early),
        )
    ):
        group = 0 if k == 0 else 1
        for j in range(2):
            mine = spans[j]
            send(
                aux_all.at[mine],
                aux_all.at[mine],
                aux_send.at[0],
                aux_recv.at[group],
                to,
                flag=flag,
            )
            send(
                state_all.at[mine],
                state_all.at[mine],
                state_send.at[0],
                state_recv.at[group],
                to,
                flag=flag,
            )

    @pl.when(near)
    def _():
        cross[2][1]()

    products(2)
    queries = acc[:, cols[2]].astype(bf16)
    intra = []
    for j in range(2):
        b_col, total, top, write_scale, peak, decay = gates[j]
        at = slice(j * span, (j + 1) * span)
        weights = dot_nt(queries[at], keys[at]) * decay
        numer = jnp.dot(weights.astype(bf16), values[at], preferred_element_type=f32)
        denom = jnp.sum(weights, axis=1, keepdims=True)
        intra.append((numer, denom))

    pl.when(near)(functools.partial(out_from_half, 0))
    arrived(aux_all.at[pl.ds(0, 2)], aux_recv.at[0])
    arrived(state_all.at[pl.ds(0, 2)], state_recv.at[0])

    @pl.when(late)
    def _():
        arrived(aux_all.at[pl.ds(0, layers)], aux_recv.at[1])
        arrived(state_all.at[pl.ds(0, layers)], state_recv.at[1])

    span_rows = aux_all[:, 0, :]
    top_rows = aux_all[:, 1, :]
    vec_rows = aux_all[:, 2, :]
    place = lax.broadcasted_iota(jnp.int32, span_rows.shape, 0)
    gain_row = head_gain_in[pl.ds(pl.multiple_of(head * dv, dv), dv)].astype(f32)[None, :]
    for j in range(2):
        b_col, total, top, write_scale, peak, decay = gates[j]
        numer, denom = intra[j]
        at = slice(j * span, (j + 1) * span)
        before = place < spans[j]
        logs = top_rows
        for m in range(1, n):
            between = (place < m) & (spans[j] > m)
            logs = logs + jnp.where(between, span_rows[m : m + 1, :], 0.0)
        logs = jnp.where(before, logs, lowest_log)
        entry = jnp.max(logs, axis=0, keepdims=True)
        weight = jnp.where(before, jnp.exp(logs - entry), 0.0)
        vec = jnp.sum(weight * vec_rows, axis=0, keepdims=True)
        mat = jnp.zeros((dk, dv), f32)
        for m in range(n - 1):
            mat = mat + weight[m : m + 1, :1] * state_all[m].astype(f32)
        carried = b_col + entry[:, :1]
        new_top = jnp.maximum(peak, carried)
        w_intra = jnp.exp(peak - new_top)
        w_carry = jnp.exp(carried - new_top)
        numer = w_intra * numer + w_carry * jnp.dot(
            queries[at], mat.astype(bf16), preferred_element_type=f32
        )
        denom = w_intra * denom + w_carry * jnp.sum(
            queries[at].astype(f32) * vec, axis=1, keepdims=True
        )
        hidden = numer / jnp.maximum(jnp.abs(denom), jnp.exp(-new_top))
        heads[j] = (
            hidden
            * lax.rsqrt(jnp.mean(hidden * hidden, axis=1, keepdims=True) + norm_floor)
            * gain_row
        ).astype(bf16)
        for d in range(2):
            send(
                heads.at[j],
                heads_in.at[z],
                heads_send.at[0],
                heads_recv.at[zh],
                dev(2 * c + d, x, y, j),
                keep=near & (zl == d) & (c == j),
            )

    out_from_x()
    pl.when(far)(functools.partial(out_from_half, 0))
    out_from_half(1)
    features = out_all.shape[3]
    home = 2 * zh + c
    wide = 2 * features

    def landing(yy, zz, zb, xb):
        start = pl.multiple_of((zz + 2 * zb) * wide + xb * features, features)
        return out.at[yy, :, pl.ds(start, features)]

    def out_arrived(zb, xb):
        arrived(out_all.at[zb, xb, flip(c)], out_recv.at[5 + 2 * zb + xb])

    def heads_arrived(half):
        arrived(heads_in.at[pl.ds(2 * half, 2)], heads_recv.at[half])

    def project(zb, xb, half):
        total = jnp.zeros((span, features), f32)
        for i in range(2):
            total = total + dot_nt(
                heads_in[2 * half + i], out_all[zb, xb, half, :, i * dv : (i + 1) * dv]
            )
        return total

    def share(zb, xb, total):
        part[zb, xb] = total.astype(bf16)
        for yy in range(2):
            for cc in range(2):
                send(
                    part.at[zb, xb, pl.ds((2 * yy + cc) * rows, rows)],
                    landing(y, zl, zb, xb),
                    final_send.at[0],
                    final_recv.at[0],
                    dev(home, x, yy, cc),
                    keep=(zl == c) & (y == yy) & (c == cc),
                )

    sides = (x, flip(x))
    for xb in sides:
        out_arrived(zh, xb)
    heads_arrived(zh)
    early_part = [project(zh, xb, zh) for xb in sides]
    for i in range(2):
        arrived(out_chunk(flip(zh), flip(x), c, i), out_recv.at[3 + i])
        out_far_x[i][0].start()
    heads_arrived(flip(zh))
    for k, xb in enumerate(sides):
        share(zh, xb, early_part[k] + project(zh, xb, flip(zh)))
    for xb in sides:
        out_arrived(flip(zh), xb)
        share(flip(zh), xb, project(flip(zh), xb, zh) + project(flip(zh), xb, flip(zh)))
    arrived(out, final_recv.at[0])

    def drained(ref, sem, flag=None):
        if flag is None:
            arrived(ref, sem)
        else:
            pl.when(flag)(functools.partial(arrived, ref, sem))

    drained(tok_all.at[pl.ds(0, 4 * rows)], tok_send.at[0], far)
    drained(tok_all.at[pl.ds(0, 6 * rows)], tok_send.at[1], far)
    drained(tok_all.at[pl.ds(0, 3 * rows)], tok_send.at[0], near)
    drained(tok_all.at[pl.ds(0, 2 * rows)], tok_send.at[1], near)
    drained(drift_in, drift_send.at[0], near)
    for p in range(3):
        _, own, full = pieces[p]
        if p == 1:
            drained(own, w_send.at[p], far)
        drained(own.at[0], w_send.at[p], near)
    drained(out_all.at[0], pass_send.at[0], near)
    drained(out_all, pass_send.at[1], near)
    drained(out_all.at[0, 0, 0], out_send.at[0])
    drained(out_all.at[0, 0], out_send.at[1])
    drained(out_all.at[0], out_send.at[2])
    for ref, sem in ((state_all, state_send.at[0]), (aux_all, aux_send.at[0])):
        drained(ref.at[pl.ds(0, 6)], sem, early)
        drained(ref.at[pl.ds(0, 2)], sem, late)
    drained(heads_in.at[pl.ds(0, 3)], heads_send.at[0], near)
    drained(heads_in, heads_send.at[0], far)
    at_home = zl == c
    drained(part, final_send.at[0], jnp.logical_not(at_home))
    drained(part.at[:, :, pl.ds(0, 3 * rows)], final_send.at[0], at_home)


def on_device_layers(
    n,
    tp,
    tokens,
    pre_gain,
    w_query,
    w_key,
    w_value,
    w_igate,
    w_fgate,
    forget_bias,
    gate_drift,
    head_gain,
    w_out,
):
    heads = w_igate.shape[1]
    rows, width = tokens.shape
    span = rows * tp
    if (
        heads != 2 * tp
        or n != heads
        or gate_drift.shape[0] != span
        or span > drift_span
    ):
        return on_device(
            tokens,
            pre_gain,
            w_query,
            w_key,
            w_value,
            w_igate,
            w_fgate,
            forget_bias,
            gate_drift,
            head_gain,
            w_out,
        )
    layers = n // 2
    depth = w_query.shape[0]
    dk = w_query.shape[1] // 2
    dv = w_value.shape[1] // 2
    features = w_out.shape[0]
    anywhere = pl.BlockSpec(memory_space=pl.ANY)
    dma = pltpu.SemaphoreType.DMA
    vmem = pltpu.VMEM
    parts = pl.pallas_call(
        functools.partial(layer_kernel, n, tp),
        out_shape=pltpu.VMEM((2, rows, features * n), bf16),
        in_specs=[anywhere] * 11,
        out_specs=anywhere,
        scratch_shapes=[
            vmem((rows, width), bf16),
            vmem((2 * span, width), bf16),
            vmem((2 * span, width), bf16),
            vmem((width,), bf16),
            vmem((heads, width), bf16),
            vmem((heads, width), bf16),
            vmem((1, heads), f32),
            vmem((heads * dv,), bf16),
            vmem((3, heads, span), f32),
            vmem((2, depth, dk), bf16),
            vmem((2, depth, dv), bf16),
            vmem((2, depth, dk), bf16),
            vmem((n, depth, dk), bf16),
            vmem((n, depth, dv), bf16),
            vmem((n, depth, dk), bf16),
            vmem((2, 2, 2, features, 2 * dv), bf16),
            vmem((2 * span, 2 * dk + dv), f32),
            vmem((n, dk, dv), bf16),
            vmem((n, 8, dk), f32),
            vmem((2, span, dv), bf16),
            vmem((layers, span, dv), bf16),
            vmem((2, 2, span, features), bf16),
            dma((11,)),
            dma((2,)),
            dma((2, 2, 2)),
            dma((1,)),
            dma((1,)),
            dma((3,)),
            dma((2,)),
            dma((3, 5)),
            dma((3,)),
            dma((9,)),
            dma((1,)),
            dma((2,)),
            dma((1,)),
            dma((2,)),
            dma((1,)),
            dma((2,)),
            dma((1,)),
            dma((1,)),
        ],
        compiler_params=pltpu.CompilerParams(collective_id=0, has_side_effects=True),
    )(
        tokens,
        pre_gain,
        w_key,
        w_value,
        w_query,
        w_igate.T,
        w_fgate.T,
        forget_bias[None, :],
        gate_drift.T,
        head_gain,
        w_out,
    )
    return jnp.sum(parts.astype(f32), axis=0).astype(bf16)


def solution(mesh):
    in_specs = (
        P(("sp", "tp"), None),
        P(),
        P("sp", "tp"),
        P("sp", "tp"),
        P("sp", "tp"),
        P(),
        P(),
        P(),
        P("sp", None),
        P(),
        P("sp", "tp"),
    )
    out_specs = P(("sp", "tp"), None)
    body = on_device
    if mesh.shape["sp"] == 2 * mesh.shape["tp"] and mesh.shape["tp"] == 4:
        body = functools.partial(on_device_layers, mesh.shape["sp"], mesh.shape["tp"])
    return jax.shard_map(
        body, mesh=mesh, in_specs=in_specs, out_specs=out_specs, check_vma=False
    )
```
